256 devices in a mesh: sp: 16 (over y, x), tp: 16 (over z, core).
Axes of the slice: x: 4, y: 4, z: 8, core: 2. Of those that a mesh axis runs over, the one named last changes fastest.
Arguments:
- queries: bfloat16 [16384, 2048], P('sp', 'tp'), may hold values from -8 to 8
- keys: bfloat16 [16384, 512], P('sp'), may hold values from -6 to 6
- values: bfloat16 [16384, 512], P('sp'), may hold values from -6 to 6
- query_gain: float32 [2048], P('tp'), may hold values from 0.2 to 40
- key_gain: float32 [128], replicated, may hold values from 0.1 to 1.9
- out_weight: bfloat16 [2048, 2048], replicated, may hold values from -0.125 to 0.125
- residual: bfloat16 [16384, 2048], P(('sp', 'tp')), may hold values from -2 to 2
- norm_gain: float32 [2048], replicated, may hold values from 0.1 to 1.9
- route_experts: int32 [16384, 2], P(('sp', 'tp')), may hold values from 0 to 15, as said below
- expert_scores: float32 [16384, 2], P(('sp', 'tp')), may hold values from -9 to 9
- group_prob: float32 [16384], P(('sp', 'tp')), may hold values from 0.5 to 1
- w_gate: bfloat16 [16, 2048, 2048], P('sp', None, 'tp'), may hold values from -0.125 to 0.125
- w_up: bfloat16 [16, 2048, 2048], P('sp', None, 'tp'), may hold values from -0.125 to 0.125
- w_down: bfloat16 [16, 2048, 2048], P('sp', 'tp'), may hold values from -0.125 to 0.125
Outputs:
- mixed: bfloat16 [16384, 2048], P(('sp', 'tp'))
The draws below stay inside these ranges and needn't reach their ends.
Inputs may be any that keep to these rules, and one draw needn't show every extreme that they name: `route_experts`: each row names 2 different experts of one group, expert e lying in group e // 8. In the rows of one device (aligned blocks of 64 rows) 5 * 8 rows choose one group and the others another; inside a group those rows are spread over its experts as evenly as whole numbers allow, so no expert is named by more than 10 rows of one device and some expert by exactly 10.
All inputs are finite; a program needn't handle non-finite values.
Results may differ from the reference program's by a relative error of at most 0.025.
Values may be sent and summed in bfloat16 or wider, within the bound.
No kernel may reach another device: no remote copies, remote signals or barrier semaphores. Data moves between devices by JAX's collectives and lax.ppermute only.
A program may use at most 128 MiB of HBM per device.

```python
import math
import jax
import jax.numpy as jnp
from jax import lax

D = 2048
HEADS = 16
KV_HEADS = 4
HEAD = 128
EXPERT_HIDDEN = 2048
GROUPS = 2
TOP = 2
GRID_W = 64
TOKENS = 16384
ROWS = 64
EXPERTS = 16
GROUP_EXPERTS = 8
UNIT_BLOCK = 128
CAP = 10
N_SP = 16
N_TP = 16


def key_field(key):
    drawn = jax.random.normal(jax.random.fold_in(key, 101), (TOKENS, KV_HEADS * HEAD), jnp.float32)
    return jnp.clip(drawn, -6.0, 6.0)


def draw_keys(key, part):
    return key_field(key).astype(jnp.bfloat16)


def draw_queries(key, part):
    anchor = jax.random.fold_in(key, 202)
    drawn = jax.random.normal(anchor, (TOKENS, HEADS * HEAD), jnp.float32)
    return jnp.clip(drawn, -6.0, 6.0).astype(jnp.bfloat16)


def draw_query_gain(key, part):
    level = jax.random.uniform(jax.random.fold_in(key, 301), (HEADS, 1), jnp.float32, math.log(1.2), math.log(3.0))
    jitter = 1.0 + 0.18 * jnp.clip(jax.random.normal(jax.random.fold_in(key, 302), (HEADS, HEAD), jnp.float32), -3.0, 3.0)
    return (jnp.exp(level) * jitter).reshape(HEADS * HEAD)


def draw_residual(key, part):
    columns = jnp.exp(jax.random.uniform(jax.random.fold_in(key, 401), (1, D), jnp.float32, math.log(0.3), math.log(3.0)))
    vectors = jnp.clip(jax.random.normal(jax.random.fold_in(key, 403), (TOKENS, D), jnp.float32), -6.0, 6.0)
    return (0.1 * vectors * columns).astype(jnp.bfloat16)


def route_block(block_key):
    order = jax.random.permutation(jax.random.fold_in(block_key, 1), ROWS)
    ranking = jnp.argsort(order).astype(jnp.int32)
    big_group = jax.random.randint(jax.random.fold_in(block_key, 2), (), 0, GROUPS)
    offset = jax.random.randint(jax.random.fold_in(block_key, 4), (), 0, GROUPS - 1)
    small_group = (big_group + 1 + offset) % GROUPS
    big_count = 5 * ROWS // 8
    in_big = ranking < big_count
    member = jnp.where(in_big, ranking, ranking - big_count)
    group_of = jnp.where(in_big, big_group, small_group)
    round_count = TOP * ROWS // GROUP_EXPERTS + 2
    round_keys = jax.random.split(jax.random.fold_in(block_key, 3), round_count)
    table = jax.vmap(lambda round_key: jax.random.permutation(round_key, GROUP_EXPERTS))(round_keys)
    first_place = TOP * member
    local = jnp.stack([table[(first_place + choice_rank) // GROUP_EXPERTS, (first_place + choice_rank) % GROUP_EXPERTS] for choice_rank in range(TOP)], axis=1)
    return group_of[:, None] * GROUP_EXPERTS + local


def draw_route_experts(key, part):
    block_total = TOKENS // ROWS
    block_keys = jax.random.split(jax.random.fold_in(key, 501), block_total)
    return jax.vmap(route_block)(block_keys).reshape(TOKENS, TOP).astype(jnp.int32)


def block_scale(own_key, dims, cuts, low, high):
    factor_of, own = 1.0, jax.random.fold_in(own_key, 6)
    for dim, parts in cuts:
        draws = jnp.exp(jax.random.uniform(jax.random.fold_in(own, dim), (parts,), jnp.float32, low / len(cuts), high / len(cuts)))
        factor_of = factor_of * jnp.repeat(draws, dims[dim] // parts).reshape([-1 if axis == dim else 1 for axis in range(len(dims))])
    return factor_of


def centred(own_key, dims, scale, bound, shards=(), kind=jnp.bfloat16):
    entries = jax.random.normal(own_key, dims, jnp.float32) * scale
    if len(shards) > 0:
        entries = block_scale(own_key, dims, shards, -0.22, 0.18) * entries
    return jnp.clip(entries, min=-bound, max=bound).astype(kind)


def setup_inputs(seed: int = 0) -> dict:
    seeds = jax.random.split(jax.random.key(seed), 15)
    queries = draw_queries(jax.random.fold_in(seeds[14], 71), 0)
    keys = draw_keys(jax.random.fold_in(seeds[14], 71), 0)
    values = centred(seeds[2], (TOKENS, KV_HEADS * HEAD), 1.0, 6.0, ((0, 16),))
    query_gain = draw_query_gain(jax.random.fold_in(seeds[14], 71), 0)
    key_gain = jnp.clip(1.0 + 0.18 * jax.random.normal(seeds[4], (HEAD,), jnp.float32), 0.1, 1.9)
    out_weight = centred(seeds[5], (HEADS * HEAD, D), (HEADS * HEAD) ** -0.5, 0.125)
    residual = draw_residual(jax.random.fold_in(seeds[14], 71), 0)
    norm_gain = jnp.clip(1.0 + 0.18 * jax.random.normal(seeds[7], (D,), jnp.float32), 0.1, 1.9)
    route_experts = draw_route_experts(jax.random.fold_in(seeds[14], 71), 0)
    expert_scores = centred(seeds[9], (TOKENS, TOP), 1.5, 9.0, ((0, 256),), jnp.float32)
    group_prob = jnp.clip(0.5 + 0.5 * jax.random.uniform(seeds[10], (TOKENS,), jnp.float32) ** block_scale(seeds[10], (TOKENS,), ((0, 256),), -0.2, 0.2), 0.5, 1.0)
    w_gate = centred(seeds[11], (EXPERTS, D, EXPERT_HIDDEN), D ** -0.5, 0.125, ((0, 16), (2, 16)))
    w_up = centred(seeds[12], (EXPERTS, D, EXPERT_HIDDEN), D ** -0.5, 0.125, ((0, 16), (2, 16)))
    w_down = centred(seeds[13], (EXPERTS, EXPERT_HIDDEN, D), EXPERT_HIDDEN ** -0.5, 0.125, ((0, 16), (1, 16)))
    return dict(queries=queries, keys=keys, values=values, query_gain=query_gain, key_gain=key_gain, out_weight=out_weight, residual=residual, norm_gain=norm_gain, route_experts=route_experts, expert_scores=expert_scores, group_prob=group_prob, w_gate=w_gate, w_up=w_up, w_down=w_down)


rope_base = 10000.0
norm_eps = 1e-06
query_block = 128

def rope_tables(positions, head_size):
    quarter = head_size // 4
    frequency = rope_base ** (-jnp.arange(quarter, dtype=jnp.float32) * 4.0 / head_size)
    grid_row = (positions // GRID_W).astype(jnp.float32)
    grid_column = (positions % GRID_W).astype(jnp.float32)
    angles = jnp.concatenate([grid_row[:, None] * frequency[None, :], grid_column[:, None] * frequency[None, :]], axis=1)
    return (jnp.cos(angles), jnp.sin(angles))

def rotate_pairs(vectors, cosine_table, sine_table):
    paired = vectors.reshape(vectors.shape[0], vectors.shape[1], vectors.shape[2] // 2, 2)
    leading = paired[..., 0]
    trailing = paired[..., 1]
    cosine_now = cosine_table[:, None, :]
    sine_now = sine_table[:, None, :]
    turned = jnp.stack([leading * cosine_now - trailing * sine_now, leading * sine_now + trailing * cosine_now], axis=-1)
    return turned.reshape(vectors.shape)

def head_norm(vectors, gain_row):
    factor = lax.rsqrt(lax.optimization_barrier(jnp.mean(vectors * vectors, axis=-1, keepdims=True)) + norm_eps)
    return vectors * factor * gain_row

def reference(queries, keys, values, query_gain, key_gain, out_weight, residual, norm_gain, route_experts, expert_scores, group_prob, w_gate, w_up, w_down):
    token_count = queries.shape[0]
    positions = jnp.arange(token_count, dtype=jnp.int32)
    cosine_table, sine_table = rope_tables(positions, HEAD)
    query_heads = queries.astype(jnp.float32).reshape(token_count, HEADS, HEAD)
    query_heads = rotate_pairs(head_norm(query_heads, query_gain.reshape(1, HEADS, HEAD)), cosine_table, sine_table)
    query_heads = lax.optimization_barrier(query_heads.astype(jnp.bfloat16))
    key_heads = keys.astype(jnp.float32).reshape(token_count, KV_HEADS, HEAD)
    key_heads = rotate_pairs(head_norm(key_heads, key_gain.reshape(1, 1, HEAD)), cosine_table, sine_table)
    key_wide = lax.optimization_barrier(key_heads.astype(jnp.bfloat16)).astype(jnp.float32)
    value_wide = values.astype(jnp.float32).reshape(token_count, KV_HEADS, HEAD)
    share = HEADS // KV_HEADS
    score_scale = HEAD ** (-0.5)
    query_blocks = query_heads.reshape(token_count // query_block, query_block, KV_HEADS, share, HEAD)

    def attend(block_queries):
        scores = jnp.einsum('qkgd,skd->kgqs', block_queries.astype(jnp.float32), key_wide) * score_scale
        row_max = lax.optimization_barrier(jnp.max(scores, axis=-1, keepdims=True))
        raised = jnp.exp(scores - row_max)
        row_total = lax.optimization_barrier(jnp.sum(raised, axis=-1))
        rounded = lax.optimization_barrier(raised.astype(jnp.bfloat16)).astype(jnp.float32)
        summed = jnp.einsum('kgqs,skd->qkgd', rounded, value_wide)
        return summed / jnp.transpose(row_total, (2, 0, 1))[..., None]
    attended = lax.map(attend, query_blocks).reshape(token_count, HEADS * HEAD).astype(jnp.bfloat16)
    update = jnp.dot(attended, out_weight, preferred_element_type=jnp.float32)
    updated = lax.optimization_barrier((residual.astype(jnp.float32) + update).astype(jnp.bfloat16))
    updated_wide = updated.astype(jnp.float32)
    normed = (updated_wide * lax.rsqrt(lax.optimization_barrier(jnp.mean(updated_wide * updated_wide, axis=1, keepdims=True)) + norm_eps) * norm_gain[None, :]).astype(jnp.bfloat16)
    mixing = group_prob[:, None] * jax.nn.softmax(expert_scores, axis=1)
    chosen_flat = route_experts.reshape(-1).astype(jnp.int32)
    owner = (jnp.arange(chosen_flat.shape[0], dtype=jnp.int32) // TOP).astype(jnp.int32)
    mixing_flat = mixing.reshape(-1)
    slot_limit = CAP * N_SP * N_TP
    block_count = EXPERT_HIDDEN // UNIT_BLOCK

    def one_expert(combined, inputs):
        gate_matrix, up_matrix, down_matrix, expert_id = inputs
        chosen = chosen_flat == expert_id
        ordinal = jnp.cumsum(chosen.astype(jnp.int32)) - 1
        target = jnp.where(chosen, ordinal, slot_limit).astype(jnp.int32)
        members = jnp.zeros((slot_limit,), jnp.int32).at[target].set(owner, mode='drop')
        member_weight = jnp.zeros((slot_limit,), jnp.float32).at[target].set(mixing_flat, mode='drop')
        picked = normed[members]
        gate_part = jnp.dot(picked, gate_matrix, preferred_element_type=jnp.float32)
        up_part = jnp.dot(picked, up_matrix, preferred_element_type=jnp.float32)
        hidden = lax.optimization_barrier((jax.nn.silu(gate_part) * up_part).astype(jnp.bfloat16))
        hidden_blocks = hidden.astype(jnp.float32).reshape(slot_limit, block_count, UNIT_BLOCK)
        down_blocks = down_matrix.astype(jnp.float32).reshape(block_count, UNIT_BLOCK, D)
        partial_value = jnp.einsum('rbh,bhd->rbd', hidden_blocks, down_blocks)
        rounded = lax.optimization_barrier(partial_value.astype(jnp.bfloat16)).astype(jnp.float32)
        expert_out = lax.optimization_barrier(lax.optimization_barrier(jnp.sum(rounded, axis=1)).astype(jnp.bfloat16))
        combined = combined.at[members].add(member_weight[:, None] * expert_out.astype(jnp.float32))
        return (combined, None)
    combined, unused = lax.scan(one_expert, jnp.zeros((token_count, D), jnp.float32), (w_gate, w_up, w_down, jnp.arange(EXPERTS, dtype=jnp.int32)))
    return (updated_wide + combined).astype(jnp.bfloat16)
```

```python
import functools
import math

import jax
import jax.numpy as jnp
from jax import lax
from jax.experimental import pallas as pl
from jax.experimental.pallas import tpu as pltpu
from jax.sharding import Mesh
from jax.sharding import PartitionSpec as P

GRID_W = 64
HEAD = 128
SP = "sp"
TP = ("z", "core")
SP_TP = ("sp", "z", "core")
rope_base = 10000.0
norm_eps = 1e-06
f32 = jnp.float32
bf16 = jnp.bfloat16


def dot(a, b):
    return jnp.dot(a, b, preferred_element_type=f32)


def prep_kernel(where_ref, q_ref, k_ref, v_ref, qg_ref, kg_ref, cos_ref, sin_ref, q_out, kv_out):
    lane = lax.broadcasted_iota(jnp.int32, (GRID_W, HEAD), 1)
    even = lane % 2 == 0
    from_row = lane < HEAD // 2
    col_cos = cos_ref[16:, :]
    col_sin = sin_ref[16:, :]

    def turn(vectors, gain, row_cos, row_sin):
        mean = jnp.mean(vectors * vectors, axis=-1, keepdims=True)
        u = vectors * lax.rsqrt(mean + norm_eps) * gain
        swapped = jnp.where(even, pltpu.roll(u, HEAD - 1, 1), pltpu.roll(u, 1, 1))
        cosine = jnp.where(from_row, row_cos, col_cos)
        sine = jnp.where(from_row, row_sin, col_sin)
        return u * cosine + swapped * sine

    for r in range(q_ref.shape[0] // GRID_W):
        rows = slice(r * GRID_W, (r + 1) * GRID_W)
        q_out[rows, :] = turn(
            q_ref[rows, :].astype(f32), qg_ref[...], cos_ref[r : r + 1, :], sin_ref[r : r + 1, :]
        ).astype(bf16)
    half = k_ref.shape[0] // GRID_W
    first = where_ref[0] * half
    for r in range(half):
        rows = slice(r * GRID_W, (r + 1) * GRID_W)
        row_cos = cos_ref[pl.ds(first + r, 1), :]
        row_sin = sin_ref[pl.ds(first + r, 1), :]
        kv_out[rows, :HEAD] = turn(
            k_ref[rows, :].astype(f32), kg_ref[...], row_cos, row_sin
        ).astype(bf16)
    kv_out[:, HEAD:] = v_ref[...]


def prep(where, queries, keys, values, query_gain, key_gain, cosine, sine):
    tokens = queries.shape[0]
    half = tokens // 2
    whole = lambda shape: pl.BlockSpec(shape, lambda i, w: (0, 0))
    part = pl.BlockSpec((half, HEAD), lambda i, w: (w[0], w[1]))
    return pl.pallas_call(
        prep_kernel,
        grid_spec=pltpu.PrefetchScalarGridSpec(
            num_scalar_prefetch=1,
            grid=(1,),
            in_specs=[
                whole((tokens, HEAD)),
                part,
                part,
                whole((1, HEAD)),
                whole((1, HEAD)),
                whole(cosine.shape),
                whole(sine.shape),
            ],
            out_specs=[whole((tokens, HEAD)), whole((half, 2 * HEAD))],
        ),
        out_shape=[
            jax.ShapeDtypeStruct((tokens, HEAD), bf16),
            jax.ShapeDtypeStruct((half, 2 * HEAD), bf16),
        ],
        name="prep",
    )(where, queries, keys, values, query_gain, key_gain, cosine, sine)


BQ = 256
CK = 1024


def attend_kernel(where_ref, own_ref, sib_ref, kv_ref, keep_ref, send_ref, kk, vv):
    blocks, rows, _ = kv_ref.shape

    @pl.when((pl.program_id(0) == 0) & (pl.program_id(1) == 0))
    def _():
        def fill(b, carry):
            span = pl.ds(pl.multiple_of(b * rows, rows), rows)
            k = kv_ref[b, :, :HEAD]
            kk[span, :HEAD] = k
            kk[span, HEAD:] = k
            vv[span, :HEAD] = kv_ref[b, :, HEAD:]
            vv[span, HEAD:] = jnp.ones((rows, HEAD), bf16)
            return carry

        lax.fori_loop(0, blocks, fill, 0)

    q = jnp.where(pl.program_id(0) == 0, own_ref[...].astype(f32), sib_ref[...].astype(f32))
    scaled = q * (HEAD ** (-0.5) * math.log2(math.e))
    high = scaled.astype(bf16)
    low = (scaled - high.astype(f32)).astype(bf16)
    pair = jnp.concatenate([high, low], axis=1)
    top = acc = None
    for j in range(blocks * rows // CK):
        span = slice(j * CK, (j + 1) * CK)
        s = lax.dot_general(
            pair, kk[span, :], (((1,), (1,)), ((), ())), preferred_element_type=f32
        )
        block_top = jnp.max(s, axis=1, keepdims=True)
        new_top = block_top if top is None else jnp.maximum(top, block_top)
        raised = jnp.exp2(s - new_top).astype(bf16)
        part = dot(raised, vv[span, :])
        acc = part if top is None else acc * jnp.exp2(top - new_top) + part
        top = new_top
    total = acc[:, HEAD:]
    normal = acc[:, :HEAD] / total
    level = top + jnp.log2(total)
    first_core = where_ref[0] == 0
    for z in range(BQ // 128):
        a = slice(z * 128, z * 128 + 64)
        b = slice(z * 128 + 64, z * 128 + 128)
        keep_ref[0, z, :, :HEAD] = jnp.where(first_core, normal[a], normal[b])
        keep_ref[0, z, :, HEAD:] = jnp.where(first_core, level[a], level[b])
        send_ref[0, z, :, :HEAD] = jnp.where(first_core, normal[b], normal[a])
        send_ref[0, z, :, HEAD:] = jnp.where(first_core, level[b], level[a])


def attend(where, own, sib, kv):
    tokens = own.shape[0]
    blocks, rows, _ = kv.shape
    q_spec = pl.BlockSpec((BQ, HEAD), lambda h, i, w: (i, 0))
    out_spec = pl.BlockSpec((1, BQ // 128, 64, 2 * HEAD), lambda h, i, w: (h, i, 0, 0))
    out = jax.ShapeDtypeStruct((2, tokens // 128, 64, 2 * HEAD), f32)
    return pl.pallas_call(
        attend_kernel,
        grid_spec=pltpu.PrefetchScalarGridSpec(
            num_scalar_prefetch=1,
            grid=(2, tokens // BQ),
            in_specs=[
                q_spec,
                q_spec,
                pl.BlockSpec((blocks, rows, 2 * HEAD), lambda h, i, w: (0, 0, 0)),
            ],
            out_specs=[out_spec, out_spec],
            scratch_shapes=[
                pltpu.VMEM((blocks * rows, 2 * HEAD), bf16),
                pltpu.VMEM((blocks * rows, 2 * HEAD), bf16),
            ],
        ),
        out_shape=[out, out],
        compiler_params=pltpu.CompilerParams(vmem_limit_bytes=48 * 1024 * 1024),
        name="attend",
    )(where, own, sib, kv)


def merge_kernel(where_ref, keep_ref, got_ref, out_ref):
    def merged(mine, other):
        level = jnp.maximum(mine[:, HEAD:], other[:, HEAD:])
        a = jnp.exp2(mine[:, HEAD:] - level)
        b = jnp.exp2(other[:, HEAD:] - level)
        return (mine[:, :HEAD] * a + other[:, :HEAD] * b) / (a + b)

    first_core = where_ref[0] == 0
    for z in range(keep_ref.shape[1]):
        own = merged(keep_ref[0, z], got_ref[1, z])
        sib = merged(keep_ref[1, z], got_ref[0, z])
        out_ref[z, :, :HEAD] = jnp.where(first_core, own, sib).astype(bf16)
        out_ref[z, :, HEAD:] = jnp.where(first_core, sib, own).astype(bf16)


def merge(where, keep, got):
    _, z, rows, _ = keep.shape
    return pl.pallas_call(
        merge_kernel,
        grid_spec=pltpu.PrefetchScalarGridSpec(
            num_scalar_prefetch=1,
            grid=(1,),
            in_specs=[pl.BlockSpec(keep.shape, lambda i, w: (0, 0, 0, 0))] * 2,
            out_specs=pl.BlockSpec((z, rows, 2 * HEAD), lambda i, w: (0, 0, 0)),
        ),
        out_shape=jax.ShapeDtypeStruct((z, rows, 2 * HEAD), bf16),
        name="merge",
    )(where, keep, got)


def swap_matrix(experts, blocks):
    count = experts * blocks * 2
    row = lax.broadcasted_iota(jnp.int32, (count, count), 0)
    col = lax.broadcasted_iota(jnp.int32, (count, count), 1)
    a, b, j = row // (blocks * 2), (row // 2) % blocks, row % 2
    return jnp.where(col == b * (experts * 2) + a * 2 + j, 1.0, 0.0).astype(bf16)


def pack(rows_of, out_ref):
    peers = out_ref.shape[0]
    blocks = 16
    tails = []
    for k in range(blocks):
        block = rows_of(k)
        head = block[: peers * 8].reshape(peers, 8, HEAD)
        out_ref[:, k * 8 : (k + 1) * 8, :] = head.astype(bf16)
        tails.append(block[peers * 8 :])
    tail = jnp.concatenate(tails, axis=0).astype(bf16)
    turned = dot(swap_matrix(peers, blocks), tail)
    out_ref[:, blocks * 8 :, :] = turned.reshape(peers, blocks * 2, HEAD).astype(bf16)


def unpack(in_ref, store):
    peers = in_ref.shape[0]
    blocks = 16
    tail = in_ref[:, blocks * 8 :, :].astype(f32).reshape(peers * blocks * 2, HEAD).astype(bf16)
    turned = dot(swap_matrix(blocks, peers), tail)
    for k in range(blocks):
        head = in_ref[:, k * 8 : (k + 1) * 8, :].astype(f32).reshape(peers * 8, HEAD)
        store(k, jnp.concatenate([head, turned[k * peers * 2 : (k + 1) * peers * 2]], axis=0))


def slot_of(expert, ordinal, experts):
    return jnp.where(ordinal < 8, expert * 8 + ordinal, experts * 8 + expert * 2 + ordinal - 8)


def project_kernel(a_ref, w_ref, res_ref, gain_ref, route_ref, route_t_ref, upd_ref, out_ref, acc):
    step = pl.program_id(0)
    part = dot(a_ref[0], w_ref[...])

    @pl.when(step == 0)
    def _():
        acc[...] = part

    @pl.when(step > 0)
    def _():
        acc[...] += part

    @pl.when(step == pl.num_programs(0) - 1)
    def _():
        updated = (res_ref[...].astype(f32) + acc[...]).astype(bf16)
        upd_ref[...] = updated
        wide = updated.astype(f32)
        mean = jnp.mean(wide * wide, axis=1, keepdims=True)
        normed = (wide * lax.rsqrt(mean + norm_eps) * gain_ref[...]).astype(bf16)
        rows = wide.shape[0]
        experts = out_ref.shape[0]
        earlier = lax.broadcasted_iota(jnp.int32, (rows, rows), 0)
        later = lax.broadcasted_iota(jnp.int32, (rows, rows), 1)
        slots = lax.broadcasted_iota(jnp.int32, (experts * 10, rows), 0)
        placing = jnp.zeros((experts * 10, rows), f32)
        for t in range(2):
            mine = route_t_ref[t : t + 1, :]
            ordinal = jnp.zeros((1, rows), jnp.int32)
            for u in range(2):
                before = (earlier < later) if u >= t else (earlier <= later)
                same = route_ref[:, u : u + 1] == mine
                ordinal += jnp.sum(jnp.where(before & same, 1, 0), axis=0, keepdims=True)
            placing += jnp.where(slots == slot_of(mine, ordinal, experts), 1.0, 0.0)
        sent = dot(placing.astype(bf16), normed)
        pack(lambda k: sent[:, k * HEAD : (k + 1) * HEAD], out_ref)


def project(attended, out_weight, residual, norm_gain, route, route_t, peers):
    steps, rows, depth = attended.shape
    width = out_weight.shape[1]
    whole = lambda a: pl.BlockSpec(a.shape, lambda i: (0,) * a.ndim)
    return pl.pallas_call(
        project_kernel,
        grid=(steps,),
        in_specs=[
            pl.BlockSpec((1, rows, depth), lambda i: (i, 0, 0)),
            pl.BlockSpec((depth, width), lambda i: (i, 0)),
            whole(residual),
            whole(norm_gain),
            whole(route),
            whole(route_t),
        ],
        out_specs=[
            pl.BlockSpec((rows, width), lambda i: (0, 0)),
            pl.BlockSpec((peers, 160, HEAD), lambda i: (0, 0, 0)),
        ],
        out_shape=[
            jax.ShapeDtypeStruct((rows, width), bf16),
            jax.ShapeDtypeStruct((peers, 160, HEAD), bf16),
        ],
        scratch_shapes=[pltpu.VMEM((rows, width), f32)],
        name="project",
    )(attended, out_weight, residual, norm_gain, route, route_t)


def hidden_kernel(in_ref, gate_ref, up_ref, hid_ref, x):
    @pl.when(pl.program_id(0) == 0)
    def _():
        def store(k, block):
            x[:, k * HEAD : (k + 1) * HEAD] = block.astype(bf16)

        unpack(in_ref, store)

    gate = dot(x[...], jnp.concatenate([gate_ref[0], gate_ref[1]], axis=1))
    up = dot(x[...], jnp.concatenate([up_ref[0], up_ref[1]], axis=1))
    hid_ref[...] = (gate / (1.0 + jnp.exp(-gate)) * up).astype(bf16)


def hidden(arrived, gate, up):
    blocks, width, units = gate.shape
    w_spec = pl.BlockSpec((2, width, units), lambda i: (i, 0, 0))
    return pl.pallas_call(
        hidden_kernel,
        grid=(blocks // 2,),
        in_specs=[pl.BlockSpec(arrived.shape, lambda i: (0, 0, 0)), w_spec, w_spec],
        out_specs=pl.BlockSpec((160, 2 * units), lambda i: (0, i)),
        out_shape=jax.ShapeDtypeStruct((160, blocks * units), bf16),
        scratch_shapes=[pltpu.VMEM((160, width), bf16)],
        name="hidden",
    )(arrived, gate, up)


def down_kernel(hid_ref, down_ref, out_ref, acc):
    step = pl.program_id(0)
    weights = jnp.concatenate([down_ref[0], down_ref[1]], axis=0)
    part = dot(hid_ref[...], weights)

    @pl.when(step == 0)
    def _():
        acc[...] = part

    @pl.when(step > 0)
    def _():
        acc[...] += part

    @pl.when(step == pl.num_programs(0) - 1)
    def _():
        pack(lambda k: acc[:, k * HEAD : (k + 1) * HEAD], out_ref)


def down(hid, weights, peers):
    blocks, units, width = weights.shape
    return pl.pallas_call(
        down_kernel,
        grid=(blocks // 2,),
        in_specs=[
            pl.BlockSpec((160, 2 * units), lambda i: (0, i)),
            pl.BlockSpec((2, units, width), lambda i: (i, 0, 0)),
        ],
        out_specs=pl.BlockSpec((peers, 160, HEAD), lambda i: (0, 0, 0)),
        out_shape=jax.ShapeDtypeStruct((peers, 160, HEAD), bf16),
        scratch_shapes=[pltpu.VMEM((160, width), f32)],
        name="down",
    )(hid, weights)


def mix_kernel(in_ref, upd_ref, route_ref, route_t_ref, score_ref, prob_ref, out_ref):
    rows = upd_ref.shape[0]
    experts = in_ref.shape[0]
    later = lax.broadcasted_iota(jnp.int32, (rows, rows), 0)
    earlier = lax.broadcasted_iota(jnp.int32, (rows, rows), 1)
    slots = lax.broadcasted_iota(jnp.int32, (rows, experts * 10), 1)
    picks = []
    for t in range(2):
        mine = route_ref[:, t : t + 1]
        ordinal = jnp.zeros((rows, 1), jnp.int32)
        for u in range(2):
            before = (earlier < later) if u >= t else (earlier <= later)
            same = route_t_ref[u : u + 1, :] == mine
            ordinal += jnp.sum(jnp.where(before & same, 1, 0), axis=1, keepdims=True)
        picks.append(jnp.where(slots == slot_of(mine, ordinal, experts), 1.0, 0.0).astype(bf16))
    scores = score_ref[...]
    raised = jnp.exp(scores - jnp.max(scores, axis=1, keepdims=True))
    mixing = prob_ref[...] * (raised / jnp.sum(raised, axis=1, keepdims=True))

    def store(k, block):
        block = block.astype(bf16)
        cols = slice(k * HEAD, (k + 1) * HEAD)
        combined = sum(dot(picks[t], block) * mixing[:, t : t + 1] for t in range(2))
        out_ref[:, cols] = (upd_ref[:, cols].astype(f32) + combined).astype(bf16)

    unpack(in_ref, store)


def mix(returned, updated, route, route_t, scores, prob):
    return pl.pallas_call(
        mix_kernel,
        out_shape=jax.ShapeDtypeStruct(updated.shape, bf16),
        name="mix",
    )(returned, updated, route, route_t, scores, prob)


def local(
    queries,
    keys,
    values,
    query_gain,
    key_gain,
    out_weight,
    residual,
    norm_gain,
    route_experts,
    expert_scores,
    group_prob,
    w_gate,
    w_up,
    w_down,
):
    peers = lax.axis_size(SP)
    core = lax.axis_index("core")
    z = lax.axis_index("z")
    seq = lax.axis_index(SP)
    tokens = queries.shape[0]

    gate = lax.all_gather(w_gate[0], TP)
    up = lax.all_gather(w_up[0], TP)
    down_weight = lax.all_gather(w_down[0], TP)

    where = jnp.stack([core, z // 2]).astype(jnp.int32)
    lane = jnp.arange(HEAD, dtype=jnp.int32)
    pair = (lane // 2) % (HEAD // 4)
    frequency = rope_base ** (-pair.astype(f32) * 4.0 / HEAD)
    grid_rows = tokens // GRID_W
    place = jnp.arange(grid_rows + GRID_W, dtype=jnp.int32)
    place = jnp.where(place < grid_rows, seq * grid_rows + place, place - grid_rows)
    angles = place.astype(f32)[:, None] * frequency[None, :]
    cosine = jnp.cos(angles)
    sine = jnp.sin(angles) * jnp.where(lane % 2 == 0, -1.0, 1.0)[None, :]

    own, kv = prep(
        where, queries, keys, values, query_gain[None, :], key_gain[None, :], cosine, sine
    )
    sib = lax.ppermute(own, "core", ((0, 1), (1, 0)))
    kv_all = lax.all_to_all(
        jnp.broadcast_to(kv[None], (peers, *kv.shape)), SP, 0, 0, tiled=True
    )
    keep, send = attend(where, own, sib, kv_all)
    got = lax.ppermute(send, "core", ((0, 1), (1, 0)))
    attended = lax.all_to_all(merge(where, keep, got), "z", 0, 0, tiled=True)
    route_t = route_experts.T
    updated, outgoing = project(
        attended, out_weight, residual, norm_gain[None, :], route_experts, route_t, peers
    )
    arrived = lax.all_to_all(outgoing, SP, 0, 0, tiled=True)
    hid = hidden(arrived, gate, up)
    result = down(hid, down_weight, peers)
    returned = lax.all_to_all(result, SP, 0, 0, tiled=True)
    return mix(
        returned, updated, route_experts, route_t, expert_scores, group_prob[:, None]
    )


def solution(mesh):
    torus = Mesh(mesh.devices.reshape(mesh.shape["sp"], 8, 2), ("sp", "z", "core"))
    placed = (
        P(SP, TP),
        P(SP, None),
        P(SP, None),
        P(TP),
        P(),
        P(),
        P(SP_TP, None),
        P(),
        P(SP_TP, None),
        P(SP_TP, None),
        P(SP_TP),
        P(SP, None, TP),
        P(SP, None, TP),
        P(SP, TP, None),
    )
    return jax.shard_map(
        local, mesh=torus, in_specs=placed, out_specs=P(SP_TP, None), check_vma=False
    )
```

```python
import functools
import math

import jax
import jax.numpy as jnp
from jax import lax
from jax.experimental import pallas as pl
from jax.experimental.pallas import tpu as pltpu
from jax.sharding import Mesh
from jax.sharding import PartitionSpec as P

GRID_W = 64
HEAD = 128
SP = ("y", "x")
TP = ("z", "core")
SP_TP = ("y", "x", "z", "core")
rope_base = 10000.0
norm_eps = 1e-06
f32 = jnp.float32
bf16 = jnp.bfloat16


def dot(a, b):
    return jnp.dot(a, b, preferred_element_type=f32)


def prep_kernel(
    where_ref,
    q_ref,
    k_ref,
    v_ref,
    qg_ref,
    kg_ref,
    cos_ref,
    sin_ref,
    gate_ref,
    up_ref,
    down_ref,
    q_out,
    kv_a,
    kv_b,
    w_out,
    sems,
):
    width = gate_ref.shape[0]
    units = gate_ref.shape[1]
    copies = [
        pltpu.make_async_copy(gate_ref, w_out.at[pl.ds(0, width)], sems.at[0]),
        pltpu.make_async_copy(up_ref, w_out.at[pl.ds(width, width)], sems.at[1]),
    ]
    for k in range(width // HEAD):
        copies.append(
            pltpu.make_async_copy(
                down_ref.at[:, pl.ds(k * HEAD, HEAD)],
                w_out.at[pl.ds(2 * width + k * units, units)],
                sems.at[2 + k],
            )
        )
    for copy in copies:
        copy.start()

    lane = lax.broadcasted_iota(jnp.int32, (GRID_W, HEAD), 1)
    even = lane % 2 == 0
    from_row = lane < HEAD // 2
    col_cos = cos_ref[16:, :]
    col_sin = sin_ref[16:, :]

    def turn(vectors, gain, row_cos, row_sin):
        mean = jnp.mean(vectors * vectors, axis=-1, keepdims=True)
        u = vectors * lax.rsqrt(mean + norm_eps) * gain
        swapped = jnp.where(even, pltpu.roll(u, HEAD - 1, 1), pltpu.roll(u, 1, 1))
        cosine = jnp.where(from_row, row_cos, col_cos)
        sine = jnp.where(from_row, row_sin, col_sin)
        return u * cosine + swapped * sine

    for r in range(q_ref.shape[0] // GRID_W):
        rows = slice(r * GRID_W, (r + 1) * GRID_W)
        q_out[rows, :] = turn(
            q_ref[rows, :].astype(f32), qg_ref[...], cos_ref[r : r + 1, :], sin_ref[r : r + 1, :]
        ).astype(bf16)
    half = k_ref.shape[0] // GRID_W
    first = where_ref[0] * half
    for r in range(half):
        rows = slice(r * GRID_W, (r + 1) * GRID_W)
        row_cos = cos_ref[pl.ds(first + r, 1), :]
        row_sin = sin_ref[pl.ds(first + r, 1), :]
        kv_out = kv_a if r < half // 2 else kv_b
        at = r % (half // 2)
        rows_out = slice(at * GRID_W, (at + 1) * GRID_W)
        kv_out[rows_out, :HEAD] = turn(
            k_ref[rows, :].astype(f32), kg_ref[...], row_cos, row_sin
        ).astype(bf16)
        kv_out[rows_out, HEAD:] = v_ref[rows, :]
    for copy in copies:
        copy.wait()


def prep(where, queries, keys, values, query_gain, key_gain, cosine, sine, gate, up, down):
    tokens = queries.shape[0]
    half = tokens // 2
    width, units = gate.shape
    whole = lambda shape: pl.BlockSpec(shape, lambda i, w: (0, 0))
    part = pl.BlockSpec((half, HEAD), lambda i, w: (w[0], w[1]))
    hbm = pl.BlockSpec(memory_space=pl.ANY)
    return pl.pallas_call(
        prep_kernel,
        grid_spec=pltpu.PrefetchScalarGridSpec(
            num_scalar_prefetch=1,
            grid=(1,),
            in_specs=[
                whole((tokens, HEAD)),
                part,
                part,
                whole((1, HEAD)),
                whole((1, HEAD)),
                whole(cosine.shape),
                whole(sine.shape),
                hbm,
                hbm,
                hbm,
            ],
            out_specs=[
                whole((tokens, HEAD)),
                whole((half // 2, 2 * HEAD)),
                whole((half // 2, 2 * HEAD)),
                hbm,
            ],
            scratch_shapes=[pltpu.SemaphoreType.DMA((2 + width // HEAD,))],
        ),
        out_shape=[
            jax.ShapeDtypeStruct((tokens, HEAD), bf16),
            jax.ShapeDtypeStruct((half // 2, 2 * HEAD), bf16),
            jax.ShapeDtypeStruct((half // 2, 2 * HEAD), bf16),
            jax.ShapeDtypeStruct((3 * width, units), bf16),
        ],
        name="prep",
    )(where, queries, keys, values, query_gain, key_gain, cosine, sine, gate, up, down)


BQ = 256


def attend_kernel(first, last, count, where_ref, own_ref, sib_ref, *refs):
    kv_refs, refs = refs[:count], refs[count:]
    if not first:
        acc_in, top_in, *refs = refs
    out_a, out_b, kk, vv = refs
    rows = kv_refs[0].shape[0]

    @pl.when((pl.program_id(0) == 0) & (pl.program_id(1) == 0))
    def _():
        for b in range(count):
            span = slice(b * rows, (b + 1) * rows)
            k = kv_refs[b][:, :HEAD]
            kk[span, :HEAD] = k
            kk[span, HEAD:] = k
            vv[span, :HEAD] = kv_refs[b][:, HEAD:]
            vv[span, HEAD:] = jnp.ones((rows, HEAD), bf16)

    q = jnp.where(pl.program_id(0) == 0, own_ref[...].astype(f32), sib_ref[...].astype(f32))
    scaled = q * (HEAD ** (-0.5) * math.log2(math.e))
    high = scaled.astype(bf16)
    low = (scaled - high.astype(f32)).astype(bf16)
    pair = jnp.concatenate([high, low], axis=1)
    top = None if first else jnp.max(top_in[0], axis=1, keepdims=True)
    acc = None if first else acc_in[0]
    for j in range(count):
        span = slice(j * rows, (j + 1) * rows)
        s = lax.dot_general(
            pair, kk[span, :], (((1,), (1,)), ((), ())), preferred_element_type=f32
        )
        block_top = jnp.max(s, axis=1, keepdims=True)
        new_top = block_top if top is None else jnp.maximum(top, block_top)
        raised = jnp.exp2(s - new_top).astype(bf16)
        part = dot(raised, vv[span, :])
        acc = part if top is None else acc * jnp.exp2(top - new_top) + part
        top = new_top
    if not last:
        out_a[0] = acc
        out_b[0] = jnp.broadcast_to(top, (top.shape[0], HEAD))
        return
    total = acc[:, HEAD:]
    normal = acc[:, :HEAD] / total
    level = top + jnp.log2(total)
    first_core = where_ref[0] == 0
    lane = lax.broadcasted_iota(jnp.int32, (64, HEAD), 1)
    for z in range(BQ // 128):
        a = slice(z * 128, z * 128 + 64)
        b = slice(z * 128 + 64, z * 128 + 128)
        out_a[0, z, :, :HEAD] = jnp.where(first_core, normal[a], normal[b])
        out_a[0, z, :, HEAD:] = jnp.where(first_core, level[a], level[b])
        out_b[0, z, :, :HEAD] = jnp.where(first_core, normal[b], normal[a]).astype(bf16)
        sent = jnp.where(first_core, level[b], level[a])
        l0 = sent.astype(bf16).astype(f32)
        l1 = (sent - l0).astype(bf16).astype(f32)
        l2 = sent - l0 - l1
        out_b[0, z, :, HEAD:] = jnp.where(lane < 32, l0, jnp.where(lane < 64, l1, l2)).astype(bf16)


def attend(where, own, sib, kvs, state, last):
    tokens = own.shape[0]
    rows = kvs[0].shape[0]
    first = state is None
    count = len(kvs)
    q_spec = pl.BlockSpec((BQ, HEAD), lambda h, i, w: (i, 0))
    kv_spec = pl.BlockSpec((rows, 2 * HEAD), lambda h, i, w: (0, 0))
    acc_spec = pl.BlockSpec((1, BQ, 2 * HEAD), lambda h, i, w: (h, i, 0))
    top_spec = pl.BlockSpec((1, BQ, HEAD), lambda h, i, w: (h, i, 0))
    if last:
        out_spec = pl.BlockSpec((1, BQ // 128, 64, 2 * HEAD), lambda h, i, w: (h, i, 0, 0))
        out_specs = [out_spec, out_spec]
        out_shape = [
            jax.ShapeDtypeStruct((2, tokens // 128, 64, 2 * HEAD), f32),
            jax.ShapeDtypeStruct((2, tokens // 128, 64, 2 * HEAD), bf16),
        ]
    else:
        out_specs = [acc_spec, top_spec]
        out_shape = [
            jax.ShapeDtypeStruct((2, tokens, 2 * HEAD), f32),
            jax.ShapeDtypeStruct((2, tokens, HEAD), f32),
        ]
    return pl.pallas_call(
        functools.partial(attend_kernel, first, last, count),
        grid_spec=pltpu.PrefetchScalarGridSpec(
            num_scalar_prefetch=1,
            grid=(2, tokens // BQ),
            in_specs=[q_spec, q_spec]
            + [kv_spec] * count
            + ([] if first else [acc_spec, top_spec]),
            out_specs=out_specs,
            scratch_shapes=[
                pltpu.VMEM((count * rows, 2 * HEAD), bf16),
                pltpu.VMEM((count * rows, 2 * HEAD), bf16),
            ],
        ),
        out_shape=out_shape,
        compiler_params=pltpu.CompilerParams(vmem_limit_bytes=32 * 1024 * 1024),
        name="attend",
    )(where, own, sib, *kvs, *([] if first else state))


def merge_kernel(where_ref, keep_ref, got_ref, out_ref):
    def merged(mine, other):
        other = other.astype(f32)
        theirs = other[:, HEAD : HEAD + 1] + other[:, HEAD + 32 : HEAD + 33]
        theirs = theirs + other[:, HEAD + 64 : HEAD + 65]
        level = jnp.maximum(mine[:, HEAD:], theirs)
        a = jnp.exp2(mine[:, HEAD:] - level)
        b = jnp.exp2(theirs - level)
        return (mine[:, :HEAD] * a + other[:, :HEAD] * b) / (a + b)

    first_core = where_ref[0] == 0
    for z in range(keep_ref.shape[1]):
        own = merged(keep_ref[0, z], got_ref[1, z])
        sib = merged(keep_ref[1, z], got_ref[0, z])
        out_ref[z, :, :HEAD] = jnp.where(first_core, own, sib).astype(bf16)
        out_ref[z, :, HEAD:] = jnp.where(first_core, sib, own).astype(bf16)


def merge(where, keep, got):
    _, z, rows, _ = keep.shape
    return pl.pallas_call(
        merge_kernel,
        grid_spec=pltpu.PrefetchScalarGridSpec(
            num_scalar_prefetch=1,
            grid=(1,),
            in_specs=[pl.BlockSpec(keep.shape, lambda i, w: (0, 0, 0, 0))] * 2,
            out_specs=pl.BlockSpec((z, rows, 2 * HEAD), lambda i, w: (0, 0, 0)),
        ),
        out_shape=jax.ShapeDtypeStruct((z, rows, 2 * HEAD), bf16),
        name="merge",
    )(where, keep, got)


def swap_matrix(experts, blocks):
    count = experts * blocks * 2
    row = lax.broadcasted_iota(jnp.int32, (count, count), 0)
    col = lax.broadcasted_iota(jnp.int32, (count, count), 1)
    a, b, j = row // (blocks * 2), (row // 2) % blocks, row % 2
    return jnp.where(col == b * (experts * 2) + a * 2 + j, 1.0, 0.0).astype(bf16)


def pack(rows_of, out_ref):
    peers = out_ref.shape[0]
    blocks = 16
    tails = []
    for k in range(blocks):
        block = rows_of(k)
        head = block[: peers * 8].reshape(peers, 8, HEAD)
        out_ref[:, k * 8 : (k + 1) * 8, :] = head.astype(bf16)
        tails.append(block[peers * 8 :])
    tail = jnp.concatenate(tails, axis=0).astype(bf16)
    turned = dot(swap_matrix(peers, blocks), tail)
    out_ref[:, blocks * 8 :, :] = turned.reshape(peers, blocks * 2, HEAD).astype(bf16)


def unpack(in_ref, store):
    peers = in_ref.shape[0]
    blocks = 16
    tail = in_ref[:, blocks * 8 :, :].astype(f32).reshape(peers * blocks * 2, HEAD).astype(bf16)
    turned = dot(swap_matrix(blocks, peers), tail)
    for k in range(blocks):
        head = in_ref[:, k * 8 : (k + 1) * 8, :].astype(f32).reshape(peers * 8, HEAD)
        store(k, jnp.concatenate([head, turned[k * peers * 2 : (k + 1) * peers * 2]], axis=0))


def slot_of(expert, ordinal, experts):
    return jnp.where(ordinal < 8, expert * 8 + ordinal, experts * 8 + expert * 2 + ordinal - 8)


def project_kernel(
    a_ref, w_ref, res_ref, gain_ref, route_ref, route_t_ref, upd_ref, out_ref, held, sems
):
    steps, rows, depth = a_ref.shape
    copies = [
        pltpu.make_async_copy(
            w_ref.at[pl.ds(i * depth, depth)], held.at[pl.ds(i * depth, depth)], sems.at[i]
        )
        for i in range(steps)
    ]
    for copy in copies:
        copy.start()
    experts = out_ref.shape[0]
    earlier = lax.broadcasted_iota(jnp.int32, (rows, rows), 0)
    later = lax.broadcasted_iota(jnp.int32, (rows, rows), 1)
    slots = lax.broadcasted_iota(jnp.int32, (experts * 10, rows), 0)
    placing = jnp.zeros((experts * 10, rows), f32)
    for t in range(2):
        mine = route_t_ref[t : t + 1, :]
        ordinal = jnp.zeros((1, rows), jnp.int32)
        for u in range(2):
            before = (earlier < later) if u >= t else (earlier <= later)
            same = route_ref[:, u : u + 1] == mine
            ordinal += jnp.sum(jnp.where(before & same, 1, 0), axis=0, keepdims=True)
        placing += jnp.where(slots == slot_of(mine, ordinal, experts), 1.0, 0.0)
    acc = res_ref[...].astype(f32)
    for i in range(steps):
        copies[i].wait()
        acc += dot(a_ref[i], held[i * depth : (i + 1) * depth, :])
    updated = acc.astype(bf16)
    upd_ref[...] = updated
    wide = updated.astype(f32)
    mean = jnp.mean(wide * wide, axis=1, keepdims=True)
    normed = (wide * lax.rsqrt(mean + norm_eps) * gain_ref[...]).astype(bf16)
    sent = dot(placing.astype(bf16), normed)
    pack(lambda k: sent[:, k * HEAD : (k + 1) * HEAD], out_ref)


VMEM = pl.BlockSpec(memory_space=pltpu.VMEM)
HBM = pl.BlockSpec(memory_space=pl.ANY)
ROOM = pltpu.CompilerParams(vmem_limit_bytes=48 * 1024 * 1024)


def project(attended, out_weight, residual, norm_gain, route, route_t, peers):
    steps, rows, depth = attended.shape
    width = out_weight.shape[1]
    return pl.pallas_call(
        project_kernel,
        in_specs=[VMEM, HBM, VMEM, VMEM, VMEM, VMEM],
        out_specs=[VMEM, VMEM],
        out_shape=[
            jax.ShapeDtypeStruct((rows, width), bf16),
            jax.ShapeDtypeStruct((peers, 160, HEAD), bf16),
        ],
        scratch_shapes=[
            pltpu.VMEM(out_weight.shape, bf16),
            pltpu.SemaphoreType.DMA((steps,)),
        ],
        compiler_params=ROOM,
        name="project",
    )(attended, out_weight, residual, norm_gain, route, route_t)


def expert_kernel(own_ref, sib_ref, *refs):
    pieces, refs = refs[:9], refs[9:]
    keep_ref, send_ref, held, x, sems = refs
    rows = keep_ref.shape[0]
    width = x.shape[1]
    whole = held.shape[1]
    copies = [pltpu.make_async_copy(pieces[i], held.at[i], sems.at[i]) for i in range(7)]
    for i in range(2):
        span = pl.ds(i * (whole // 2), whole // 2)
        copies.append(pltpu.make_async_copy(pieces[7 + i], held.at[7, span], sems.at[7 + i]))
    for copy in copies:
        copy.start()
    for half, ref in enumerate((own_ref, sib_ref)):

        def store(k, block):
            x[half * rows : (half + 1) * rows, k * HEAD : (k + 1) * HEAD] = block.astype(bf16)

        unpack(ref, store)
    total = None
    for i in range(4):
        pair = (2 * i, 2 * i + 1)
        for j in pair:
            copies[j].wait()
        if i == 3:
            copies[8].wait()
        side = lambda at: jnp.concatenate([held[j, at : at + width, :] for j in pair], axis=1)
        gate = dot(x[...], side(0))
        up = dot(x[...], side(width))
        hid = (gate / (1.0 + jnp.exp(-gate)) * up).astype(bf16)
        down = jnp.concatenate(
            [
                jnp.concatenate(
                    [held[j, 2 * width + k * HEAD : 2 * width + (k + 1) * HEAD, :] for j in pair],
                    axis=0,
                )
                for k in range(width // HEAD)
            ],
            axis=1,
        )
        part = dot(hid, down)
        total = part if total is None else total + part
    keep_ref[...] = total[:rows]
    send_ref[...] = total[rows:].astype(bf16)


def expert(own, sib, pieces):
    width = 2048
    return pl.pallas_call(
        expert_kernel,
        in_specs=[VMEM, VMEM] + [HBM] * 9,
        out_specs=[VMEM, VMEM],
        out_shape=[
            jax.ShapeDtypeStruct((160, width), f32),
            jax.ShapeDtypeStruct((160, width), bf16),
        ],
        scratch_shapes=[
            pltpu.VMEM((8, *pieces[0].shape), bf16),
            pltpu.VMEM((320, width), bf16),
            pltpu.SemaphoreType.DMA((9,)),
        ],
        compiler_params=ROOM,
        name="expert",
    )(own, sib, *pieces)


def finish_kernel(keep_ref, got_ref, out_ref):
    def rows_of(k):
        cols = slice(k * HEAD, (k + 1) * HEAD)
        return keep_ref[:, cols] + got_ref[:, cols].astype(f32)

    pack(rows_of, out_ref)


def finish(keep, got, peers):
    return pl.pallas_call(
        finish_kernel,
        out_shape=jax.ShapeDtypeStruct((peers, 160, HEAD), bf16),
        name="finish",
    )(keep, got)


def mix_kernel(in_ref, upd_ref, route_ref, route_t_ref, score_ref, prob_ref, out_ref):
    rows = upd_ref.shape[0]
    experts = in_ref.shape[0]
    later = lax.broadcasted_iota(jnp.int32, (rows, rows), 0)
    earlier = lax.broadcasted_iota(jnp.int32, (rows, rows), 1)
    slots = lax.broadcasted_iota(jnp.int32, (rows, experts * 10), 1)
    picks = []
    for t in range(2):
        mine = route_ref[:, t : t + 1]
        ordinal = jnp.zeros((rows, 1), jnp.int32)
        for u in range(2):
            before = (earlier < later) if u >= t else (earlier <= later)
            same = route_t_ref[u : u + 1, :] == mine
            ordinal += jnp.sum(jnp.where(before & same, 1, 0), axis=1, keepdims=True)
        picks.append(jnp.where(slots == slot_of(mine, ordinal, experts), 1.0, 0.0).astype(bf16))
    scores = score_ref[...]
    raised = jnp.exp(scores - jnp.max(scores, axis=1, keepdims=True))
    mixing = prob_ref[...] * (raised / jnp.sum(raised, axis=1, keepdims=True))

    def store(k, block):
        block = block.astype(bf16)
        cols = slice(k * HEAD, (k + 1) * HEAD)
        combined = sum(dot(picks[t], block) * mixing[:, t : t + 1] for t in range(2))
        out_ref[:, cols] = (upd_ref[:, cols].astype(f32) + combined).astype(bf16)

    unpack(in_ref, store)


def mix(returned, updated, route, route_t, scores, prob):
    return pl.pallas_call(
        mix_kernel,
        out_shape=jax.ShapeDtypeStruct(updated.shape, bf16),
        name="mix",
    )(returned, updated, route, route_t, scores, prob)


def shift(value, axis, by):
    size = lax.axis_size(axis)
    return lax.ppermute(value, axis, [(i, (i + by) % size) for i in range(size)])


def onward(value, axis):
    size = lax.axis_size(axis)
    pairs = []
    for i in range(size):
        pairs.append((2 * i, 2 * ((i + 1) % size)))
        pairs.append((2 * i + 1, 2 * ((i - 1) % size) + 1))
    return lax.ppermute(value, (axis, "core"), pairs)


def swap_cores(value):
    return lax.ppermute(value, "core", ((0, 1), (1, 0)))


def local(
    queries,
    keys,
    values,
    query_gain,
    key_gain,
    out_weight,
    residual,
    norm_gain,
    route_experts,
    expert_scores,
    group_prob,
    w_gate,
    w_up,
    w_down,
):
    peers = lax.axis_size(SP)
    core = lax.axis_index("core")
    z = lax.axis_index("z")
    seq = lax.axis_index(SP)
    tokens = queries.shape[0]

    where = jnp.stack([core, z // 2]).astype(jnp.int32)
    lane = jnp.arange(HEAD, dtype=jnp.int32)
    pair = (lane // 2) % (HEAD // 4)
    frequency = rope_base ** (-pair.astype(f32) * 4.0 / HEAD)
    grid_rows = tokens // GRID_W
    place = jnp.arange(grid_rows + GRID_W, dtype=jnp.int32)
    place = jnp.where(place < grid_rows, seq * grid_rows + place, place - grid_rows)
    angles = place.astype(f32)[:, None] * frequency[None, :]
    cosine = jnp.cos(angles)
    sine = jnp.sin(angles) * jnp.where(lane % 2 == 0, -1.0, 1.0)[None, :]

    own, kv_a, kv_b, w0 = prep(
        where,
        queries,
        keys,
        values,
        query_gain[None, :],
        key_gain[None, :],
        cosine,
        sine,
        w_gate[0],
        w_up[0],
        w_down[0],
    )
    ax = jnp.concatenate([kv_a] + [shift(kv_a, "x", d) for d in (1, -1, 2)], axis=0)
    by = jnp.concatenate([kv_b] + [shift(kv_b, "y", d) for d in (1, -1, 2)], axis=0)
    w1p, w1m = shift(w0, "z", 1), shift(w0, "z", -1)
    sib = swap_cores(own)
    a_next = [shift(ax, "y", 1), shift(ax, "y", -1)]
    b_next = [shift(by, "x", 1), shift(by, "x", -1)]
    state = attend(where, own, sib, [ax, by], None, False)
    w1p, w1m, state, a_next, b_next = lax.optimization_barrier((w1p, w1m, state, a_next, b_next))
    w2p, w2m = shift(w1p, "z", 1), shift(w1m, "z", -1)
    a_far = onward(jnp.where(core == 0, a_next[0], a_next[1]), "y")
    b_far = onward(jnp.where(core == 0, b_next[0], b_next[1]), "x")
    state = attend(where, own, sib, a_next + b_next, state, False)
    keep, send = attend(where, own, sib, [a_far, b_far], state, True)
    merged = merge(where, keep, swap_cores(send))
    w2p, w2m, merged = lax.optimization_barrier((w2p, w2m, merged))
    w3p, w3m = shift(w2p, "z", 1), shift(w2m, "z", -1)
    attended = lax.all_to_all(merged, "z", 0, 0, tiled=True)
    route_t = route_experts.T
    updated, outgoing = project(
        attended, out_weight, residual, norm_gain[None, :], route_experts, route_t, peers
    )
    arrived = lax.all_to_all(outgoing, SP, 0, 0, tiled=True)
    w3p, w3m, arrived = lax.optimization_barrier((w3p, w3m, arrived))
    middle = w0.shape[0] // 2
    w4 = [shift(w3p[:middle], "z", 1), shift(w3m[middle:], "z", -1)]
    pieces = [w0, w1p, w1m, w2p, w2m, w3p, w3m, *w4]
    kept, sent = expert(arrived, swap_cores(arrived), pieces)
    returned = lax.all_to_all(finish(kept, swap_cores(sent), peers), SP, 0, 0, tiled=True)
    return mix(
        returned, updated, route_experts, route_t, expert_scores, group_prob[:, None]
    )


def solution(mesh):
    torus = Mesh(mesh.devices.reshape(4, 4, 8, 2), ("y", "x", "z", "core"))
    placed = (
        P(SP, TP),
        P(SP, None),
        P(SP, None),
        P(TP),
        P(),
        P(),
        P(SP_TP, None),
        P(),
        P(SP_TP, None),
        P(SP_TP, None),
        P(SP_TP),
        P(SP, None, TP),
        P(SP, None, TP),
        P(SP, TP, None),
    )
    return jax.shard_map(
        local, mesh=torus, in_specs=placed, out_specs=P(SP_TP, None), check_vma=False
    )
```

```python
import functools
import math

import jax
import jax.numpy as jnp
from jax import lax
from jax.experimental import pallas as pl
from jax.experimental.pallas import tpu as pltpu
from jax.sharding import Mesh
from jax.sharding import PartitionSpec as P

GRID_W = 64
HEAD = 128
SP = ("y", "x")
TP = ("z", "core")
SP_TP = ("y", "x", "z", "core")
rope_base = 10000.0
norm_eps = 1e-06
f32 = jnp.float32
bf16 = jnp.bfloat16


def dot(a, b):
    return jnp.dot(a, b, preferred_element_type=f32)


def bundle_kernel(gate_ref, up_ref, down_ref, out_ref):
    units = gate_ref.shape[1]
    out_ref[0] = gate_ref[...]
    out_ref[1] = up_ref[...]
    for k in range(down_ref.shape[1] // HEAD):
        out_ref[2, k * units : (k + 1) * units, :] = down_ref[:, k * HEAD : (k + 1) * HEAD]


def bundle(gate, up, down):
    width, units = gate.shape
    rows = width // 2
    spec = pl.BlockSpec((rows, units), lambda i: (i, 0))
    return pl.pallas_call(
        bundle_kernel,
        grid=(2,),
        in_specs=[spec, spec, pl.BlockSpec((units, rows), lambda i: (0, i))],
        out_specs=pl.BlockSpec((3, rows, units), lambda i: (0, i, 0)),
        out_shape=jax.ShapeDtypeStruct((3, width, units), bf16),
        name="bundle",
    )(gate, up, down)


def prep_kernel(
    where_ref, q_ref, k_ref, v_ref, qg_ref, kg_ref, cos_ref, sin_ref, q_out, kv_a, kv_b
):
    lane = lax.broadcasted_iota(jnp.int32, (GRID_W, HEAD), 1)
    even = lane % 2 == 0
    from_row = lane < HEAD // 2
    col_cos = cos_ref[16:, :]
    col_sin = sin_ref[16:, :]

    def turn(vectors, gain, row_cos, row_sin):
        mean = jnp.mean(vectors * vectors, axis=-1, keepdims=True)
        u = vectors * lax.rsqrt(mean + norm_eps) * gain
        swapped = jnp.where(even, pltpu.roll(u, HEAD - 1, 1), pltpu.roll(u, 1, 1))
        cosine = jnp.where(from_row, row_cos, col_cos)
        sine = jnp.where(from_row, row_sin, col_sin)
        return u * cosine + swapped * sine

    for r in range(q_ref.shape[0] // GRID_W):
        rows = slice(r * GRID_W, (r + 1) * GRID_W)
        q_out[rows, :] = turn(
            q_ref[rows, :].astype(f32), qg_ref[...], cos_ref[r : r + 1, :], sin_ref[r : r + 1, :]
        ).astype(bf16)
    half = k_ref.shape[0] // GRID_W
    first = where_ref[0] * half
    for r in range(half):
        rows = slice(r * GRID_W, (r + 1) * GRID_W)
        row_cos = cos_ref[pl.ds(first + r, 1), :]
        row_sin = sin_ref[pl.ds(first + r, 1), :]
        kv_out = kv_a if r < half // 2 else kv_b
        at = r % (half // 2)
        rows_out = slice(at * GRID_W, (at + 1) * GRID_W)
        kv_out[rows_out, :HEAD] = turn(
            k_ref[rows, :].astype(f32), kg_ref[...], row_cos, row_sin
        ).astype(bf16)
        kv_out[rows_out, HEAD:] = v_ref[rows, :]


def prep(where, queries, keys, values, query_gain, key_gain, cosine, sine):
    tokens = queries.shape[0]
    half = tokens // 2
    whole = lambda shape: pl.BlockSpec(shape, lambda i, w: (0, 0))
    part = pl.BlockSpec((half, HEAD), lambda i, w: (w[0], w[1]))
    return pl.pallas_call(
        prep_kernel,
        grid_spec=pltpu.PrefetchScalarGridSpec(
            num_scalar_prefetch=1,
            grid=(1,),
            in_specs=[
                whole((tokens, HEAD)),
                part,
                part,
                whole((1, HEAD)),
                whole((1, HEAD)),
                whole(cosine.shape),
                whole(sine.shape),
            ],
            out_specs=[
                whole((tokens, HEAD)),
                whole((half // 2, 2 * HEAD)),
                whole((half // 2, 2 * HEAD)),
            ],
        ),
        out_shape=[
            jax.ShapeDtypeStruct((tokens, HEAD), bf16),
            jax.ShapeDtypeStruct((half // 2, 2 * HEAD), bf16),
            jax.ShapeDtypeStruct((half // 2, 2 * HEAD), bf16),
        ],
        name="prep",
    )(where, queries, keys, values, query_gain, key_gain, cosine, sine)


BQ = 256


def attend_kernel(first, last, count, where_ref, own_ref, sib_ref, *refs):
    kv_refs, refs = refs[:count], refs[count:]
    if not first:
        acc_in, top_in, *refs = refs
    out_a, out_b, kk, vv = refs
    rows = kv_refs[0].shape[0]

    @pl.when((pl.program_id(0) == 0) & (pl.program_id(1) == 0))
    def _():
        for b in range(count):
            span = slice(b * rows, (b + 1) * rows)
            k = kv_refs[b][:, :HEAD]
            kk[span, :HEAD] = k
            kk[span, HEAD:] = k
            vv[span, :HEAD] = kv_refs[b][:, HEAD:]
            vv[span, HEAD:] = jnp.ones((rows, HEAD), bf16)

    q = jnp.where(pl.program_id(0) == 0, own_ref[...].astype(f32), sib_ref[...].astype(f32))
    scaled = q * (HEAD ** (-0.5) * math.log2(math.e))
    high = scaled.astype(bf16)
    low = (scaled - high.astype(f32)).astype(bf16)
    pair = jnp.concatenate([high, low], axis=1)
    top = None if first else jnp.max(top_in[0], axis=1, keepdims=True)
    acc = None if first else acc_in[0]
    for j in range(count):
        span = slice(j * rows, (j + 1) * rows)
        s = lax.dot_general(
            pair, kk[span, :], (((1,), (1,)), ((), ())), preferred_element_type=f32
        )
        block_top = jnp.max(s, axis=1, keepdims=True)
        new_top = block_top if top is None else jnp.maximum(top, block_top)
        raised = jnp.exp2(s - new_top).astype(bf16)
        part = dot(raised, vv[span, :])
        acc = part if top is None else acc * jnp.exp2(top - new_top) + part
        top = new_top
    if not last:
        out_a[0] = acc
        out_b[0] = jnp.broadcast_to(top, (top.shape[0], HEAD))
        return
    total = acc[:, HEAD:]
    normal = acc[:, :HEAD] / total
    level = top + jnp.log2(total)
    first_core = where_ref[0] == 0
    lane = lax.broadcasted_iota(jnp.int32, (64, HEAD), 1)
    for z in range(BQ // 128):
        a = slice(z * 128, z * 128 + 64)
        b = slice(z * 128 + 64, z * 128 + 128)
        out_a[0, z, :, :HEAD] = jnp.where(first_core, normal[a], normal[b])
        out_a[0, z, :, HEAD:] = jnp.where(first_core, level[a], level[b])
        out_b[0, z, :, :HEAD] = jnp.where(first_core, normal[b], normal[a]).astype(bf16)
        sent = jnp.where(first_core, level[b], level[a])
        l0 = sent.astype(bf16).astype(f32)
        l1 = (sent - l0).astype(bf16).astype(f32)
        l2 = sent - l0 - l1
        out_b[0, z, :, HEAD:] = jnp.where(lane < 32, l0, jnp.where(lane < 64, l1, l2)).astype(bf16)


def attend(where, own, sib, kvs, state, last):
    tokens = own.shape[0]
    rows = kvs[0].shape[0]
    first = state is None
    count = len(kvs)
    q_spec = pl.BlockSpec((BQ, HEAD), lambda h, i, w: (i, 0))
    kv_spec = pl.BlockSpec((rows, 2 * HEAD), lambda h, i, w: (0, 0))
    acc_spec = pl.BlockSpec((1, BQ, 2 * HEAD), lambda h, i, w: (h, i, 0))
    top_spec = pl.BlockSpec((1, BQ, HEAD), lambda h, i, w: (h, i, 0))
    if last:
        out_spec = pl.BlockSpec((1, BQ // 128, 64, 2 * HEAD), lambda h, i, w: (h, i, 0, 0))
        out_specs = [out_spec, out_spec]
        out_shape = [
            jax.ShapeDtypeStruct((2, tokens // 128, 64, 2 * HEAD), f32),
            jax.ShapeDtypeStruct((2, tokens // 128, 64, 2 * HEAD), bf16),
        ]
    else:
        out_specs = [acc_spec, top_spec]
        out_shape = [
            jax.ShapeDtypeStruct((2, tokens, 2 * HEAD), f32),
            jax.ShapeDtypeStruct((2, tokens, HEAD), f32),
        ]
    return pl.pallas_call(
        functools.partial(attend_kernel, first, last, count),
        grid_spec=pltpu.PrefetchScalarGridSpec(
            num_scalar_prefetch=1,
            grid=(2, tokens // BQ),
            in_specs=[q_spec, q_spec]
            + [kv_spec] * count
            + ([] if first else [acc_spec, top_spec]),
            out_specs=out_specs,
            scratch_shapes=[
                pltpu.VMEM((count * rows, 2 * HEAD), bf16),
                pltpu.VMEM((count * rows, 2 * HEAD), bf16),
            ],
        ),
        out_shape=out_shape,
        compiler_params=pltpu.CompilerParams(vmem_limit_bytes=32 * 1024 * 1024),
        name="attend",
    )(where, own, sib, *kvs, *([] if first else state))


def merge_kernel(where_ref, keep_ref, got_ref, out_ref):
    def merged(mine, other):
        other = other.astype(f32)
        theirs = other[:, HEAD : HEAD + 1] + other[:, HEAD + 32 : HEAD + 33]
        theirs = theirs + other[:, HEAD + 64 : HEAD + 65]
        level = jnp.maximum(mine[:, HEAD:], theirs)
        a = jnp.exp2(mine[:, HEAD:] - level)
        b = jnp.exp2(theirs - level)
        return (mine[:, :HEAD] * a + other[:, :HEAD] * b) / (a + b)

    first_core = where_ref[0] == 0
    for z in range(keep_ref.shape[1]):
        own = merged(keep_ref[0, z], got_ref[1, z])
        sib = merged(keep_ref[1, z], got_ref[0, z])
        out_ref[z, :, :HEAD] = jnp.where(first_core, own, sib).astype(bf16)
        out_ref[z, :, HEAD:] = jnp.where(first_core, sib, own).astype(bf16)


def merge(where, keep, got):
    _, z, rows, _ = keep.shape
    return pl.pallas_call(
        merge_kernel,
        grid_spec=pltpu.PrefetchScalarGridSpec(
            num_scalar_prefetch=1,
            grid=(1,),
            in_specs=[pl.BlockSpec(keep.shape, lambda i, w: (0, 0, 0, 0))] * 2,
            out_specs=pl.BlockSpec((z, rows, 2 * HEAD), lambda i, w: (0, 0, 0)),
        ),
        out_shape=jax.ShapeDtypeStruct((z, rows, 2 * HEAD), bf16),
        name="merge",
    )(where, keep, got)


def swap_matrix(experts, blocks):
    count = experts * blocks * 2
    row = lax.broadcasted_iota(jnp.int32, (count, count), 0)
    col = lax.broadcasted_iota(jnp.int32, (count, count), 1)
    a, b, j = row // (blocks * 2), (row // 2) % blocks, row % 2
    return jnp.where(col == b * (experts * 2) + a * 2 + j, 1.0, 0.0).astype(bf16)


def pack(rows_of, out_ref):
    peers = out_ref.shape[0]
    blocks = 16
    tails = []
    for k in range(blocks):
        block = rows_of(k)
        head = block[: peers * 8].reshape(peers, 8, HEAD)
        out_ref[:, k * 8 : (k + 1) * 8, :] = head.astype(bf16)
        tails.append(block[peers * 8 :])
    tail = jnp.concatenate(tails, axis=0).astype(bf16)
    turned = dot(swap_matrix(peers, blocks), tail)
    out_ref[:, blocks * 8 :, :] = turned.reshape(peers, blocks * 2, HEAD).astype(bf16)


def unpack(in_ref, store):
    peers = in_ref.shape[0]
    blocks = 16
    tail = in_ref[:, blocks * 8 :, :].astype(f32).reshape(peers * blocks * 2, HEAD).astype(bf16)
    turned = dot(swap_matrix(blocks, peers), tail)
    for k in range(blocks):
        head = in_ref[:, k * 8 : (k + 1) * 8, :].astype(f32).reshape(peers * 8, HEAD)
        store(k, jnp.concatenate([head, turned[k * peers * 2 : (k + 1) * peers * 2]], axis=0))


def slot_of(expert, ordinal, experts):
    return jnp.where(ordinal < 8, expert * 8 + ordinal, experts * 8 + expert * 2 + ordinal - 8)


def project_kernel(
    a_ref, w_ref, res_ref, gain_ref, route_ref, route_t_ref, upd_ref, out_ref, held, sems
):
    steps, rows, depth = a_ref.shape
    copies = [
        pltpu.make_async_copy(
            w_ref.at[pl.ds(i * depth, depth)], held.at[pl.ds(i * depth, depth)], sems.at[i]
        )
        for i in range(steps)
    ]
    for copy in copies:
        copy.start()
    experts = out_ref.shape[0]
    earlier = lax.broadcasted_iota(jnp.int32, (rows, rows), 0)
    later = lax.broadcasted_iota(jnp.int32, (rows, rows), 1)
    slots = lax.broadcasted_iota(jnp.int32, (experts * 10, rows), 0)
    placing = jnp.zeros((experts * 10, rows), f32)
    for t in range(2):
        mine = route_t_ref[t : t + 1, :]
        ordinal = jnp.zeros((1, rows), jnp.int32)
        for u in range(2):
            before = (earlier < later) if u >= t else (earlier <= later)
            same = route_ref[:, u : u + 1] == mine
            ordinal += jnp.sum(jnp.where(before & same, 1, 0), axis=0, keepdims=True)
        placing += jnp.where(slots == slot_of(mine, ordinal, experts), 1.0, 0.0)
    acc = res_ref[...].astype(f32)
    for i in range(steps):
        copies[i].wait()
        acc += dot(a_ref[i], held[i * depth : (i + 1) * depth, :])
    updated = acc.astype(bf16)
    upd_ref[...] = updated
    wide = updated.astype(f32)
    mean = jnp.mean(wide * wide, axis=1, keepdims=True)
    normed = (wide * lax.rsqrt(mean + norm_eps) * gain_ref[...]).astype(bf16)
    sent = dot(placing.astype(bf16), normed)
    pack(lambda k: sent[:, k * HEAD : (k + 1) * HEAD], out_ref)


VMEM = pl.BlockSpec(memory_space=pltpu.VMEM)
HBM = pl.BlockSpec(memory_space=pl.ANY)
ROOM = pltpu.CompilerParams(vmem_limit_bytes=48 * 1024 * 1024)


def project(attended, out_weight, residual, norm_gain, route, route_t, peers):
    steps, rows, depth = attended.shape
    width = out_weight.shape[1]
    return pl.pallas_call(
        project_kernel,
        in_specs=[VMEM, HBM, VMEM, VMEM, VMEM, VMEM],
        out_specs=[VMEM, VMEM],
        out_shape=[
            jax.ShapeDtypeStruct((rows, width), bf16),
            jax.ShapeDtypeStruct((peers, 160, HEAD), bf16),
        ],
        scratch_shapes=[
            pltpu.VMEM(out_weight.shape, bf16),
            pltpu.SemaphoreType.DMA((steps,)),
        ],
        compiler_params=ROOM,
        name="project",
    )(attended, out_weight, residual, norm_gain, route, route_t)


def expert_kernel(in_ref, w_ref, out_ref, held, x, acc, sems):
    blocks, _, width, _ = held.shape
    copies = [pltpu.make_async_copy(w_ref.at[i], held.at[i], sems.at[i]) for i in range(blocks)]
    for copy in copies:
        copy.start()

    def store(k, block):
        x[:, k * HEAD : (k + 1) * HEAD] = block.astype(bf16)

    unpack(in_ref, store)
    for i in range(0, blocks, 2):
        pair = (i, i + 1)
        for j in pair:
            copies[j].wait()
        gate = dot(x[...], jnp.concatenate([held[j, 0] for j in pair], axis=1))
        up = dot(x[...], jnp.concatenate([held[j, 1] for j in pair], axis=1))
        hid = (gate / (1.0 + jnp.exp(-gate)) * up).astype(bf16)
        down = jnp.concatenate(
            [
                jnp.concatenate(
                    [held[j, 2, k * HEAD : (k + 1) * HEAD, :] for j in pair], axis=0
                )
                for k in range(width // HEAD)
            ],
            axis=1,
        )
        part = dot(hid, down)
        if i == 0:
            acc[...] = part
        else:
            acc[...] += part
    pack(lambda k: acc[:, k * HEAD : (k + 1) * HEAD], out_ref)


def expert(arrived, weights):
    blocks, _, width, _ = weights.shape
    return pl.pallas_call(
        expert_kernel,
        in_specs=[VMEM, HBM],
        out_specs=VMEM,
        out_shape=jax.ShapeDtypeStruct(arrived.shape, bf16),
        scratch_shapes=[
            pltpu.VMEM(weights.shape, bf16),
            pltpu.VMEM((160, width), bf16),
            pltpu.VMEM((160, width), f32),
            pltpu.SemaphoreType.DMA((blocks,)),
        ],
        compiler_params=ROOM,
        name="expert",
    )(arrived, weights)


def mix_kernel(in_ref, upd_ref, route_ref, route_t_ref, score_ref, prob_ref, out_ref):
    rows = upd_ref.shape[0]
    experts = in_ref.shape[0]
    later = lax.broadcasted_iota(jnp.int32, (rows, rows), 0)
    earlier = lax.broadcasted_iota(jnp.int32, (rows, rows), 1)
    slots = lax.broadcasted_iota(jnp.int32, (rows, experts * 10), 1)
    picks = []
    for t in range(2):
        mine = route_ref[:, t : t + 1]
        ordinal = jnp.zeros((rows, 1), jnp.int32)
        for u in range(2):
            before = (earlier < later) if u >= t else (earlier <= later)
            same = route_t_ref[u : u + 1, :] == mine
            ordinal += jnp.sum(jnp.where(before & same, 1, 0), axis=1, keepdims=True)
        picks.append(jnp.where(slots == slot_of(mine, ordinal, experts), 1.0, 0.0).astype(bf16))
    scores = score_ref[...]
    raised = jnp.exp(scores - jnp.max(scores, axis=1, keepdims=True))
    mixing = prob_ref[...] * (raised / jnp.sum(raised, axis=1, keepdims=True))

    def store(k, block):
        block = block.astype(bf16)
        cols = slice(k * HEAD, (k + 1) * HEAD)
        combined = sum(dot(picks[t], block) * mixing[:, t : t + 1] for t in range(2))
        out_ref[:, cols] = (upd_ref[:, cols].astype(f32) + combined).astype(bf16)

    unpack(in_ref, store)


def mix(returned, updated, route, route_t, scores, prob):
    return pl.pallas_call(
        mix_kernel,
        out_shape=jax.ShapeDtypeStruct(updated.shape, bf16),
        name="mix",
    )(returned, updated, route, route_t, scores, prob)


def shift(value, axis, by):
    size = lax.axis_size(axis)
    return lax.ppermute(value, axis, [(i, (i + by) % size) for i in range(size)])


def onward(value, axis):
    size = lax.axis_size(axis)
    pairs = []
    for i in range(size):
        pairs.append((2 * i, 2 * ((i + 1) % size)))
        pairs.append((2 * i + 1, 2 * ((i - 1) % size) + 1))
    return lax.ppermute(value, (axis, "core"), pairs)


def swap_cores(value):
    return lax.ppermute(value, "core", ((0, 1), (1, 0)))


def local(
    queries,
    keys,
    values,
    query_gain,
    key_gain,
    out_weight,
    residual,
    norm_gain,
    route_experts,
    expert_scores,
    group_prob,
    w_gate,
    w_up,
    w_down,
):
    peers = lax.axis_size(SP)
    core = lax.axis_index("core")
    z = lax.axis_index("z")
    seq = lax.axis_index(SP)
    tokens = queries.shape[0]

    where = jnp.stack([core, z // 2]).astype(jnp.int32)
    lane = jnp.arange(HEAD, dtype=jnp.int32)
    pair = (lane // 2) % (HEAD // 4)
    frequency = rope_base ** (-pair.astype(f32) * 4.0 / HEAD)
    grid_rows = tokens // GRID_W
    place = jnp.arange(grid_rows + GRID_W, dtype=jnp.int32)
    place = jnp.where(place < grid_rows, seq * grid_rows + place, place - grid_rows)
    angles = place.astype(f32)[:, None] * frequency[None, :]
    cosine = jnp.cos(angles)
    sine = jnp.sin(angles) * jnp.where(lane % 2 == 0, -1.0, 1.0)[None, :]

    weights = lax.all_gather(bundle(w_gate[0], w_up[0], w_down[0]), TP)
    own, kv_a, kv_b = prep(
        where, queries, keys, values, query_gain[None, :], key_gain[None, :], cosine, sine
    )
    ax = jnp.concatenate([kv_a] + [shift(kv_a, "x", d) for d in (1, -1, 2)], axis=0)
    by = jnp.concatenate([kv_b] + [shift(kv_b, "y", d) for d in (1, -1, 2)], axis=0)
    sib = swap_cores(own)
    a_next = [shift(ax, "y", 1), shift(ax, "y", -1)]
    b_next = [shift(by, "x", 1), shift(by, "x", -1)]
    state = attend(where, own, sib, [ax, by], None, False)
    state, a_next, b_next = lax.optimization_barrier((state, a_next, b_next))
    a_far = onward(jnp.where(core == 0, a_next[0], a_next[1]), "y")
    b_far = onward(jnp.where(core == 0, b_next[0], b_next[1]), "x")
    state = attend(where, own, sib, a_next + b_next, state, False)
    keep, send = attend(where, own, sib, [a_far, b_far], state, True)
    merged = merge(where, keep, swap_cores(send))
    attended = lax.all_to_all(merged, "z", 0, 0, tiled=True)
    route_t = route_experts.T
    updated, outgoing = project(
        attended, out_weight, residual, norm_gain[None, :], route_experts, route_t, peers
    )
    arrived = lax.all_to_all(outgoing, SP, 0, 0, tiled=True)
    returned = lax.all_to_all(expert(arrived, weights), SP, 0, 0, tiled=True)
    return mix(
        returned, updated, route_experts, route_t, expert_scores, group_prob[:, None]
    )


def solution(mesh):
    torus = Mesh(mesh.devices.reshape(4, 4, 8, 2), ("y", "x", "z", "core"))
    placed = (
        P(SP, TP),
        P(SP, None),
        P(SP, None),
        P(TP),
        P(),
        P(),
        P(SP_TP, None),
        P(),
        P(SP_TP, None),
        P(SP_TP, None),
        P(SP_TP),
        P(SP, None, TP),
        P(SP, None, TP),
        P(SP, TP, None),
    )
    return jax.shard_map(
        local, mesh=torus, in_specs=placed, out_specs=P(SP_TP, None), check_vma=False
    )
```

```python
import functools
import math

import jax
import jax.numpy as jnp
from jax import lax
from jax.experimental import pallas as pl
from jax.experimental.pallas import tpu as pltpu
from jax.sharding import Mesh
from jax.sharding import PartitionSpec as P

GRID_W = 64
HEAD = 128
SP = ("y", "x")
TP = ("z", "core")
SP_TP = ("y", "x", "z", "core")
rope_base = 10000.0
norm_eps = 1e-06
f32 = jnp.float32
bf16 = jnp.bfloat16


def dot(a, b):
    return jnp.dot(a, b, preferred_element_type=f32)


def bundle_kernel(gate_ref, up_ref, down_ref, out_ref):
    units = gate_ref.shape[1]
    out_ref[0] = gate_ref[...]
    out_ref[1] = up_ref[...]
    for k in range(down_ref.shape[1] // HEAD):
        out_ref[2, k * units : (k + 1) * units, :] = down_ref[:, k * HEAD : (k + 1) * HEAD]


def bundle(gate, up, down):
    width, units = gate.shape
    rows = width // 2
    spec = pl.BlockSpec((rows, units), lambda i: (i, 0))
    return pl.pallas_call(
        bundle_kernel,
        grid=(2,),
        in_specs=[spec, spec, pl.BlockSpec((units, rows), lambda i: (0, i))],
        out_specs=pl.BlockSpec((3, rows, units), lambda i: (0, i, 0)),
        out_shape=jax.ShapeDtypeStruct((3, width, units), bf16),
        name="bundle",
    )(gate, up, down)


def prep_kernel(
    where_ref, q_ref, k_ref, v_ref, qg_ref, kg_ref, cos_ref, sin_ref, q_out, kv_a, kv_b
):
    lane = lax.broadcasted_iota(jnp.int32, (GRID_W, HEAD), 1)
    even = lane % 2 == 0
    from_row = lane < HEAD // 2
    col_cos = cos_ref[16:, :]
    col_sin = sin_ref[16:, :]

    def turn(vectors, gain, row_cos, row_sin):
        mean = jnp.mean(vectors * vectors, axis=-1, keepdims=True)
        u = vectors * lax.rsqrt(mean + norm_eps) * gain
        swapped = jnp.where(even, pltpu.roll(u, HEAD - 1, 1), pltpu.roll(u, 1, 1))
        cosine = jnp.where(from_row, row_cos, col_cos)
        sine = jnp.where(from_row, row_sin, col_sin)
        return u * cosine + swapped * sine

    for r in range(q_ref.shape[0] // GRID_W):
        rows = slice(r * GRID_W, (r + 1) * GRID_W)
        q_out[rows, :] = turn(
            q_ref[rows, :].astype(f32), qg_ref[...], cos_ref[r : r + 1, :], sin_ref[r : r + 1, :]
        ).astype(bf16)
    half = k_ref.shape[0] // GRID_W
    first = where_ref[0] * half
    for r in range(half):
        rows = slice(r * GRID_W, (r + 1) * GRID_W)
        row_cos = cos_ref[pl.ds(first + r, 1), :]
        row_sin = sin_ref[pl.ds(first + r, 1), :]
        kv_out = kv_a if r < half // 2 else kv_b
        at = r % (half // 2)
        rows_out = slice(at * GRID_W, (at + 1) * GRID_W)
        kv_out[rows_out, :HEAD] = turn(
            k_ref[rows, :].astype(f32), kg_ref[...], row_cos, row_sin
        ).astype(bf16)
        kv_out[rows_out, HEAD:] = v_ref[rows, :]


def prep(where, queries, keys, values, query_gain, key_gain, cosine, sine):
    tokens = queries.shape[0]
    half = tokens // 2
    whole = lambda shape: pl.BlockSpec(shape, lambda i, w: (0, 0))
    part = pl.BlockSpec((half, HEAD), lambda i, w: (w[0], w[1]))
    return pl.pallas_call(
        prep_kernel,
        grid_spec=pltpu.PrefetchScalarGridSpec(
            num_scalar_prefetch=1,
            grid=(1,),
            in_specs=[
                whole((tokens, HEAD)),
                part,
                part,
                whole((1, HEAD)),
                whole((1, HEAD)),
                whole(cosine.shape),
                whole(sine.shape),
            ],
            out_specs=[
                whole((tokens, HEAD)),
                whole((half // 2, 2 * HEAD)),
                whole((half // 2, 2 * HEAD)),
            ],
        ),
        out_shape=[
            jax.ShapeDtypeStruct((tokens, HEAD), bf16),
            jax.ShapeDtypeStruct((half // 2, 2 * HEAD), bf16),
            jax.ShapeDtypeStruct((half // 2, 2 * HEAD), bf16),
        ],
        name="prep",
    )(where, queries, keys, values, query_gain, key_gain, cosine, sine)


BQ = 256


def attend_kernel(first, last, count, where_ref, own_ref, sib_ref, *refs):
    kv_refs, refs = refs[:count], refs[count:]
    if not first:
        acc_in, top_in, *refs = refs
    out_a, out_b, kk, vv = refs
    rows = kv_refs[0].shape[0]

    @pl.when((pl.program_id(0) == 0) & (pl.program_id(1) == 0))
    def _():
        for b in range(count):
            span = slice(b * rows, (b + 1) * rows)
            k = kv_refs[b][:, :HEAD]
            kk[span, :HEAD] = k
            kk[span, HEAD:] = k
            vv[span, :HEAD] = kv_refs[b][:, HEAD:]
            vv[span, HEAD:] = jnp.ones((rows, HEAD), bf16)

    q = jnp.where(pl.program_id(0) == 0, own_ref[...].astype(f32), sib_ref[...].astype(f32))
    scaled = q * (HEAD ** (-0.5) * math.log2(math.e))
    high = scaled.astype(bf16)
    low = (scaled - high.astype(f32)).astype(bf16)
    pair = jnp.concatenate([high, low], axis=1)
    top = None if first else jnp.max(top_in[0], axis=1, keepdims=True)
    acc = None if first else acc_in[0]
    for j in range(count):
        span = slice(j * rows, (j + 1) * rows)
        s = lax.dot_general(
            pair, kk[span, :], (((1,), (1,)), ((), ())), preferred_element_type=f32
        )
        block_top = jnp.max(s, axis=1, keepdims=True)
        new_top = block_top if top is None else jnp.maximum(top, block_top)
        raised = jnp.exp2(s - new_top).astype(bf16)
        part = dot(raised, vv[span, :])
        acc = part if top is None else acc * jnp.exp2(top - new_top) + part
        top = new_top
    if not last:
        out_a[0] = acc
        out_b[0] = jnp.broadcast_to(top, (top.shape[0], HEAD))
        return
    total = acc[:, HEAD:]
    normal = acc[:, :HEAD] / total
    level = top + jnp.log2(total)
    first_core = where_ref[0] == 0
    lane = lax.broadcasted_iota(jnp.int32, (64, HEAD), 1)
    for z in range(BQ // 128):
        a = slice(z * 128, z * 128 + 64)
        b = slice(z * 128 + 64, z * 128 + 128)
        out_a[0, z, :, :HEAD] = jnp.where(first_core, normal[a], normal[b])
        out_a[0, z, :, HEAD:] = jnp.where(first_core, level[a], level[b])
        out_b[0, z, :, :HEAD] = jnp.where(first_core, normal[b], normal[a]).astype(bf16)
        sent = jnp.where(first_core, level[b], level[a])
        l0 = sent.astype(bf16).astype(f32)
        l1 = (sent - l0).astype(bf16).astype(f32)
        l2 = sent - l0 - l1
        out_b[0, z, :, HEAD:] = jnp.where(lane < 32, l0, jnp.where(lane < 64, l1, l2)).astype(bf16)


def attend(where, own, sib, kvs, state, last):
    tokens = own.shape[0]
    rows = kvs[0].shape[0]
    first = state is None
    count = len(kvs)
    q_spec = pl.BlockSpec((BQ, HEAD), lambda h, i, w: (i, 0))
    kv_spec = pl.BlockSpec((rows, 2 * HEAD), lambda h, i, w: (0, 0))
    acc_spec = pl.BlockSpec((1, BQ, 2 * HEAD), lambda h, i, w: (h, i, 0))
    top_spec = pl.BlockSpec((1, BQ, HEAD), lambda h, i, w: (h, i, 0))
    if last:
        out_spec = pl.BlockSpec((1, BQ // 128, 64, 2 * HEAD), lambda h, i, w: (h, i, 0, 0))
        out_specs = [out_spec, out_spec]
        out_shape = [
            jax.ShapeDtypeStruct((2, tokens // 128, 64, 2 * HEAD), f32),
            jax.ShapeDtypeStruct((2, tokens // 128, 64, 2 * HEAD), bf16),
        ]
    else:
        out_specs = [acc_spec, top_spec]
        out_shape = [
            jax.ShapeDtypeStruct((2, tokens, 2 * HEAD), f32),
            jax.ShapeDtypeStruct((2, tokens, HEAD), f32),
        ]
    return pl.pallas_call(
        functools.partial(attend_kernel, first, last, count),
        grid_spec=pltpu.PrefetchScalarGridSpec(
            num_scalar_prefetch=1,
            grid=(2, tokens // BQ),
            in_specs=[q_spec, q_spec]
            + [kv_spec] * count
            + ([] if first else [acc_spec, top_spec]),
            out_specs=out_specs,
            scratch_shapes=[
                pltpu.VMEM((count * rows, 2 * HEAD), bf16),
                pltpu.VMEM((count * rows, 2 * HEAD), bf16),
            ],
        ),
        out_shape=out_shape,
        compiler_params=pltpu.CompilerParams(vmem_limit_bytes=32 * 1024 * 1024),
        name="attend",
    )(where, own, sib, *kvs, *([] if first else state))


def merge_kernel(where_ref, keep_ref, got_ref, out_ref):
    def merged(mine, other):
        other = other.astype(f32)
        theirs = other[:, HEAD : HEAD + 1] + other[:, HEAD + 32 : HEAD + 33]
        theirs = theirs + other[:, HEAD + 64 : HEAD + 65]
        level = jnp.maximum(mine[:, HEAD:], theirs)
        a = jnp.exp2(mine[:, HEAD:] - level)
        b = jnp.exp2(theirs - level)
        return (mine[:, :HEAD] * a + other[:, :HEAD] * b) / (a + b)

    first_core = where_ref[0] == 0
    for z in range(keep_ref.shape[1]):
        own = merged(keep_ref[0, z], got_ref[1, z])
        sib = merged(keep_ref[1, z], got_ref[0, z])
        out_ref[z, :, :HEAD] = jnp.where(first_core, own, sib).astype(bf16)
        out_ref[z, :, HEAD:] = jnp.where(first_core, sib, own).astype(bf16)


def merge(where, keep, got):
    _, z, rows, _ = keep.shape
    return pl.pallas_call(
        merge_kernel,
        grid_spec=pltpu.PrefetchScalarGridSpec(
            num_scalar_prefetch=1,
            grid=(1,),
            in_specs=[pl.BlockSpec(keep.shape, lambda i, w: (0, 0, 0, 0))] * 2,
            out_specs=pl.BlockSpec((z, rows, 2 * HEAD), lambda i, w: (0, 0, 0)),
        ),
        out_shape=jax.ShapeDtypeStruct((z, rows, 2 * HEAD), bf16),
        name="merge",
    )(where, keep, got)


def swap_matrix(experts, blocks):
    count = experts * blocks * 2
    row = lax.broadcasted_iota(jnp.int32, (count, count), 0)
    col = lax.broadcasted_iota(jnp.int32, (count, count), 1)
    a, b, j = row // (blocks * 2), (row // 2) % blocks, row % 2
    return jnp.where(col == b * (experts * 2) + a * 2 + j, 1.0, 0.0).astype(bf16)


def pack(rows_of, out_ref, swap):
    peers = out_ref.shape[0]
    blocks = 16
    tails = []
    for k in range(blocks):
        block = rows_of(k)
        head = block[: peers * 8].reshape(peers, 8, HEAD)
        out_ref[:, k * 8 : (k + 1) * 8, :] = head.astype(bf16)
        tails.append(block[peers * 8 :])
    tail = jnp.concatenate(tails, axis=0).astype(bf16)
    turned = dot(swap, tail)
    out_ref[:, blocks * 8 :, :] = turned.reshape(peers, blocks * 2, HEAD).astype(bf16)


def unpack(in_ref, store, swap):
    peers = in_ref.shape[0]
    blocks = 16
    tail = in_ref[:, blocks * 8 :, :].astype(f32).reshape(peers * blocks * 2, HEAD).astype(bf16)
    turned = dot(swap, tail)
    for k in range(blocks):
        head = in_ref[:, k * 8 : (k + 1) * 8, :].astype(f32).reshape(peers * 8, HEAD)
        store(k, jnp.concatenate([head, turned[k * peers * 2 : (k + 1) * peers * 2]], axis=0))


def slot_of(expert, ordinal, experts):
    return jnp.where(ordinal < 8, expert * 8 + ordinal, experts * 8 + expert * 2 + ordinal - 8)


def project_kernel(
    a_ref, w_ref, res_ref, gain_ref, route_ref, route_t_ref, swap_ref, upd_ref, out_ref, held, sems
):
    steps, rows, depth = a_ref.shape
    copies = [
        pltpu.make_async_copy(
            w_ref.at[pl.ds(i * depth, depth)], held.at[pl.ds(i * depth, depth)], sems.at[i]
        )
        for i in range(steps)
    ]
    for copy in copies:
        copy.start()
    experts = out_ref.shape[0]
    earlier = lax.broadcasted_iota(jnp.int32, (rows, rows), 0)
    later = lax.broadcasted_iota(jnp.int32, (rows, rows), 1)
    slots = lax.broadcasted_iota(jnp.int32, (experts * 10, rows), 0)
    placing = jnp.zeros((experts * 10, rows), f32)
    for t in range(2):
        mine = route_t_ref[t : t + 1, :]
        ordinal = jnp.zeros((1, rows), jnp.int32)
        for u in range(2):
            before = (earlier < later) if u >= t else (earlier <= later)
            same = route_ref[:, u : u + 1] == mine
            ordinal += jnp.sum(jnp.where(before & same, 1, 0), axis=0, keepdims=True)
        placing += jnp.where(slots == slot_of(mine, ordinal, experts), 1.0, 0.0)
    acc = res_ref[...].astype(f32)
    for i in range(steps):
        copies[i].wait()
        acc += dot(a_ref[i], held[i * depth : (i + 1) * depth, :])
    updated = acc.astype(bf16)
    upd_ref[...] = updated
    wide = updated.astype(f32)
    mean = jnp.mean(wide * wide, axis=1, keepdims=True)
    normed = (wide * lax.rsqrt(mean + norm_eps) * gain_ref[...]).astype(bf16)
    sent = dot(placing.astype(bf16), normed)
    pack(lambda k: sent[:, k * HEAD : (k + 1) * HEAD], out_ref, swap_ref[...])


VMEM = pl.BlockSpec(memory_space=pltpu.VMEM)
HBM = pl.BlockSpec(memory_space=pl.ANY)
ROOM = pltpu.CompilerParams(vmem_limit_bytes=48 * 1024 * 1024)


def project(attended, out_weight, residual, norm_gain, route, route_t, swap, peers):
    steps, rows, depth = attended.shape
    width = out_weight.shape[1]
    return pl.pallas_call(
        project_kernel,
        in_specs=[VMEM, HBM, VMEM, VMEM, VMEM, VMEM, VMEM],
        out_specs=[VMEM, VMEM],
        out_shape=[
            jax.ShapeDtypeStruct((rows, width), bf16),
            jax.ShapeDtypeStruct((peers, 160, HEAD), bf16),
        ],
        scratch_shapes=[
            pltpu.VMEM(out_weight.shape, bf16),
            pltpu.SemaphoreType.DMA((steps,)),
        ],
        compiler_params=ROOM,
        name="project",
    )(attended, out_weight, residual, norm_gain, route, route_t, swap)


def rows_kernel(in_ref, swap_ref, x_ref):
    def store(k, block):
        x_ref[:, k * HEAD : (k + 1) * HEAD] = block.astype(bf16)

    unpack(in_ref, store, swap_ref[...])


def rows_in(arrived, swap):
    peers = arrived.shape[0]
    return pl.pallas_call(
        rows_kernel,
        in_specs=[VMEM, VMEM],
        out_specs=VMEM,
        out_shape=jax.ShapeDtypeStruct((peers * 10, 16 * HEAD), bf16),
        name="rows_in",
    )(arrived, swap)


FLIGHT = 6


def expert_kernel(rows_ref, w_ref, turn_ref, out_ref, held, x_ref, swap_ref, acc, sems):
    blocks, _, width, _ = held.shape
    copies = [pltpu.make_async_copy(w_ref.at[i], held.at[i], sems.at[i]) for i in range(blocks)]
    rows_copy = pltpu.make_async_copy(rows_ref, x_ref, sems.at[blocks])
    turn_copy = pltpu.make_async_copy(turn_ref, swap_ref, sems.at[blocks + 1])
    rows_copy.start()
    for copy in copies[:FLIGHT]:
        copy.start()
    turn_copy.start()
    rows_copy.wait()
    for i in range(0, blocks, 2):
        pair = (i, i + 1)
        for j in pair:
            copies[j].wait()
        for j in range(i + FLIGHT, min(i + FLIGHT + 2, blocks)):
            copies[j].start()
        gate = dot(x_ref[...], jnp.concatenate([held[j, 0] for j in pair], axis=1))
        up = dot(x_ref[...], jnp.concatenate([held[j, 1] for j in pair], axis=1))
        hid = (gate / (1.0 + jnp.exp(-gate)) * up).astype(bf16)
        down = jnp.concatenate(
            [
                jnp.concatenate(
                    [held[j, 2, k * HEAD : (k + 1) * HEAD, :] for j in pair], axis=0
                )
                for k in range(width // HEAD)
            ],
            axis=1,
        )
        part = dot(hid, down)
        if i == 0:
            acc[...] = part
        else:
            acc[...] += part
    turn_copy.wait()
    pack(lambda k: acc[:, k * HEAD : (k + 1) * HEAD], out_ref, swap_ref[...])


def expert(x, weights, swap, peers):
    blocks, _, width, _ = weights.shape
    return pl.pallas_call(
        expert_kernel,
        in_specs=[HBM, HBM, HBM],
        out_specs=VMEM,
        out_shape=jax.ShapeDtypeStruct((peers, 160, HEAD), bf16),
        scratch_shapes=[
            pltpu.VMEM(weights.shape, bf16),
            pltpu.VMEM(x.shape, bf16),
            pltpu.VMEM(swap.shape, bf16),
            pltpu.VMEM((160, width), f32),
            pltpu.SemaphoreType.DMA((blocks + 2,)),
        ],
        compiler_params=ROOM,
        name="expert",
    )(x, weights, swap)


def plan_kernel(route_ref, route_t_ref, score_ref, prob_ref, pick_ref, mix_ref, swap_ref):
    rows = route_ref.shape[0]
    experts = pick_ref.shape[2] // 10
    later = lax.broadcasted_iota(jnp.int32, (rows, rows), 0)
    earlier = lax.broadcasted_iota(jnp.int32, (rows, rows), 1)
    slots = lax.broadcasted_iota(jnp.int32, (rows, experts * 10), 1)
    scores = score_ref[...]
    raised = jnp.exp(scores - jnp.max(scores, axis=1, keepdims=True))
    mixing = prob_ref[...] * (raised / jnp.sum(raised, axis=1, keepdims=True))
    for t in range(2):
        mine = route_ref[:, t : t + 1]
        ordinal = jnp.zeros((rows, 1), jnp.int32)
        for u in range(2):
            before = (earlier < later) if u >= t else (earlier <= later)
            same = route_t_ref[u : u + 1, :] == mine
            ordinal += jnp.sum(jnp.where(before & same, 1, 0), axis=1, keepdims=True)
        placed = slots == slot_of(mine, ordinal, experts)
        pick_ref[t] = jnp.where(placed, 1.0, 0.0).astype(bf16)
        mix_ref[t] = jnp.broadcast_to(mixing[:, t : t + 1], (rows, HEAD))
    swap_ref[...] = swap_matrix(experts, 16)


def plan(route, route_t, scores, prob, experts):
    rows = route.shape[0]
    return pl.pallas_call(
        plan_kernel,
        in_specs=[VMEM] * 4,
        out_specs=[VMEM] * 3,
        out_shape=[
            jax.ShapeDtypeStruct((2, rows, experts * 10), bf16),
            jax.ShapeDtypeStruct((2, rows, HEAD), f32),
            jax.ShapeDtypeStruct((experts * 32, experts * 32), bf16),
        ],
        name="plan",
    )(route, route_t, scores, prob)


def mix_kernel(in_ref, upd_ref, pick_ref, mix_ref, swap_ref, out_ref):
    def store(k, block):
        block = block.astype(bf16)
        cols = slice(k * HEAD, (k + 1) * HEAD)
        combined = sum(dot(pick_ref[t], block) * mix_ref[t] for t in range(2))
        out_ref[:, cols] = (upd_ref[:, cols].astype(f32) + combined).astype(bf16)

    unpack(in_ref, store, swap_ref[...])


def mix(returned, updated, picks, mixing, swap):
    return pl.pallas_call(
        mix_kernel,
        in_specs=[VMEM] * 5,
        out_specs=VMEM,
        out_shape=jax.ShapeDtypeStruct(updated.shape, bf16),
        name="mix",
    )(returned, updated, picks, mixing, swap)


def shift(value, axis, by):
    size = lax.axis_size(axis)
    return lax.ppermute(value, axis, [(i, (i + by) % size) for i in range(size)])


def onward(value, axis):
    size = lax.axis_size(axis)
    pairs = []
    for i in range(size):
        pairs.append((2 * i, 2 * ((i + 1) % size)))
        pairs.append((2 * i + 1, 2 * ((i - 1) % size) + 1))
    return lax.ppermute(value, (axis, "core"), pairs)


def swap_cores(value):
    return lax.ppermute(value, "core", ((0, 1), (1, 0)))


def local(
    queries,
    keys,
    values,
    query_gain,
    key_gain,
    out_weight,
    residual,
    norm_gain,
    route_experts,
    expert_scores,
    group_prob,
    w_gate,
    w_up,
    w_down,
):
    peers = lax.axis_size(SP)
    core = lax.axis_index("core")
    z = lax.axis_index("z")
    seq = lax.axis_index(SP)
    tokens = queries.shape[0]

    where = jnp.stack([core, z // 2]).astype(jnp.int32)
    lane = jnp.arange(HEAD, dtype=jnp.int32)
    pair = (lane // 2) % (HEAD // 4)
    frequency = rope_base ** (-pair.astype(f32) * 4.0 / HEAD)
    grid_rows = tokens // GRID_W
    place = jnp.arange(grid_rows + GRID_W, dtype=jnp.int32)
    place = jnp.where(place < grid_rows, seq * grid_rows + place, place - grid_rows)
    angles = place.astype(f32)[:, None] * frequency[None, :]
    cosine = jnp.cos(angles)
    sine = jnp.sin(angles) * jnp.where(lane % 2 == 0, -1.0, 1.0)[None, :]

    weights = lax.all_gather(bundle(w_gate[0], w_up[0], w_down[0]), TP)
    route_t = route_experts.T
    picks, mixing, swap = plan(
        route_experts, route_t, expert_scores, group_prob[:, None], peers
    )
    own, kv_a, kv_b = prep(
        where, queries, keys, values, query_gain[None, :], key_gain[None, :], cosine, sine
    )
    ax = jnp.concatenate([kv_a] + [shift(kv_a, "x", d) for d in (1, -1, 2)], axis=0)
    by = jnp.concatenate([kv_b] + [shift(kv_b, "y", d) for d in (1, -1, 2)], axis=0)
    sib = swap_cores(own)
    a_next = [shift(ax, "y", 1), shift(ax, "y", -1)]
    b_next = [shift(by, "x", 1), shift(by, "x", -1)]
    state = attend(where, own, sib, [ax, by], None, False)
    state, a_next, b_next = lax.optimization_barrier((state, a_next, b_next))
    a_far = onward(jnp.where(core == 0, a_next[0], a_next[1]), "y")
    b_far = onward(jnp.where(core == 0, b_next[0], b_next[1]), "x")
    state = attend(where, own, sib, a_next + b_next, state, False)
    keep, send = attend(where, own, sib, [a_far, b_far], state, True)
    merged = merge(where, keep, swap_cores(send))
    attended = lax.all_to_all(merged, "z", 0, 0, tiled=True)
    updated, outgoing = project(
        attended, out_weight, residual, norm_gain[None, :], route_experts, route_t, swap, peers
    )
    arrived = lax.all_to_all(outgoing, SP, 0, 0, tiled=True)
    result = expert(rows_in(arrived, swap), weights, swap, peers)
    returned = lax.all_to_all(result, SP, 0, 0, tiled=True)
    return mix(returned, updated, picks, mixing, swap)


def solution(mesh):
    torus = Mesh(mesh.devices.reshape(4, 4, 8, 2), ("y", "x", "z", "core"))
    placed = (
        P(SP, TP),
        P(SP, None),
        P(SP, None),
        P(TP),
        P(),
        P(),
        P(SP_TP, None),
        P(),
        P(SP_TP, None),
        P(SP_TP, None),
        P(SP_TP),
        P(SP, None, TP),
        P(SP, None, TP),
        P(SP, TP, None),
    )
    return jax.shard_map(
        local, mesh=torus, in_specs=placed, out_specs=P(SP_TP, None), check_vma=False
    )
```

```python
import functools
import math

import jax
import jax.numpy as jnp
from jax import lax
from jax.experimental import pallas as pl
from jax.experimental.pallas import tpu as pltpu
from jax.sharding import Mesh
from jax.sharding import PartitionSpec as P

GRID_W = 64
HEAD = 128
SP = ("y", "x")
TP = ("z", "core")
SP_TP = ("y", "x", "z", "core")
rope_base = 10000.0
norm_eps = 1e-06
f32 = jnp.float32
bf16 = jnp.bfloat16


def room(mib):
    return pltpu.CompilerParams(vmem_limit_bytes=mib * 1024 * 1024)


def dot(a, b):
    return jnp.dot(a, b, preferred_element_type=f32)


def bundle_kernel(gate_ref, up_ref, down_ref, out_ref):
    units = gate_ref.shape[1]
    out_ref[0] = gate_ref[...]
    out_ref[1] = up_ref[...]
    for k in range(down_ref.shape[1] // HEAD):
        out_ref[2, k * units : (k + 1) * units, :] = down_ref[:, k * HEAD : (k + 1) * HEAD]


def bundle(gate, up, down):
    width, units = gate.shape
    rows = width // 2
    spec = pl.BlockSpec((rows, units), lambda i: (i, 0))
    return pl.pallas_call(
        bundle_kernel,
        grid=(2,),
        in_specs=[spec, spec, pl.BlockSpec((units, rows), lambda i: (0, i))],
        out_specs=pl.BlockSpec((3, rows, units), lambda i: (0, i, 0)),
        out_shape=jax.ShapeDtypeStruct((3, width, units), bf16),
        name="bundle",
    )(gate, up, down)


def prep_kernel(
    where_ref, q_ref, k_ref, v_ref, qg_ref, kg_ref, cos_ref, sin_ref, q_out, kv_a, kv_b
):
    lane = lax.broadcasted_iota(jnp.int32, (GRID_W, HEAD), 1)
    even = lane % 2 == 0
    from_row = lane < HEAD // 2
    col_cos = cos_ref[16:, :]
    col_sin = sin_ref[16:, :]

    def turn(vectors, gain, row_cos, row_sin):
        mean = jnp.mean(vectors * vectors, axis=-1, keepdims=True)
        u = vectors * lax.rsqrt(mean + norm_eps) * gain
        swapped = jnp.where(even, pltpu.roll(u, HEAD - 1, 1), pltpu.roll(u, 1, 1))
        cosine = jnp.where(from_row, row_cos, col_cos)
        sine = jnp.where(from_row, row_sin, col_sin)
        return u * cosine + swapped * sine

    for r in range(q_ref.shape[0] // GRID_W):
        rows = slice(r * GRID_W, (r + 1) * GRID_W)
        q_out[rows, :] = turn(
            q_ref[rows, :].astype(f32), qg_ref[...], cos_ref[r : r + 1, :], sin_ref[r : r + 1, :]
        ).astype(bf16)
    half = k_ref.shape[0] // GRID_W
    first = where_ref[0] * half
    for r in range(half):
        rows = slice(r * GRID_W, (r + 1) * GRID_W)
        row_cos = cos_ref[pl.ds(first + r, 1), :]
        row_sin = sin_ref[pl.ds(first + r, 1), :]
        kv_out = kv_a if r < half // 2 else kv_b
        at = r % (half // 2)
        rows_out = slice(at * GRID_W, (at + 1) * GRID_W)
        kv_out[rows_out, :HEAD] = turn(
            k_ref[rows, :].astype(f32), kg_ref[...], row_cos, row_sin
        ).astype(bf16)
        kv_out[rows_out, HEAD:] = v_ref[rows, :]


def prep(where, queries, keys, values, query_gain, key_gain, cosine, sine):
    tokens = queries.shape[0]
    half = tokens // 2
    whole = lambda shape: pl.BlockSpec(shape, lambda i, w: (0, 0))
    part = pl.BlockSpec((half, HEAD), lambda i, w: (w[0], w[1]))
    return pl.pallas_call(
        prep_kernel,
        grid_spec=pltpu.PrefetchScalarGridSpec(
            num_scalar_prefetch=1,
            grid=(1,),
            in_specs=[
                whole((tokens, HEAD)),
                part,
                part,
                whole((1, HEAD)),
                whole((1, HEAD)),
                whole(cosine.shape),
                whole(sine.shape),
            ],
            out_specs=[
                whole((tokens, HEAD)),
                whole((half // 2, 2 * HEAD)),
                whole((half // 2, 2 * HEAD)),
            ],
        ),
        out_shape=[
            jax.ShapeDtypeStruct((tokens, HEAD), bf16),
            jax.ShapeDtypeStruct((half // 2, 2 * HEAD), bf16),
            jax.ShapeDtypeStruct((half // 2, 2 * HEAD), bf16),
        ],
        name="prep",
    )(where, queries, keys, values, query_gain, key_gain, cosine, sine)


BQ = 256


def attend_kernel(first, last, count, where_ref, own_ref, sib_ref, *refs):
    kv_refs, refs = refs[:count], refs[count:]
    if not first:
        acc_in, top_in, *refs = refs
    out_a, out_b, kk, vv = refs
    rows = kv_refs[0].shape[0]

    @pl.when((pl.program_id(0) == 0) & (pl.program_id(1) == 0))
    def _():
        for b in range(count):
            span = slice(b * rows, (b + 1) * rows)
            k = kv_refs[b][:, :HEAD]
            kk[span, :HEAD] = k
            kk[span, HEAD:] = k
            vv[span, :HEAD] = kv_refs[b][:, HEAD:]
            vv[span, HEAD:] = jnp.ones((rows, HEAD), bf16)

    q = jnp.where(pl.program_id(0) == 0, own_ref[...].astype(f32), sib_ref[...].astype(f32))
    scaled = q * (HEAD ** (-0.5) * math.log2(math.e))
    high = scaled.astype(bf16)
    low = (scaled - high.astype(f32)).astype(bf16)
    pair = jnp.concatenate([high, low], axis=1)
    top = None if first else jnp.max(top_in[0], axis=1, keepdims=True)
    acc = None if first else acc_in[0]
    for j in range(count):
        span = slice(j * rows, (j + 1) * rows)
        s = lax.dot_general(
            pair, kk[span, :], (((1,), (1,)), ((), ())), preferred_element_type=f32
        )
        block_top = jnp.max(s, axis=1, keepdims=True)
        new_top = block_top if top is None else jnp.maximum(top, block_top)
        raised = jnp.exp2(s - new_top).astype(bf16)
        part = dot(raised, vv[span, :])
        acc = part if top is None else acc * jnp.exp2(top - new_top) + part
        top = new_top
    if not last:
        out_a[0] = acc
        out_b[0] = jnp.broadcast_to(top, (top.shape[0], HEAD))
        return
    total = acc[:, HEAD:]
    normal = acc[:, :HEAD] / total
    level = top + jnp.log2(total)
    first_core = where_ref[0] == 0
    lane = lax.broadcasted_iota(jnp.int32, (64, HEAD), 1)
    for z in range(BQ // 128):
        a = slice(z * 128, z * 128 + 64)
        b = slice(z * 128 + 64, z * 128 + 128)
        out_a[0, z, :, :HEAD] = jnp.where(first_core, normal[a], normal[b])
        out_a[0, z, :, HEAD:] = jnp.where(first_core, level[a], level[b])
        out_b[0, z, :, :HEAD] = jnp.where(first_core, normal[b], normal[a]).astype(bf16)
        sent = jnp.where(first_core, level[b], level[a])
        l0 = sent.astype(bf16).astype(f32)
        l1 = (sent - l0).astype(bf16).astype(f32)
        l2 = sent - l0 - l1
        out_b[0, z, :, HEAD:] = jnp.where(lane < 32, l0, jnp.where(lane < 64, l1, l2)).astype(bf16)


def attend(where, own, sib, kvs, state, last):
    tokens = own.shape[0]
    rows = kvs[0].shape[0]
    first = state is None
    count = len(kvs)
    q_spec = pl.BlockSpec((BQ, HEAD), lambda h, i, w: (i, 0))
    kv_spec = pl.BlockSpec((rows, 2 * HEAD), lambda h, i, w: (0, 0))
    acc_spec = pl.BlockSpec((1, BQ, 2 * HEAD), lambda h, i, w: (h, i, 0))
    top_spec = pl.BlockSpec((1, BQ, HEAD), lambda h, i, w: (h, i, 0))
    if last:
        out_spec = pl.BlockSpec((1, BQ // 128, 64, 2 * HEAD), lambda h, i, w: (h, i, 0, 0))
        out_specs = [out_spec, out_spec]
        out_shape = [
            jax.ShapeDtypeStruct((2, tokens // 128, 64, 2 * HEAD), f32),
            jax.ShapeDtypeStruct((2, tokens // 128, 64, 2 * HEAD), bf16),
        ]
    else:
        out_specs = [acc_spec, top_spec]
        out_shape = [
            jax.ShapeDtypeStruct((2, tokens, 2 * HEAD), f32),
            jax.ShapeDtypeStruct((2, tokens, HEAD), f32),
        ]
    return pl.pallas_call(
        functools.partial(attend_kernel, first, last, count),
        grid_spec=pltpu.PrefetchScalarGridSpec(
            num_scalar_prefetch=1,
            grid=(2, tokens // BQ),
            in_specs=[q_spec, q_spec]
            + [kv_spec] * count
            + ([] if first else [acc_spec, top_spec]),
            out_specs=out_specs,
            scratch_shapes=[
                pltpu.VMEM((count * rows, 2 * HEAD), bf16),
                pltpu.VMEM((count * rows, 2 * HEAD), bf16),
            ],
        ),
        out_shape=out_shape,
        compiler_params=room(28),
        name="attend",
    )(where, own, sib, *kvs, *([] if first else state))


def merge_kernel(where_ref, keep_ref, got_ref, out_ref):
    def merged(mine, other):
        other = other.astype(f32)
        theirs = other[:, HEAD : HEAD + 1] + other[:, HEAD + 32 : HEAD + 33]
        theirs = theirs + other[:, HEAD + 64 : HEAD + 65]
        level = jnp.maximum(mine[:, HEAD:], theirs)
        a = jnp.exp2(mine[:, HEAD:] - level)
        b = jnp.exp2(theirs - level)
        return (mine[:, :HEAD] * a + other[:, :HEAD] * b) / (a + b)

    first_core = where_ref[0] == 0
    for z in range(keep_ref.shape[1]):
        own = merged(keep_ref[0, z], got_ref[1, z])
        sib = merged(keep_ref[1, z], got_ref[0, z])
        out_ref[z, :, :HEAD] = jnp.where(first_core, own, sib).astype(bf16)
        out_ref[z, :, HEAD:] = jnp.where(first_core, sib, own).astype(bf16)


def merge(where, keep, got):
    _, z, rows, _ = keep.shape
    return pl.pallas_call(
        merge_kernel,
        grid_spec=pltpu.PrefetchScalarGridSpec(
            num_scalar_prefetch=1,
            grid=(1,),
            in_specs=[pl.BlockSpec(keep.shape, lambda i, w: (0, 0, 0, 0))] * 2,
            out_specs=pl.BlockSpec((z, rows, 2 * HEAD), lambda i, w: (0, 0, 0)),
        ),
        out_shape=jax.ShapeDtypeStruct((z, rows, 2 * HEAD), bf16),
        compiler_params=room(8),
        name="merge",
    )(where, keep, got)


def swap_matrix(experts, blocks):
    count = experts * blocks * 2
    row = lax.broadcasted_iota(jnp.int32, (count, count), 0)
    col = lax.broadcasted_iota(jnp.int32, (count, count), 1)
    a, b, j = row // (blocks * 2), (row // 2) % blocks, row % 2
    return jnp.where(col == b * (experts * 2) + a * 2 + j, 1.0, 0.0).astype(bf16)


def pack(rows_of, out_ref, swap):
    peers = out_ref.shape[0]
    blocks = 16
    tails = []
    for k in range(blocks):
        block = rows_of(k)
        head = block[: peers * 8].reshape(peers, 8, HEAD)
        out_ref[:, k * 8 : (k + 1) * 8, :] = head.astype(bf16)
        tails.append(block[peers * 8 :])
    tail = jnp.concatenate(tails, axis=0).astype(bf16)
    turned = dot(swap, tail)
    out_ref[:, blocks * 8 :, :] = turned.reshape(peers, blocks * 2, HEAD).astype(bf16)


def unpack(in_ref, store, swap):
    peers = in_ref.shape[0]
    blocks = 16
    tail = in_ref[:, blocks * 8 :, :].astype(f32).reshape(peers * blocks * 2, HEAD).astype(bf16)
    turned = dot(swap, tail)
    for k in range(blocks):
        head = in_ref[:, k * 8 : (k + 1) * 8, :].astype(f32).reshape(peers * 8, HEAD)
        store(k, jnp.concatenate([head, turned[k * peers * 2 : (k + 1) * peers * 2]], axis=0))


def slot_of(expert, ordinal, experts):
    return jnp.where(ordinal < 8, expert * 8 + ordinal, experts * 8 + expert * 2 + ordinal - 8)


def project_kernel(
    a_ref, w_ref, res_ref, gain_ref, route_ref, route_t_ref, swap_ref, upd_ref, out_ref, held, sems
):
    steps, rows, depth = a_ref.shape
    copies = [
        pltpu.make_async_copy(
            w_ref.at[pl.ds(i * depth, depth)], held.at[pl.ds(i * depth, depth)], sems.at[i]
        )
        for i in range(steps)
    ]
    for copy in copies:
        copy.start()
    experts = out_ref.shape[0]
    earlier = lax.broadcasted_iota(jnp.int32, (rows, rows), 0)
    later = lax.broadcasted_iota(jnp.int32, (rows, rows), 1)
    slots = lax.broadcasted_iota(jnp.int32, (experts * 10, rows), 0)
    placing = jnp.zeros((experts * 10, rows), f32)
    for t in range(2):
        mine = route_t_ref[t : t + 1, :]
        ordinal = jnp.zeros((1, rows), jnp.int32)
        for u in range(2):
            before = (earlier < later) if u >= t else (earlier <= later)
            same = route_ref[:, u : u + 1] == mine
            ordinal += jnp.sum(jnp.where(before & same, 1, 0), axis=0, keepdims=True)
        placing += jnp.where(slots == slot_of(mine, ordinal, experts), 1.0, 0.0)
    acc = res_ref[...].astype(f32)
    for i in range(steps):
        copies[i].wait()
        acc += dot(a_ref[i], held[i * depth : (i + 1) * depth, :])
    updated = acc.astype(bf16)
    upd_ref[...] = updated
    wide = updated.astype(f32)
    mean = jnp.mean(wide * wide, axis=1, keepdims=True)
    normed = (wide * lax.rsqrt(mean + norm_eps) * gain_ref[...]).astype(bf16)
    sent = dot(placing.astype(bf16), normed)
    pack(lambda k: sent[:, k * HEAD : (k + 1) * HEAD], out_ref, swap_ref[...])


VMEM = pl.BlockSpec(memory_space=pltpu.VMEM)
HBM = pl.BlockSpec(memory_space=pltpu.HBM)


def project(attended, out_weight, residual, norm_gain, route, route_t, swap, peers):
    steps, rows, depth = attended.shape
    width = out_weight.shape[1]
    return pl.pallas_call(
        project_kernel,
        in_specs=[VMEM, HBM, VMEM, VMEM, VMEM, VMEM, VMEM],
        out_specs=[VMEM, VMEM],
        out_shape=[
            jax.ShapeDtypeStruct((rows, width), bf16),
            jax.ShapeDtypeStruct((peers, 160, HEAD), bf16),
        ],
        scratch_shapes=[
            pltpu.VMEM(out_weight.shape, bf16),
            pltpu.SemaphoreType.DMA((steps,)),
        ],
        compiler_params=room(56),
        name="project",
    )(attended, out_weight, residual, norm_gain, route, route_t, swap)


def rows_kernel(in_ref, swap_ref, x_ref):
    def store(k, block):
        x_ref[:, k * HEAD : (k + 1) * HEAD] = block.astype(bf16)

    unpack(in_ref, store, swap_ref[...])


def rows_in(arrived, swap):
    peers = arrived.shape[0]
    return pl.pallas_call(
        rows_kernel,
        in_specs=[VMEM, VMEM],
        out_specs=VMEM,
        out_shape=jax.ShapeDtypeStruct((peers * 10, 16 * HEAD), bf16),
        compiler_params=room(8),
        name="rows_in",
    )(arrived, swap)


FLIGHT = 6


def expert_kernel(own_ref, sib_ref, w_ref, keep_ref, send_ref, held, x, sems):
    blocks, _, width, _ = held.shape
    rows = keep_ref.shape[0]
    copies = [
        pltpu.make_async_copy(
            w_ref.at[i, pl.ds(0, 2)], held.at[i, pl.ds(0, 2)], sems.at[i]
        )
        for i in range(blocks)
    ] + [
        pltpu.make_async_copy(w_ref.at[i, 2], held.at[i, 2], sems.at[blocks + i])
        for i in range(blocks)
    ]
    for copy in copies[:FLIGHT]:
        copy.start()
    waiting = FLIGHT
    x[:rows, :] = own_ref[...]
    x[rows:, :] = sib_ref[...]
    parts = []
    for i in range(0, blocks, 2):
        pair = (i, i + 1)
        for j in pair:
            copies[j].wait()
        for copy in copies[waiting : waiting + 3]:
            copy.start()
        waiting += 3
        gate = dot(x[...], jnp.concatenate([held[j, 0] for j in pair], axis=1))
        up = dot(x[...], jnp.concatenate([held[j, 1] for j in pair], axis=1))
        parts.append((gate / (1.0 + jnp.exp(-gate)) * up).astype(bf16))
    hid = jnp.concatenate(parts, axis=1)
    for copy in copies[blocks:]:
        copy.wait()
    for k in range(0, width // HEAD, 2):
        down = jnp.concatenate(
            [
                jnp.concatenate(
                    [held[j, 2, c * HEAD : (c + 1) * HEAD, :] for j in range(blocks)], axis=0
                )
                for c in (k, k + 1)
            ],
            axis=1,
        )
        total = dot(hid, down)
        cols = slice(k * HEAD, (k + 2) * HEAD)
        keep_ref[:, cols] = total[:rows]
        send_ref[:, cols] = total[rows:].astype(bf16)


def expert(own, sib, weights):
    blocks, _, width, _ = weights.shape
    return pl.pallas_call(
        expert_kernel,
        in_specs=[VMEM, VMEM, HBM],
        out_specs=[VMEM, VMEM],
        out_shape=[
            jax.ShapeDtypeStruct((160, width), f32),
            jax.ShapeDtypeStruct((160, width), bf16),
        ],
        scratch_shapes=[
            pltpu.VMEM(weights.shape, bf16),
            pltpu.VMEM((320, width), bf16),
            pltpu.SemaphoreType.DMA((2 * blocks,)),
        ],
        compiler_params=room(50),
        name="expert",
    )(own, sib, weights)


def finish_kernel(keep_ref, got_ref, swap_ref, out_ref):
    def rows_of(k):
        cols = slice(k * HEAD, (k + 1) * HEAD)
        return keep_ref[:, cols] + got_ref[:, cols].astype(f32)

    pack(rows_of, out_ref, swap_ref[...])


def finish(keep, got, swap, peers):
    return pl.pallas_call(
        finish_kernel,
        in_specs=[VMEM] * 3,
        out_specs=VMEM,
        out_shape=jax.ShapeDtypeStruct((peers, 160, HEAD), bf16),
        compiler_params=room(12),
        name="finish",
    )(keep, got, swap)


def plan_kernel(route_ref, route_t_ref, score_ref, prob_ref, pick_ref, mix_ref, swap_ref):
    rows = route_ref.shape[0]
    experts = pick_ref.shape[2] // 10
    later = lax.broadcasted_iota(jnp.int32, (rows, rows), 0)
    earlier = lax.broadcasted_iota(jnp.int32, (rows, rows), 1)
    slots = lax.broadcasted_iota(jnp.int32, (rows, experts * 10), 1)
    scores = score_ref[...]
    raised = jnp.exp(scores - jnp.max(scores, axis=1, keepdims=True))
    mixing = prob_ref[...] * (raised / jnp.sum(raised, axis=1, keepdims=True))
    for t in range(2):
        mine = route_ref[:, t : t + 1]
        ordinal = jnp.zeros((rows, 1), jnp.int32)
        for u in range(2):
            before = (earlier < later) if u >= t else (earlier <= later)
            same = route_t_ref[u : u + 1, :] == mine
            ordinal += jnp.sum(jnp.where(before & same, 1, 0), axis=1, keepdims=True)
        placed = slots == slot_of(mine, ordinal, experts)
        pick_ref[t] = jnp.where(placed, 1.0, 0.0).astype(bf16)
        mix_ref[t] = jnp.broadcast_to(mixing[:, t : t + 1], (rows, HEAD))
    swap_ref[...] = swap_matrix(experts, 16)


def plan(route, route_t, scores, prob, experts):
    rows = route.shape[0]
    return pl.pallas_call(
        plan_kernel,
        in_specs=[VMEM] * 4,
        out_specs=[VMEM] * 3,
        out_shape=[
            jax.ShapeDtypeStruct((2, rows, experts * 10), bf16),
            jax.ShapeDtypeStruct((2, rows, HEAD), f32),
            jax.ShapeDtypeStruct((experts * 32, experts * 32), bf16),
        ],
        compiler_params=room(8),
        name="plan",
    )(route, route_t, scores, prob)


def mix_kernel(in_ref, upd_ref, pick_ref, mix_ref, swap_ref, out_ref):
    def store(k, block):
        block = block.astype(bf16)
        cols = slice(k * HEAD, (k + 1) * HEAD)
        combined = sum(dot(pick_ref[t], block) * mix_ref[t] for t in range(2))
        out_ref[:, cols] = (upd_ref[:, cols].astype(f32) + combined).astype(bf16)

    unpack(in_ref, store, swap_ref[...])


def mix(returned, updated, picks, mixing, swap):
    return pl.pallas_call(
        mix_kernel,
        in_specs=[VMEM] * 5,
        out_specs=VMEM,
        out_shape=jax.ShapeDtypeStruct(updated.shape, bf16),
        compiler_params=room(12),
        name="mix",
    )(returned, updated, picks, mixing, swap)


def shift(value, axis, by):
    size = lax.axis_size(axis)
    return lax.ppermute(value, axis, [(i, (i + by) % size) for i in range(size)])


def onward(value, axis):
    size = lax.axis_size(axis)
    pairs = []
    for i in range(size):
        pairs.append((2 * i, 2 * ((i + 1) % size)))
        pairs.append((2 * i + 1, 2 * ((i - 1) % size) + 1))
    return lax.ppermute(value, (axis, "core"), pairs)


def swap_cores(value):
    return lax.ppermute(value, "core", ((0, 1), (1, 0)))


def local(
    queries,
    keys,
    values,
    query_gain,
    key_gain,
    out_weight,
    residual,
    norm_gain,
    route_experts,
    expert_scores,
    group_prob,
    w_gate,
    w_up,
    w_down,
):
    peers = lax.axis_size(SP)
    core = lax.axis_index("core")
    z = lax.axis_index("z")
    seq = lax.axis_index(SP)
    tokens = queries.shape[0]

    where = jnp.stack([core, z // 2]).astype(jnp.int32)
    lane = jnp.arange(HEAD, dtype=jnp.int32)
    pair = (lane // 2) % (HEAD // 4)
    frequency = rope_base ** (-pair.astype(f32) * 4.0 / HEAD)
    grid_rows = tokens // GRID_W
    place = jnp.arange(grid_rows + GRID_W, dtype=jnp.int32)
    place = jnp.where(place < grid_rows, seq * grid_rows + place, place - grid_rows)
    angles = place.astype(f32)[:, None] * frequency[None, :]
    cosine = jnp.cos(angles)
    sine = jnp.sin(angles) * jnp.where(lane % 2 == 0, -1.0, 1.0)[None, :]

    weights = lax.all_gather(bundle(w_gate[0], w_up[0], w_down[0]), "z")
    route_t = route_experts.T
    picks, mixing, swap = plan(
        route_experts, route_t, expert_scores, group_prob[:, None], peers
    )
    own, kv_a, kv_b = prep(
        where, queries, keys, values, query_gain[None, :], key_gain[None, :], cosine, sine
    )
    ax = jnp.concatenate([kv_a] + [shift(kv_a, "x", d) for d in (1, -1, 2)], axis=0)
    by = jnp.concatenate([kv_b] + [shift(kv_b, "y", d) for d in (1, -1, 2)], axis=0)
    sib = swap_cores(own)
    a_next = [shift(ax, "y", 1), shift(ax, "y", -1)]
    b_next = [shift(by, "x", 1), shift(by, "x", -1)]
    state = attend(where, own, sib, [ax, by], None, False)
    state, a_next, b_next = lax.optimization_barrier((state, a_next, b_next))
    a_far = onward(jnp.where(core == 0, a_next[0], a_next[1]), "y")
    b_far = onward(jnp.where(core == 0, b_next[0], b_next[1]), "x")
    state = attend(where, own, sib, a_next + b_next, state, False)
    keep, send = attend(where, own, sib, [a_far, b_far], state, True)
    merged = merge(where, keep, swap_cores(send))
    attended = lax.all_to_all(merged, "z", 0, 0, tiled=True)
    updated, outgoing = project(
        attended, out_weight, residual, norm_gain[None, :], route_experts, route_t, swap, peers
    )
    arrived = lax.all_to_all(outgoing, SP, 0, 0, tiled=True)
    rows = rows_in(arrived, swap)
    keep, send = expert(rows, swap_cores(rows), weights)
    result = finish(keep, swap_cores(send), swap, peers)
    returned = lax.all_to_all(result, SP, 0, 0, tiled=True)
    return mix(returned, updated, picks, mixing, swap)


def solution(mesh):
    torus = Mesh(mesh.devices.reshape(4, 4, 8, 2), ("y", "x", "z", "core"))
    placed = (
        P(SP, TP),
        P(SP, None),
        P(SP, None),
        P(TP),
        P(),
        P(),
        P(SP_TP, None),
        P(),
        P(SP_TP, None),
        P(SP_TP, None),
        P(SP_TP),
        P(SP, None, TP),
        P(SP, None, TP),
        P(SP, TP, None),
    )
    return jax.shard_map(
        local, mesh=torus, in_specs=placed, out_specs=P(SP_TP, None), check_vma=False
    )
```

```python
import functools
import math

import jax
import jax.numpy as jnp
from jax import lax
from jax.experimental import pallas as pl
from jax.experimental.pallas import tpu as pltpu
from jax.sharding import Mesh
from jax.sharding import PartitionSpec as P

GRID_W = 64
HEAD = 128
SP = ("y", "x")
TP = ("z", "core")
SP_TP = ("y", "x", "z", "core")
rope_base = 10000.0
norm_eps = 1e-06
f32 = jnp.float32
bf16 = jnp.bfloat16


def room(mib):
    return pltpu.CompilerParams(vmem_limit_bytes=mib * 1024 * 1024)


def dot(a, b):
    return jnp.dot(a, b, preferred_element_type=f32)


def bundle_kernel(gate_ref, up_ref, down_ref, out_ref):
    units = gate_ref.shape[1]
    out_ref[0] = gate_ref[...]
    out_ref[1] = up_ref[...]
    for k in range(down_ref.shape[1] // HEAD):
        out_ref[2, k * units : (k + 1) * units, :] = down_ref[:, k * HEAD : (k + 1) * HEAD]


def bundle(gate, up, down):
    width, units = gate.shape
    rows = width // 2
    spec = pl.BlockSpec((rows, units), lambda i: (i, 0))
    return pl.pallas_call(
        bundle_kernel,
        grid=(2,),
        in_specs=[spec, spec, pl.BlockSpec((units, rows), lambda i: (0, i))],
        out_specs=pl.BlockSpec((3, rows, units), lambda i: (0, i, 0)),
        out_shape=jax.ShapeDtypeStruct((3, width, units), bf16),
        name="bundle",
    )(gate, up, down)


def prep_kernel(
    where_ref, q_ref, k_ref, v_ref, qg_ref, kg_ref, cos_ref, sin_ref, q_out, kv_a, kv_b
):
    lane = lax.broadcasted_iota(jnp.int32, (GRID_W, HEAD), 1)
    even = lane % 2 == 0
    from_row = lane < HEAD // 2
    col_cos = cos_ref[16:, :]
    col_sin = sin_ref[16:, :]

    def turn(vectors, gain, row_cos, row_sin):
        mean = jnp.mean(vectors * vectors, axis=-1, keepdims=True)
        u = vectors * lax.rsqrt(mean + norm_eps) * gain
        swapped = jnp.where(even, pltpu.roll(u, HEAD - 1, 1), pltpu.roll(u, 1, 1))
        cosine = jnp.where(from_row, row_cos, col_cos)
        sine = jnp.where(from_row, row_sin, col_sin)
        return u * cosine + swapped * sine

    for r in range(q_ref.shape[0] // GRID_W):
        rows = slice(r * GRID_W, (r + 1) * GRID_W)
        q_out[rows, :] = turn(
            q_ref[rows, :].astype(f32), qg_ref[...], cos_ref[r : r + 1, :], sin_ref[r : r + 1, :]
        ).astype(bf16)
    half = k_ref.shape[0] // GRID_W
    first = where_ref[0] * half
    for r in range(half):
        rows = slice(r * GRID_W, (r + 1) * GRID_W)
        row_cos = cos_ref[pl.ds(first + r, 1), :]
        row_sin = sin_ref[pl.ds(first + r, 1), :]
        kv_out = kv_a if r < half // 2 else kv_b
        at = r % (half // 2)
        rows_out = slice(at * GRID_W, (at + 1) * GRID_W)
        kv_out[rows_out, :HEAD] = turn(
            k_ref[rows, :].astype(f32), kg_ref[...], row_cos, row_sin
        ).astype(bf16)
        kv_out[rows_out, HEAD:] = v_ref[rows, :]


def prep(where, queries, keys, values, query_gain, key_gain, cosine, sine):
    tokens = queries.shape[0]
    half = tokens // 2
    whole = lambda shape: pl.BlockSpec(shape, lambda i, w: (0, 0))
    part = pl.BlockSpec((half, HEAD), lambda i, w: (w[0], w[1]))
    return pl.pallas_call(
        prep_kernel,
        grid_spec=pltpu.PrefetchScalarGridSpec(
            num_scalar_prefetch=1,
            grid=(1,),
            in_specs=[
                whole((tokens, HEAD)),
                part,
                part,
                whole((1, HEAD)),
                whole((1, HEAD)),
                whole(cosine.shape),
                whole(sine.shape),
            ],
            out_specs=[
                whole((tokens, HEAD)),
                whole((half // 2, 2 * HEAD)),
                whole((half // 2, 2 * HEAD)),
            ],
        ),
        out_shape=[
            jax.ShapeDtypeStruct((tokens, HEAD), bf16),
            jax.ShapeDtypeStruct((half // 2, 2 * HEAD), bf16),
            jax.ShapeDtypeStruct((half // 2, 2 * HEAD), bf16),
        ],
        name="prep",
    )(where, queries, keys, values, query_gain, key_gain, cosine, sine)


BQ = 256


def attend_kernel(first, last, count, where_ref, own_ref, sib_ref, *refs):
    kv_refs, refs = refs[:count], refs[count:]
    if not first:
        acc_in, top_in, *refs = refs
    out_a, out_b, kk, vv = refs
    rows = kv_refs[0].shape[0]

    @pl.when((pl.program_id(0) == 0) & (pl.program_id(1) == 0))
    def _():
        for b in range(count):
            span = slice(b * rows, (b + 1) * rows)
            k = kv_refs[b][:, :HEAD]
            kk[span, :HEAD] = k
            kk[span, HEAD:] = k
            vv[span, :HEAD] = kv_refs[b][:, HEAD:]
            vv[span, HEAD:] = jnp.ones((rows, HEAD), bf16)

    q = jnp.where(pl.program_id(0) == 0, own_ref[...].astype(f32), sib_ref[...].astype(f32))
    scaled = q * (HEAD ** (-0.5) * math.log2(math.e))
    high = scaled.astype(bf16)
    low = (scaled - high.astype(f32)).astype(bf16)
    pair = jnp.concatenate([high, low], axis=1)
    top = None if first else jnp.max(top_in[0], axis=1, keepdims=True)
    acc = None if first else acc_in[0]
    for j in range(count):
        span = slice(j * rows, (j + 1) * rows)
        s = lax.dot_general(
            pair, kk[span, :], (((1,), (1,)), ((), ())), preferred_element_type=f32
        )
        block_top = jnp.max(s, axis=1, keepdims=True)
        new_top = block_top if top is None else jnp.maximum(top, block_top)
        raised = jnp.exp2(s - new_top).astype(bf16)
        part = dot(raised, vv[span, :])
        acc = part if top is None else acc * jnp.exp2(top - new_top) + part
        top = new_top
    if not last:
        out_a[0] = acc
        out_b[0] = jnp.broadcast_to(top, (top.shape[0], HEAD))
        return
    total = acc[:, HEAD:]
    normal = acc[:, :HEAD] / total
    level = top + jnp.log2(total)
    first_core = where_ref[0] == 0
    lane = lax.broadcasted_iota(jnp.int32, (64, HEAD), 1)
    for z in range(BQ // 128):
        a = slice(z * 128, z * 128 + 64)
        b = slice(z * 128 + 64, z * 128 + 128)
        out_a[0, z, :, :HEAD] = jnp.where(first_core, normal[a], normal[b])
        out_a[0, z, :, HEAD:] = jnp.where(first_core, level[a], level[b])
        out_b[0, z, :, :HEAD] = jnp.where(first_core, normal[b], normal[a]).astype(bf16)
        sent = jnp.where(first_core, level[b], level[a])
        l0 = sent.astype(bf16).astype(f32)
        l1 = (sent - l0).astype(bf16).astype(f32)
        l2 = sent - l0 - l1
        out_b[0, z, :, HEAD:] = jnp.where(lane < 32, l0, jnp.where(lane < 64, l1, l2)).astype(bf16)


def attend(where, own, sib, kvs, state, last):
    tokens = own.shape[0]
    rows = kvs[0].shape[0]
    first = state is None
    count = len(kvs)
    q_spec = pl.BlockSpec((BQ, HEAD), lambda h, i, w: (i, 0))
    kv_spec = pl.BlockSpec((rows, 2 * HEAD), lambda h, i, w: (0, 0))
    acc_spec = pl.BlockSpec((1, BQ, 2 * HEAD), lambda h, i, w: (h, i, 0))
    top_spec = pl.BlockSpec((1, BQ, HEAD), lambda h, i, w: (h, i, 0))
    if last:
        out_spec = pl.BlockSpec((1, BQ // 128, 64, 2 * HEAD), lambda h, i, w: (h, i, 0, 0))
        out_specs = [out_spec, out_spec]
        out_shape = [
            jax.ShapeDtypeStruct((2, tokens // 128, 64, 2 * HEAD), f32),
            jax.ShapeDtypeStruct((2, tokens // 128, 64, 2 * HEAD), bf16),
        ]
    else:
        out_specs = [acc_spec, top_spec]
        out_shape = [
            jax.ShapeDtypeStruct((2, tokens, 2 * HEAD), f32),
            jax.ShapeDtypeStruct((2, tokens, HEAD), f32),
        ]
    return pl.pallas_call(
        functools.partial(attend_kernel, first, last, count),
        grid_spec=pltpu.PrefetchScalarGridSpec(
            num_scalar_prefetch=1,
            grid=(2, tokens // BQ),
            in_specs=[q_spec, q_spec]
            + [kv_spec] * count
            + ([] if first else [acc_spec, top_spec]),
            out_specs=out_specs,
            scratch_shapes=[
                pltpu.VMEM((count * rows, 2 * HEAD), bf16),
                pltpu.VMEM((count * rows, 2 * HEAD), bf16),
            ],
        ),
        out_shape=out_shape,
        compiler_params=room(28),
        name="attend",
    )(where, own, sib, *kvs, *([] if first else state))


def merge_kernel(where_ref, keep_ref, got_ref, out_ref):
    def merged(mine, other):
        other = other.astype(f32)
        theirs = other[:, HEAD : HEAD + 1] + other[:, HEAD + 32 : HEAD + 33]
        theirs = theirs + other[:, HEAD + 64 : HEAD + 65]
        level = jnp.maximum(mine[:, HEAD:], theirs)
        a = jnp.exp2(mine[:, HEAD:] - level)
        b = jnp.exp2(theirs - level)
        return (mine[:, :HEAD] * a + other[:, :HEAD] * b) / (a + b)

    first_core = where_ref[0] == 0
    for z in range(keep_ref.shape[1]):
        own = merged(keep_ref[0, z], got_ref[1, z])
        sib = merged(keep_ref[1, z], got_ref[0, z])
        out_ref[z, :, :HEAD] = jnp.where(first_core, own, sib).astype(bf16)
        out_ref[z, :, HEAD:] = jnp.where(first_core, sib, own).astype(bf16)


def merge(where, keep, got):
    _, z, rows, _ = keep.shape
    return pl.pallas_call(
        merge_kernel,
        grid_spec=pltpu.PrefetchScalarGridSpec(
            num_scalar_prefetch=1,
            grid=(1,),
            in_specs=[pl.BlockSpec(keep.shape, lambda i, w: (0, 0, 0, 0))] * 2,
            out_specs=pl.BlockSpec((z, rows, 2 * HEAD), lambda i, w: (0, 0, 0)),
        ),
        out_shape=jax.ShapeDtypeStruct((z, rows, 2 * HEAD), bf16),
        compiler_params=room(8),
        name="merge",
    )(where, keep, got)


def swap_matrix(experts, blocks):
    count = experts * blocks * 2
    row = lax.broadcasted_iota(jnp.int32, (count, count), 0)
    col = lax.broadcasted_iota(jnp.int32, (count, count), 1)
    a, b, j = row // (blocks * 2), (row // 2) % blocks, row % 2
    return jnp.where(col == b * (experts * 2) + a * 2 + j, 1.0, 0.0).astype(bf16)


def pack(rows_of, out_ref, swap):
    peers = out_ref.shape[0]
    blocks = 16
    tails = []
    for k in range(blocks):
        block = rows_of(k)
        head = block[: peers * 8].reshape(peers, 8, HEAD)
        out_ref[:, k * 8 : (k + 1) * 8, :] = head.astype(bf16)
        tails.append(block[peers * 8 :])
    tail = jnp.concatenate(tails, axis=0).astype(bf16)
    turned = dot(swap, tail)
    out_ref[:, blocks * 8 :, :] = turned.reshape(peers, blocks * 2, HEAD).astype(bf16)


def unpack(in_ref, store, swap):
    peers = in_ref.shape[0]
    blocks = 16
    tail = in_ref[:, blocks * 8 :, :].astype(f32).reshape(peers * blocks * 2, HEAD).astype(bf16)
    turned = dot(swap, tail)
    for k in range(blocks):
        head = in_ref[:, k * 8 : (k + 1) * 8, :].astype(f32).reshape(peers * 8, HEAD)
        store(k, jnp.concatenate([head, turned[k * peers * 2 : (k + 1) * peers * 2]], axis=0))


def slot_of(expert, ordinal, experts):
    return jnp.where(ordinal < 8, expert * 8 + ordinal, experts * 8 + expert * 2 + ordinal - 8)


def project_kernel(
    a_ref, w_ref, res_ref, gain_ref, route_ref, route_t_ref, swap_ref, upd_ref, out_ref, held, sems
):
    steps, rows, depth = a_ref.shape
    copies = [
        pltpu.make_async_copy(
            w_ref.at[pl.ds(i * depth, depth)], held.at[pl.ds(i * depth, depth)], sems.at[i]
        )
        for i in range(steps)
    ]
    for copy in copies:
        copy.start()
    experts = out_ref.shape[0]
    earlier = lax.broadcasted_iota(jnp.int32, (rows, rows), 0)
    later = lax.broadcasted_iota(jnp.int32, (rows, rows), 1)
    slots = lax.broadcasted_iota(jnp.int32, (experts * 10, rows), 0)
    placing = jnp.zeros((experts * 10, rows), f32)
    for t in range(2):
        mine = route_t_ref[t : t + 1, :]
        ordinal = jnp.zeros((1, rows), jnp.int32)
        for u in range(2):
            before = (earlier < later) if u >= t else (earlier <= later)
            same = route_ref[:, u : u + 1] == mine
            ordinal += jnp.sum(jnp.where(before & same, 1, 0), axis=0, keepdims=True)
        placing += jnp.where(slots == slot_of(mine, ordinal, experts), 1.0, 0.0)
    acc = res_ref[...].astype(f32)
    for i in range(steps):
        copies[i].wait()
        acc += dot(a_ref[i], held[i * depth : (i + 1) * depth, :])
    updated = acc.astype(bf16)
    upd_ref[...] = updated
    wide = updated.astype(f32)
    mean = jnp.mean(wide * wide, axis=1, keepdims=True)
    normed = (wide * lax.rsqrt(mean + norm_eps) * gain_ref[...]).astype(bf16)
    sent = dot(placing.astype(bf16), normed)
    pack(lambda k: sent[:, k * HEAD : (k + 1) * HEAD], out_ref, swap_ref[...])


VMEM = pl.BlockSpec(memory_space=pltpu.VMEM)
HBM = pl.BlockSpec(memory_space=pltpu.HBM)


def project(attended, out_weight, residual, norm_gain, route, route_t, swap, peers):
    steps, rows, _ = attended.shape
    width = out_weight.shape[1]
    return pl.pallas_call(
        project_kernel,
        in_specs=[VMEM, HBM, VMEM, VMEM, VMEM, VMEM, VMEM],
        out_specs=[VMEM, VMEM],
        out_shape=[
            jax.ShapeDtypeStruct((rows, width), bf16),
            jax.ShapeDtypeStruct((peers, 160, HEAD), bf16),
        ],
        scratch_shapes=[
            pltpu.VMEM(out_weight.shape, bf16),
            pltpu.SemaphoreType.DMA((steps,)),
        ],
        compiler_params=room(56),
        name="project",
    )(attended, out_weight, residual, norm_gain, route, route_t, swap)


def rows_kernel(in_ref, swap_ref, x_ref):
    def store(k, block):
        x_ref[:, k * HEAD : (k + 1) * HEAD] = block.astype(bf16)

    unpack(in_ref, store, swap_ref[...])


def rows_in(arrived, swap):
    peers = arrived.shape[0]
    return pl.pallas_call(
        rows_kernel,
        in_specs=[VMEM, VMEM],
        out_specs=VMEM,
        out_shape=jax.ShapeDtypeStruct((peers * 10, 16 * HEAD), bf16),
        compiler_params=room(8),
        name="rows_in",
    )(arrived, swap)


def expert_kernel(counts, more, last, own_ref, sib_ref, *refs):
    pieces = []
    for count in counts:
        pieces.append(refs[:count])
        refs = refs[count:]
    if more:
        acc_ref, refs = refs[0], refs[1:]
    out_refs, (x, total) = refs[:-2], refs[-2:]
    rows = own_ref.shape[0]
    width = own_ref.shape[1]

    def take(piece, at, length):
        found, base = [], 0
        for ref in piece:
            lo, hi = max(at - base, 0), min(at + length - base, ref.shape[0])
            if lo < hi:
                found.append(ref[lo:hi, :])
            base += ref.shape[0]
        return found[0] if len(found) == 1 else jnp.concatenate(found, axis=0)

    x[:rows, :] = own_ref[...]
    x[rows:, :] = sib_ref[...]
    parts = []
    for i in range(0, len(pieces), 2):
        pair = pieces[i : i + 2]
        gate = dot(x[...], jnp.concatenate([take(p, 0, width) for p in pair], axis=1))
        up = dot(x[...], jnp.concatenate([take(p, width, width) for p in pair], axis=1))
        parts.append((gate / (1.0 + jnp.exp(-gate)) * up).astype(bf16))
    hid = jnp.concatenate(parts, axis=1)
    for k in range(0, width // HEAD, 2):
        down = jnp.concatenate(
            [
                jnp.concatenate([take(p, 2 * width + c * HEAD, HEAD) for p in pieces], axis=0)
                for c in (k, k + 1)
            ],
            axis=1,
        )
        cols = slice(k * HEAD, (k + 2) * HEAD)
        total[...] = dot(hid, down)
        if more:
            total[...] += acc_ref[:, cols]
        if last:
            keep_ref, send_ref = out_refs
            keep_ref[:, cols] = total[:rows, :]
            send_ref[:, cols] = total[rows:, :].astype(bf16)
        else:
            out_refs[0][:, cols] = total[...]


def expert(own, sib, pieces, acc, last):
    rows, width = own.shape
    flat = [array for piece in pieces for array in piece]
    if last:
        out_shape = [
            jax.ShapeDtypeStruct((rows, width), f32),
            jax.ShapeDtypeStruct((rows, width), bf16),
        ]
    else:
        out_shape = [jax.ShapeDtypeStruct((2 * rows, width), f32)]
    more = [] if acc is None else [acc]
    return pl.pallas_call(
        functools.partial(
            expert_kernel, tuple(len(piece) for piece in pieces), acc is not None, last
        ),
        in_specs=[VMEM] * (2 + len(flat) + len(more)),
        out_specs=[VMEM] * len(out_shape),
        out_shape=out_shape,
        scratch_shapes=[
            pltpu.VMEM((2 * rows, width), bf16),
            pltpu.VMEM((2 * rows, 2 * HEAD), f32),
        ],
        compiler_params=room(40),
        name="expert",
    )(own, sib, *flat, *more)


def finish_kernel(keep_ref, got_ref, swap_ref, out_ref):
    def rows_of(k):
        cols = slice(k * HEAD, (k + 1) * HEAD)
        return keep_ref[:, cols] + got_ref[:, cols].astype(f32)

    pack(rows_of, out_ref, swap_ref[...])


def finish(keep, got, swap, peers):
    return pl.pallas_call(
        finish_kernel,
        in_specs=[VMEM] * 3,
        out_specs=VMEM,
        out_shape=jax.ShapeDtypeStruct((peers, 160, HEAD), bf16),
        compiler_params=room(12),
        name="finish",
    )(keep, got, swap)


def plan_kernel(route_ref, route_t_ref, score_ref, prob_ref, pick_ref, mix_ref, swap_ref):
    rows = route_ref.shape[0]
    experts = pick_ref.shape[2] // 10
    later = lax.broadcasted_iota(jnp.int32, (rows, rows), 0)
    earlier = lax.broadcasted_iota(jnp.int32, (rows, rows), 1)
    slots = lax.broadcasted_iota(jnp.int32, (rows, experts * 10), 1)
    scores = score_ref[...]
    raised = jnp.exp(scores - jnp.max(scores, axis=1, keepdims=True))
    mixing = prob_ref[...] * (raised / jnp.sum(raised, axis=1, keepdims=True))
    for t in range(2):
        mine = route_ref[:, t : t + 1]
        ordinal = jnp.zeros((rows, 1), jnp.int32)
        for u in range(2):
            before = (earlier < later) if u >= t else (earlier <= later)
            same = route_t_ref[u : u + 1, :] == mine
            ordinal += jnp.sum(jnp.where(before & same, 1, 0), axis=1, keepdims=True)
        placed = slots == slot_of(mine, ordinal, experts)
        pick_ref[t] = jnp.where(placed, 1.0, 0.0).astype(bf16)
        mix_ref[t] = jnp.broadcast_to(mixing[:, t : t + 1], (rows, HEAD))
    swap_ref[...] = swap_matrix(experts, 16)


def plan(route, route_t, scores, prob, experts):
    rows = route.shape[0]
    return pl.pallas_call(
        plan_kernel,
        in_specs=[VMEM] * 4,
        out_specs=[VMEM] * 3,
        out_shape=[
            jax.ShapeDtypeStruct((2, rows, experts * 10), bf16),
            jax.ShapeDtypeStruct((2, rows, HEAD), f32),
            jax.ShapeDtypeStruct((experts * 32, experts * 32), bf16),
        ],
        compiler_params=room(8),
        name="plan",
    )(route, route_t, scores, prob)


def mix_kernel(in_ref, upd_ref, pick_ref, mix_ref, swap_ref, out_ref):
    def store(k, block):
        block = block.astype(bf16)
        cols = slice(k * HEAD, (k + 1) * HEAD)
        combined = sum(dot(pick_ref[t], block) * mix_ref[t] for t in range(2))
        out_ref[:, cols] = (upd_ref[:, cols].astype(f32) + combined).astype(bf16)

    unpack(in_ref, store, swap_ref[...])


def mix(returned, updated, picks, mixing, swap):
    return pl.pallas_call(
        mix_kernel,
        in_specs=[VMEM] * 5,
        out_specs=VMEM,
        out_shape=jax.ShapeDtypeStruct(updated.shape, bf16),
        compiler_params=room(12),
        name="mix",
    )(returned, updated, picks, mixing, swap)


def shift(value, axis, by):
    size = lax.axis_size(axis)
    return lax.ppermute(value, axis, [(i, (i + by) % size) for i in range(size)])


def onward(value, axis):
    size = lax.axis_size(axis)
    pairs = []
    for i in range(size):
        pairs.append((2 * i, 2 * ((i + 1) % size)))
        pairs.append((2 * i + 1, 2 * ((i - 1) % size) + 1))
    return lax.ppermute(value, (axis, "core"), pairs)


def swap_cores(value):
    return lax.ppermute(value, "core", ((0, 1), (1, 0)))


def local(
    queries,
    keys,
    values,
    query_gain,
    key_gain,
    out_weight,
    residual,
    norm_gain,
    route_experts,
    expert_scores,
    group_prob,
    w_gate,
    w_up,
    w_down,
):
    peers = lax.axis_size(SP)
    core = lax.axis_index("core")
    z = lax.axis_index("z")
    seq = lax.axis_index(SP)
    tokens = queries.shape[0]

    where = jnp.stack([core, z // 2]).astype(jnp.int32)
    lane = jnp.arange(HEAD, dtype=jnp.int32)
    pair = (lane // 2) % (HEAD // 4)
    frequency = rope_base ** (-pair.astype(f32) * 4.0 / HEAD)
    grid_rows = tokens // GRID_W
    place = jnp.arange(grid_rows + GRID_W, dtype=jnp.int32)
    place = jnp.where(place < grid_rows, seq * grid_rows + place, place - grid_rows)
    angles = place.astype(f32)[:, None] * frequency[None, :]
    cosine = jnp.cos(angles)
    sine = jnp.sin(angles) * jnp.where(lane % 2 == 0, -1.0, 1.0)[None, :]

    w0 = bundle(w_gate[0], w_up[0], w_down[0]).reshape(-1, HEAD)
    w1p, w1m = shift(w0, "z", 1), shift(w0, "z", -1)
    route_t = route_experts.T
    picks, mixing, swap = plan(
        route_experts, route_t, expert_scores, group_prob[:, None], peers
    )
    own, kv_a, kv_b = prep(
        where, queries, keys, values, query_gain[None, :], key_gain[None, :], cosine, sine
    )
    ax = jnp.concatenate([kv_a] + [shift(kv_a, "x", d) for d in (1, -1, 2)], axis=0)
    by = jnp.concatenate([kv_b] + [shift(kv_b, "y", d) for d in (1, -1, 2)], axis=0)
    sib = swap_cores(own)
    a_next = [shift(ax, "y", 1), shift(ax, "y", -1)]
    b_next = [shift(by, "x", 1), shift(by, "x", -1)]
    state = attend(where, own, sib, [ax, by], None, False)
    w1p, w1m, state, a_next, b_next = lax.optimization_barrier((w1p, w1m, state, a_next, b_next))
    w2p, w2m = shift(w1p, "z", 1), shift(w1m, "z", -1)
    a_far = onward(jnp.where(core == 0, a_next[0], a_next[1]), "y")
    b_far = onward(jnp.where(core == 0, b_next[0], b_next[1]), "x")
    state = attend(where, own, sib, a_next + b_next, state, False)
    keep, send = attend(where, own, sib, [a_far, b_far], state, True)
    got = swap_cores(send)
    w2p, w2m, _ = lax.optimization_barrier((w2p, w2m, keep))
    third = w0.shape[0] // 3
    w3p = [shift(w2p[:third], "z", 1)]
    w3m = [shift(w2m[:third], "z", -1)]
    merged = merge(where, keep, got)
    attended = lax.all_to_all(merged, "z", 0, 0, tiled=True)
    rest_p, rest_m, attended = lax.optimization_barrier((w2p[third:], w2m[third:], attended))
    w3p.append(shift(rest_p, "z", 1))
    w3m.append(shift(rest_m, "z", -1))
    updated, outgoing = project(
        attended, out_weight, residual, norm_gain[None, :], route_experts, route_t, swap, peers
    )
    arrived = lax.all_to_all(outgoing, SP, 0, 0, tiled=True)
    w3p, w3m, arrived = lax.optimization_barrier((w3p, w3m, arrived))
    w4 = [
        shift(w3p[0], "z", 1),
        shift(w3p[1][: third // 2], "z", 1),
        shift(w3m[1][third // 2 :], "z", -1),
    ]
    rows = rows_in(arrived, swap)
    sib_rows = swap_cores(rows)
    (acc,) = expert(rows, sib_rows, [[w0], [w1p], [w1m], [w2p], [w2m], w3p], None, False)
    keep, send = expert(rows, sib_rows, [w3m, w4], acc, True)
    result = finish(keep, swap_cores(send), swap, peers)
    returned = lax.all_to_all(result, SP, 0, 0, tiled=True)
    return mix(returned, updated, picks, mixing, swap)


def solution(mesh):
    torus = Mesh(mesh.devices.reshape(4, 4, 8, 2), ("y", "x", "z", "core"))
    placed = (
        P(SP, TP),
        P(SP, None),
        P(SP, None),
        P(TP),
        P(),
        P(),
        P(SP_TP, None),
        P(),
        P(SP_TP, None),
        P(SP_TP, None),
        P(SP_TP),
        P(SP, None, TP),
        P(SP, None, TP),
        P(SP, TP, None),
    )
    return jax.shard_map(
        local, mesh=torus, in_specs=placed, out_specs=P(SP_TP, None), check_vma=False
    )
```

```python
import functools
import math

import jax
import jax.numpy as jnp
from jax import lax
from jax.experimental import pallas as pl
from jax.experimental.pallas import tpu as pltpu
from jax.sharding import Mesh
from jax.sharding import PartitionSpec as P

GRID_W = 64
HEAD = 128
SP = ("y", "x")
TP = ("z", "core")
SP_TP = ("y", "x", "z", "core")
rope_base = 10000.0
norm_eps = 1e-06
f32 = jnp.float32
bf16 = jnp.bfloat16


def room(mib):
    return pltpu.CompilerParams(vmem_limit_bytes=mib * 1024 * 1024)


def dot(a, b):
    return jnp.dot(a, b, preferred_element_type=f32)


def bundle_kernel(gate_ref, up_ref, down_ref, out_ref):
    units = gate_ref.shape[1]
    out_ref[0] = gate_ref[...]
    out_ref[1] = up_ref[...]
    for k in range(down_ref.shape[1] // HEAD):
        out_ref[2, k * units : (k + 1) * units, :] = down_ref[:, k * HEAD : (k + 1) * HEAD]


def bundle(gate, up, down):
    width, units = gate.shape
    rows = width // 2
    spec = pl.BlockSpec((rows, units), lambda i: (i, 0))
    return pl.pallas_call(
        bundle_kernel,
        grid=(2,),
        in_specs=[spec, spec, pl.BlockSpec((units, rows), lambda i: (0, i))],
        out_specs=pl.BlockSpec((3, rows, units), lambda i: (0, i, 0)),
        out_shape=jax.ShapeDtypeStruct((3, width, units), bf16),
        name="bundle",
    )(gate, up, down)


def prep_kernel(
    where_ref, q_ref, k_ref, v_ref, qg_ref, kg_ref, cos_ref, sin_ref, q_out, kv_a, kv_b
):
    lane = lax.broadcasted_iota(jnp.int32, (GRID_W, HEAD), 1)
    even = lane % 2 == 0
    from_row = lane < HEAD // 2
    col_cos = cos_ref[16:, :]
    col_sin = sin_ref[16:, :]

    def turn(vectors, gain, row_cos, row_sin):
        mean = jnp.mean(vectors * vectors, axis=-1, keepdims=True)
        u = vectors * lax.rsqrt(mean + norm_eps) * gain
        swapped = jnp.where(even, pltpu.roll(u, HEAD - 1, 1), pltpu.roll(u, 1, 1))
        cosine = jnp.where(from_row, row_cos, col_cos)
        sine = jnp.where(from_row, row_sin, col_sin)
        return u * cosine + swapped * sine

    for r in range(q_ref.shape[0] // GRID_W):
        rows = slice(r * GRID_W, (r + 1) * GRID_W)
        q_out[rows, :] = turn(
            q_ref[rows, :].astype(f32), qg_ref[...], cos_ref[r : r + 1, :], sin_ref[r : r + 1, :]
        ).astype(bf16)
    half = k_ref.shape[0] // GRID_W
    first = where_ref[0] * half
    for r in range(half):
        rows = slice(r * GRID_W, (r + 1) * GRID_W)
        row_cos = cos_ref[pl.ds(first + r, 1), :]
        row_sin = sin_ref[pl.ds(first + r, 1), :]
        kv_out = kv_a if r < half // 2 else kv_b
        at = r % (half // 2)
        rows_out = slice(at * GRID_W, (at + 1) * GRID_W)
        kv_out[rows_out, :HEAD] = turn(
            k_ref[rows, :].astype(f32), kg_ref[...], row_cos, row_sin
        ).astype(bf16)
        kv_out[rows_out, HEAD:] = v_ref[rows, :]


def prep(where, queries, keys, values, query_gain, key_gain, cosine, sine):
    tokens = queries.shape[0]
    half = tokens // 2
    whole = lambda shape: pl.BlockSpec(shape, lambda i, w: (0, 0))
    part = pl.BlockSpec((half, HEAD), lambda i, w: (w[0], w[1]))
    return pl.pallas_call(
        prep_kernel,
        grid_spec=pltpu.PrefetchScalarGridSpec(
            num_scalar_prefetch=1,
            grid=(1,),
            in_specs=[
                whole((tokens, HEAD)),
                part,
                part,
                whole((1, HEAD)),
                whole((1, HEAD)),
                whole(cosine.shape),
                whole(sine.shape),
            ],
            out_specs=[
                whole((tokens, HEAD)),
                whole((half // 2, 2 * HEAD)),
                whole((half // 2, 2 * HEAD)),
            ],
        ),
        out_shape=[
            jax.ShapeDtypeStruct((tokens, HEAD), bf16),
            jax.ShapeDtypeStruct((half // 2, 2 * HEAD), bf16),
            jax.ShapeDtypeStruct((half // 2, 2 * HEAD), bf16),
        ],
        name="prep",
    )(where, queries, keys, values, query_gain, key_gain, cosine, sine)


def stack_kernel(*refs):
    *parts, out_a, out_b = refs
    half = len(parts) // 2
    rows = parts[0].shape[0]
    for i in range(half):
        out_a[i * rows : (i + 1) * rows, :] = parts[i][...]
        out_b[i * rows : (i + 1) * rows, :] = parts[half + i][...]


def stack(parts_a, parts_b):
    rows, width = parts_a[0].shape
    out = jax.ShapeDtypeStruct((len(parts_a) * rows, width), bf16)
    return pl.pallas_call(
        stack_kernel,
        in_specs=[pl.BlockSpec(memory_space=pltpu.VMEM)] * (2 * len(parts_a)),
        out_specs=[pl.BlockSpec(memory_space=pltpu.VMEM)] * 2,
        out_shape=[out, out],
        compiler_params=room(8),
        name="stack",
    )(*parts_a, *parts_b)


BQ = 256


def attend_kernel(first, last, count, where_ref, own_ref, sib_ref, *refs):
    kv_refs, refs = refs[:count], refs[count:]
    if not first:
        acc_in, top_in, *refs = refs
    out_a, out_b, kk, vv = refs
    rows = kv_refs[0].shape[0]

    @pl.when((pl.program_id(0) == 0) & (pl.program_id(1) == 0))
    def _():
        for b in range(count):
            span = slice(b * rows, (b + 1) * rows)
            k = kv_refs[b][:, :HEAD]
            kk[span, :HEAD] = k
            kk[span, HEAD:] = k
            vv[span, :HEAD] = kv_refs[b][:, HEAD:]
            vv[span, HEAD:] = jnp.ones((rows, HEAD), bf16)

    q = jnp.where(pl.program_id(0) == 0, own_ref[...].astype(f32), sib_ref[...].astype(f32))
    scaled = q * (HEAD ** (-0.5) * math.log2(math.e))
    high = scaled.astype(bf16)
    low = (scaled - high.astype(f32)).astype(bf16)
    pair = jnp.concatenate([high, low], axis=1)
    top = None if first else jnp.max(top_in[0], axis=1, keepdims=True)
    acc = None if first else acc_in[0]
    for j in range(count):
        span = slice(j * rows, (j + 1) * rows)
        s = lax.dot_general(
            pair, kk[span, :], (((1,), (1,)), ((), ())), preferred_element_type=f32
        )
        block_top = jnp.max(s, axis=1, keepdims=True)
        new_top = block_top if top is None else jnp.maximum(top, block_top)
        raised = jnp.exp2(s - new_top).astype(bf16)
        part = dot(raised, vv[span, :])
        acc = part if top is None else acc * jnp.exp2(top - new_top) + part
        top = new_top
    if not last:
        out_a[0] = acc
        out_b[0] = jnp.broadcast_to(top, (top.shape[0], HEAD))
        return
    total = acc[:, HEAD:]
    normal = acc[:, :HEAD] / total
    level = top + jnp.log2(total)
    first_core = where_ref[0] == 0
    lane = lax.broadcasted_iota(jnp.int32, (64, HEAD), 1)
    for z in range(BQ // 128):
        a = slice(z * 128, z * 128 + 64)
        b = slice(z * 128 + 64, z * 128 + 128)
        out_a[0, z, :, :HEAD] = jnp.where(first_core, normal[a], normal[b])
        out_a[0, z, :, HEAD:] = jnp.where(first_core, level[a], level[b])
        out_b[0, z, :, :HEAD] = jnp.where(first_core, normal[b], normal[a]).astype(bf16)
        sent = jnp.where(first_core, level[b], level[a])
        l0 = sent.astype(bf16).astype(f32)
        l1 = (sent - l0).astype(bf16).astype(f32)
        l2 = sent - l0 - l1
        out_b[0, z, :, HEAD:] = jnp.where(lane < 32, l0, jnp.where(lane < 64, l1, l2)).astype(bf16)


def attend(where, own, sib, kvs, state, last):
    tokens = own.shape[0]
    rows = kvs[0].shape[0]
    first = state is None
    count = len(kvs)
    q_spec = pl.BlockSpec((BQ, HEAD), lambda h, i, w: (i, 0))
    kv_spec = pl.BlockSpec((rows, 2 * HEAD), lambda h, i, w: (0, 0))
    acc_spec = pl.BlockSpec((1, BQ, 2 * HEAD), lambda h, i, w: (h, i, 0))
    top_spec = pl.BlockSpec((1, BQ, HEAD), lambda h, i, w: (h, i, 0))
    if last:
        out_spec = pl.BlockSpec((1, BQ // 128, 64, 2 * HEAD), lambda h, i, w: (h, i, 0, 0))
        out_specs = [out_spec, out_spec]
        out_shape = [
            jax.ShapeDtypeStruct((2, tokens // 128, 64, 2 * HEAD), f32),
            jax.ShapeDtypeStruct((2, tokens // 128, 64, 2 * HEAD), bf16),
        ]
    else:
        out_specs = [acc_spec, top_spec]
        out_shape = [
            jax.ShapeDtypeStruct((2, tokens, 2 * HEAD), f32),
            jax.ShapeDtypeStruct((2, tokens, HEAD), f32),
        ]
    return pl.pallas_call(
        functools.partial(attend_kernel, first, last, count),
        grid_spec=pltpu.PrefetchScalarGridSpec(
            num_scalar_prefetch=1,
            grid=(2, tokens // BQ),
            in_specs=[q_spec, q_spec]
            + [kv_spec] * count
            + ([] if first else [acc_spec, top_spec]),
            out_specs=out_specs,
            scratch_shapes=[
                pltpu.VMEM((count * rows, 2 * HEAD), bf16),
                pltpu.VMEM((count * rows, 2 * HEAD), bf16),
            ],
        ),
        out_shape=out_shape,
        compiler_params=room(28),
        name="attend",
    )(where, own, sib, *kvs, *([] if first else state))


def merge_kernel(where_ref, keep_ref, got_ref, out_ref):
    def merged(mine, other):
        other = other.astype(f32)
        theirs = other[:, HEAD : HEAD + 1] + other[:, HEAD + 32 : HEAD + 33]
        theirs = theirs + other[:, HEAD + 64 : HEAD + 65]
        level = jnp.maximum(mine[:, HEAD:], theirs)
        a = jnp.exp2(mine[:, HEAD:] - level)
        b = jnp.exp2(theirs - level)
        return (mine[:, :HEAD] * a + other[:, :HEAD] * b) / (a + b)

    first_core = where_ref[0] == 0
    for z in range(keep_ref.shape[1]):
        own = merged(keep_ref[0, z], got_ref[1, z])
        sib = merged(keep_ref[1, z], got_ref[0, z])
        out_ref[z, :, :HEAD] = jnp.where(first_core, own, sib).astype(bf16)
        out_ref[z, :, HEAD:] = jnp.where(first_core, sib, own).astype(bf16)


def merge(where, keep, got):
    _, z, rows, _ = keep.shape
    return pl.pallas_call(
        merge_kernel,
        grid_spec=pltpu.PrefetchScalarGridSpec(
            num_scalar_prefetch=1,
            grid=(1,),
            in_specs=[pl.BlockSpec(keep.shape, lambda i, w: (0, 0, 0, 0))] * 2,
            out_specs=pl.BlockSpec((z, rows, 2 * HEAD), lambda i, w: (0, 0, 0)),
        ),
        out_shape=jax.ShapeDtypeStruct((z, rows, 2 * HEAD), bf16),
        compiler_params=room(8),
        name="merge",
    )(where, keep, got)


def swap_matrix(experts, blocks):
    count = experts * blocks * 2
    row = lax.broadcasted_iota(jnp.int32, (count, count), 0)
    col = lax.broadcasted_iota(jnp.int32, (count, count), 1)
    a, b, j = row // (blocks * 2), (row // 2) % blocks, row % 2
    return jnp.where(col == b * (experts * 2) + a * 2 + j, 1.0, 0.0).astype(bf16)


def pack(rows_of, out_ref, swap):
    peers = out_ref.shape[0]
    blocks = 16
    tails = []
    for k in range(blocks):
        block = rows_of(k)
        head = block[: peers * 8].reshape(peers, 8, HEAD)
        out_ref[:, k * 8 : (k + 1) * 8, :] = head.astype(bf16)
        tails.append(block[peers * 8 :])
    tail = jnp.concatenate(tails, axis=0).astype(bf16)
    turned = dot(swap, tail)
    out_ref[:, blocks * 8 :, :] = turned.reshape(peers, blocks * 2, HEAD).astype(bf16)


def unpack(in_ref, store, swap):
    peers = in_ref.shape[0]
    blocks = 16
    tail = in_ref[:, blocks * 8 :, :].astype(f32).reshape(peers * blocks * 2, HEAD).astype(bf16)
    turned = dot(swap, tail)
    for k in range(blocks):
        head = in_ref[:, k * 8 : (k + 1) * 8, :].astype(f32).reshape(peers * 8, HEAD)
        store(k, jnp.concatenate([head, turned[k * peers * 2 : (k + 1) * peers * 2]], axis=0))


def slot_of(expert, ordinal, experts):
    return jnp.where(ordinal < 8, expert * 8 + ordinal, experts * 8 + expert * 2 + ordinal - 8)


def project_kernel(
    a_ref, w_ref, res_ref, gain_ref, route_ref, route_t_ref, swap_ref, upd_ref, out_ref, held, sems
):
    steps, rows, depth = a_ref.shape
    copies = [
        pltpu.make_async_copy(
            w_ref.at[pl.ds(i * depth, depth)], held.at[pl.ds(i * depth, depth)], sems.at[i]
        )
        for i in range(steps)
    ]
    for copy in copies:
        copy.start()
    experts = out_ref.shape[0]
    earlier = lax.broadcasted_iota(jnp.int32, (rows, rows), 0)
    later = lax.broadcasted_iota(jnp.int32, (rows, rows), 1)
    slots = lax.broadcasted_iota(jnp.int32, (experts * 10, rows), 0)
    placing = jnp.zeros((experts * 10, rows), f32)
    for t in range(2):
        mine = route_t_ref[t : t + 1, :]
        ordinal = jnp.zeros((1, rows), jnp.int32)
        for u in range(2):
            before = (earlier < later) if u >= t else (earlier <= later)
            same = route_ref[:, u : u + 1] == mine
            ordinal += jnp.sum(jnp.where(before & same, 1, 0), axis=0, keepdims=True)
        placing += jnp.where(slots == slot_of(mine, ordinal, experts), 1.0, 0.0)
    acc = res_ref[...].astype(f32)
    for i in range(steps):
        copies[i].wait()
        acc += dot(a_ref[i], held[i * depth : (i + 1) * depth, :])
    updated = acc.astype(bf16)
    upd_ref[...] = updated
    wide = updated.astype(f32)
    mean = jnp.mean(wide * wide, axis=1, keepdims=True)
    normed = (wide * lax.rsqrt(mean + norm_eps) * gain_ref[...]).astype(bf16)
    sent = dot(placing.astype(bf16), normed)
    pack(lambda k: sent[:, k * HEAD : (k + 1) * HEAD], out_ref, swap_ref[...])


VMEM = pl.BlockSpec(memory_space=pltpu.VMEM)
HBM = pl.BlockSpec(memory_space=pltpu.HBM)


def project(attended, out_weight, residual, norm_gain, route, route_t, swap, peers):
    steps, rows, _ = attended.shape
    width = out_weight.shape[1]
    return pl.pallas_call(
        project_kernel,
        in_specs=[VMEM, HBM, VMEM, VMEM, VMEM, VMEM, VMEM],
        out_specs=[VMEM, VMEM],
        out_shape=[
            jax.ShapeDtypeStruct((rows, width), bf16),
            jax.ShapeDtypeStruct((peers, 160, HEAD), bf16),
        ],
        scratch_shapes=[
            pltpu.VMEM(out_weight.shape, bf16),
            pltpu.SemaphoreType.DMA((steps,)),
        ],
        compiler_params=room(56),
        name="project",
    )(attended, out_weight, residual, norm_gain, route, route_t, swap)


def rows_kernel(in_ref, swap_ref, x_ref):
    def store(k, block):
        x_ref[:, k * HEAD : (k + 1) * HEAD] = block.astype(bf16)

    unpack(in_ref, store, swap_ref[...])


def rows_in(arrived, swap):
    peers = arrived.shape[0]
    return pl.pallas_call(
        rows_kernel,
        in_specs=[VMEM, VMEM],
        out_specs=VMEM,
        out_shape=jax.ShapeDtypeStruct((peers * 10, 16 * HEAD), bf16),
        compiler_params=room(8),
        name="rows_in",
    )(arrived, swap)


def expert_kernel(counts, more, last, own_ref, sib_ref, *refs):
    pieces = []
    for count in counts:
        pieces.append(refs[:count])
        refs = refs[count:]
    if more:
        acc_ref, refs = refs[0], refs[1:]
    out_refs, (x, total) = refs[:-2], refs[-2:]
    rows = own_ref.shape[0]
    width = own_ref.shape[1]

    def take(piece, at, length):
        found, base = [], 0
        for ref in piece:
            lo, hi = max(at - base, 0), min(at + length - base, ref.shape[0])
            if lo < hi:
                found.append(ref[lo:hi, :])
            base += ref.shape[0]
        return found[0] if len(found) == 1 else jnp.concatenate(found, axis=0)

    x[:rows, :] = own_ref[...]
    x[rows:, :] = sib_ref[...]
    parts = []
    for i in range(0, len(pieces), 2):
        pair = pieces[i : i + 2]
        gate = dot(x[...], jnp.concatenate([take(p, 0, width) for p in pair], axis=1))
        up = dot(x[...], jnp.concatenate([take(p, width, width) for p in pair], axis=1))
        parts.append((gate / (1.0 + jnp.exp(-gate)) * up).astype(bf16))
    hid = jnp.concatenate(parts, axis=1)
    for k in range(0, width // HEAD, 2):
        down = jnp.concatenate(
            [
                jnp.concatenate([take(p, 2 * width + c * HEAD, HEAD) for p in pieces], axis=0)
                for c in (k, k + 1)
            ],
            axis=1,
        )
        cols = slice(k * HEAD, (k + 2) * HEAD)
        total[...] = dot(hid, down)
        if more:
            total[...] += acc_ref[:, cols]
        if last:
            keep_ref, send_ref = out_refs
            keep_ref[:, cols] = total[:rows, :]
            send_ref[:, cols] = total[rows:, :].astype(bf16)
        else:
            out_refs[0][:, cols] = total[...]


def expert(own, sib, pieces, acc, last):
    rows, width = own.shape
    flat = [array for piece in pieces for array in piece]
    if last:
        out_shape = [
            jax.ShapeDtypeStruct((rows, width), f32),
            jax.ShapeDtypeStruct((rows, width), bf16),
        ]
    else:
        out_shape = [jax.ShapeDtypeStruct((2 * rows, width), f32)]
    more = [] if acc is None else [acc]
    return pl.pallas_call(
        functools.partial(
            expert_kernel, tuple(len(piece) for piece in pieces), acc is not None, last
        ),
        in_specs=[VMEM] * (2 + len(flat) + len(more)),
        out_specs=[VMEM] * len(out_shape),
        out_shape=out_shape,
        scratch_shapes=[
            pltpu.VMEM((2 * rows, width), bf16),
            pltpu.VMEM((2 * rows, 2 * HEAD), f32),
        ],
        compiler_params=room(40),
        name="expert",
    )(own, sib, *flat, *more)


def finish_kernel(keep_ref, got_ref, swap_ref, out_ref):
    def rows_of(k):
        cols = slice(k * HEAD, (k + 1) * HEAD)
        return keep_ref[:, cols] + got_ref[:, cols].astype(f32)

    pack(rows_of, out_ref, swap_ref[...])


def finish(keep, got, swap, peers):
    return pl.pallas_call(
        finish_kernel,
        in_specs=[VMEM] * 3,
        out_specs=VMEM,
        out_shape=jax.ShapeDtypeStruct((peers, 160, HEAD), bf16),
        compiler_params=room(12),
        name="finish",
    )(keep, got, swap)


def plan_kernel(route_ref, route_t_ref, score_ref, prob_ref, pick_ref, mix_ref, swap_ref):
    rows = route_ref.shape[0]
    experts = pick_ref.shape[2] // 10
    later = lax.broadcasted_iota(jnp.int32, (rows, rows), 0)
    earlier = lax.broadcasted_iota(jnp.int32, (rows, rows), 1)
    slots = lax.broadcasted_iota(jnp.int32, (rows, experts * 10), 1)
    scores = score_ref[...]
    raised = jnp.exp(scores - jnp.max(scores, axis=1, keepdims=True))
    mixing = prob_ref[...] * (raised / jnp.sum(raised, axis=1, keepdims=True))
    for t in range(2):
        mine = route_ref[:, t : t + 1]
        ordinal = jnp.zeros((rows, 1), jnp.int32)
        for u in range(2):
            before = (earlier < later) if u >= t else (earlier <= later)
            same = route_t_ref[u : u + 1, :] == mine
            ordinal += jnp.sum(jnp.where(before & same, 1, 0), axis=1, keepdims=True)
        placed = slots == slot_of(mine, ordinal, experts)
        pick_ref[t] = jnp.where(placed, 1.0, 0.0).astype(bf16)
        mix_ref[t] = jnp.broadcast_to(mixing[:, t : t + 1], (rows, HEAD))
    swap_ref[...] = swap_matrix(experts, 16)


def plan(route, route_t, scores, prob, experts):
    rows = route.shape[0]
    return pl.pallas_call(
        plan_kernel,
        in_specs=[VMEM] * 4,
        out_specs=[VMEM] * 3,
        out_shape=[
            jax.ShapeDtypeStruct((2, rows, experts * 10), bf16),
            jax.ShapeDtypeStruct((2, rows, HEAD), f32),
            jax.ShapeDtypeStruct((experts * 32, experts * 32), bf16),
        ],
        compiler_params=room(8),
        name="plan",
    )(route, route_t, scores, prob)


def mix_kernel(in_ref, upd_ref, pick_ref, mix_ref, swap_ref, out_ref):
    def store(k, block):
        block = block.astype(bf16)
        cols = slice(k * HEAD, (k + 1) * HEAD)
        combined = sum(dot(pick_ref[t], block) * mix_ref[t] for t in range(2))
        out_ref[:, cols] = (upd_ref[:, cols].astype(f32) + combined).astype(bf16)

    unpack(in_ref, store, swap_ref[...])


def mix(returned, updated, picks, mixing, swap):
    return pl.pallas_call(
        mix_kernel,
        in_specs=[VMEM] * 5,
        out_specs=VMEM,
        out_shape=jax.ShapeDtypeStruct(updated.shape, bf16),
        compiler_params=room(12),
        name="mix",
    )(returned, updated, picks, mixing, swap)


def shift(value, axis, by):
    size = lax.axis_size(axis)
    return lax.ppermute(value, axis, [(i, (i + by) % size) for i in range(size)])


def onward(value, axis):
    size = lax.axis_size(axis)
    pairs = []
    for i in range(size):
        pairs.append((2 * i, 2 * ((i + 1) % size)))
        pairs.append((2 * i + 1, 2 * ((i - 1) % size) + 1))
    return lax.ppermute(value, (axis, "core"), pairs)


def swap_cores(value):
    return lax.ppermute(value, "core", ((0, 1), (1, 0)))


def local(
    queries,
    keys,
    values,
    query_gain,
    key_gain,
    out_weight,
    residual,
    norm_gain,
    route_experts,
    expert_scores,
    group_prob,
    w_gate,
    w_up,
    w_down,
):
    peers = lax.axis_size(SP)
    core = lax.axis_index("core")
    z = lax.axis_index("z")
    seq = lax.axis_index(SP)
    tokens = queries.shape[0]

    where = jnp.stack([core, z // 2]).astype(jnp.int32)
    lane = jnp.arange(HEAD, dtype=jnp.int32)
    pair = (lane // 2) % (HEAD // 4)
    frequency = rope_base ** (-pair.astype(f32) * 4.0 / HEAD)
    grid_rows = tokens // GRID_W
    place = jnp.arange(grid_rows + GRID_W, dtype=jnp.int32)
    place = jnp.where(place < grid_rows, seq * grid_rows + place, place - grid_rows)
    angles = place.astype(f32)[:, None] * frequency[None, :]
    cosine = jnp.cos(angles)
    sine = jnp.sin(angles) * jnp.where(lane % 2 == 0, -1.0, 1.0)[None, :]

    w0 = bundle(w_gate[0], w_up[0], w_down[0]).reshape(-1, HEAD)
    w1p, w1m = shift(w0, "z", 1), shift(w0, "z", -1)
    route_t = route_experts.T
    picks, mixing, swap = plan(
        route_experts, route_t, expert_scores, group_prob[:, None], peers
    )
    own, kv_a, kv_b = prep(
        where, queries, keys, values, query_gain[None, :], key_gain[None, :], cosine, sine
    )
    ax, by = stack(
        [kv_a] + [shift(kv_a, "x", d) for d in (1, -1, 2)],
        [kv_b] + [shift(kv_b, "y", d) for d in (1, -1, 2)],
    )
    sib = swap_cores(own)
    a_next = [shift(ax, "y", 1), shift(ax, "y", -1)]
    b_next = [shift(by, "x", 1), shift(by, "x", -1)]
    state = attend(where, own, sib, [ax, by], None, False)
    w1p, w1m, state, a_next, b_next = lax.optimization_barrier((w1p, w1m, state, a_next, b_next))
    w2p, w2m = shift(w1p, "z", 1), shift(w1m, "z", -1)
    a_far = onward(jnp.where(core == 0, a_next[0], a_next[1]), "y")
    b_far = onward(jnp.where(core == 0, b_next[0], b_next[1]), "x")
    state = attend(where, own, sib, a_next + b_next, state, False)
    keep, send = attend(where, own, sib, [a_far, b_far], state, True)
    got = swap_cores(send)
    w2p, w2m, _ = lax.optimization_barrier((w2p, w2m, keep))
    third = w0.shape[0] // 3
    w3p = [shift(w2p[:third], "z", 1)]
    w3m = [shift(w2m[:third], "z", -1)]
    merged = merge(where, keep, got)
    attended = lax.all_to_all(merged, "z", 0, 0, tiled=True)
    rest_p, rest_m, attended = lax.optimization_barrier((w2p[third:], w2m[third:], attended))
    w3p.append(shift(rest_p, "z", 1))
    w3m.append(shift(rest_m, "z", -1))
    w4 = [shift(w3p[0][: third // 2], "z", 1), shift(w3m[0][third // 2 :], "z", -1)]
    updated, outgoing = project(
        attended,
        out_weight,
        residual,
        norm_gain[None, :],
        route_experts,
        route_t,
        swap,
        peers,
    )
    arrived = lax.all_to_all(outgoing, SP, 0, 0, tiled=True)
    rest_p, rest_m, arrived = lax.optimization_barrier((w3p[1], w3m[1], arrived))
    w4 += [shift(rest_p[:third], "z", 1), shift(rest_m[third:], "z", -1)]
    rows = rows_in(arrived, swap)
    sib_rows = swap_cores(rows)
    (acc,) = expert(rows, sib_rows, [[w0], [w1p], [w1m], [w2p], [w2m], w3p], None, False)
    keep, send = expert(rows, sib_rows, [w3m, w4], acc, True)
    result = finish(keep, swap_cores(send), swap, peers)
    returned = lax.all_to_all(result, SP, 0, 0, tiled=True)
    return mix(returned, updated, picks, mixing, swap)


def solution(mesh):
    torus = Mesh(mesh.devices.reshape(4, 4, 8, 2), ("y", "x", "z", "core"))
    placed = (
        P(SP, TP),
        P(SP, None),
        P(SP, None),
        P(TP),
        P(),
        P(),
        P(SP_TP, None),
        P(),
        P(SP_TP, None),
        P(SP_TP, None),
        P(SP_TP),
        P(SP, None, TP),
        P(SP, None, TP),
        P(SP, TP, None),
    )
    return jax.shard_map(
        local, mesh=torus, in_specs=placed, out_specs=P(SP_TP, None), check_vma=False
    )
```

```python
import functools
import math

import jax
import jax.numpy as jnp
from jax import lax
from jax.experimental import pallas as pl
from jax.experimental.pallas import tpu as pltpu
from jax.sharding import Mesh
from jax.sharding import PartitionSpec as P

GRID_W = 64
HEAD = 128
SP = ("y", "x")
TP = ("z", "core")
SP_TP = ("y", "x", "z", "core")
rope_base = 10000.0
norm_eps = 1e-06
f32 = jnp.float32
bf16 = jnp.bfloat16


def room(mib):
    return pltpu.CompilerParams(vmem_limit_bytes=mib * 1024 * 1024)


def dot(a, b):
    return jnp.dot(a, b, preferred_element_type=f32)


def bundle_kernel(gate_ref, up_ref, down_ref, out_ref):
    units = gate_ref.shape[1]
    out_ref[0] = gate_ref[...]
    out_ref[1] = up_ref[...]
    for k in range(down_ref.shape[1] // HEAD):
        out_ref[2, k * units : (k + 1) * units, :] = down_ref[:, k * HEAD : (k + 1) * HEAD]


def bundle(gate, up, down):
    width, units = gate.shape
    rows = width // 2
    spec = pl.BlockSpec((rows, units), lambda i: (i, 0))
    return pl.pallas_call(
        bundle_kernel,
        grid=(2,),
        in_specs=[spec, spec, pl.BlockSpec((units, rows), lambda i: (0, i))],
        out_specs=pl.BlockSpec((3, rows, units), lambda i: (0, i, 0)),
        out_shape=jax.ShapeDtypeStruct((3, width, units), bf16),
        name="bundle",
    )(gate, up, down)


def prep_kernel(
    where_ref, q_ref, k_ref, v_ref, qg_ref, kg_ref, cos_ref, sin_ref, q_out, kv_a, kv_b
):
    lane = lax.broadcasted_iota(jnp.int32, (GRID_W, HEAD), 1)
    even = lane % 2 == 0
    from_row = lane < HEAD // 2
    col_cos = cos_ref[16:, :]
    col_sin = sin_ref[16:, :]

    def turn(vectors, gain, row_cos, row_sin):
        mean = jnp.mean(vectors * vectors, axis=-1, keepdims=True)
        u = vectors * lax.rsqrt(mean + norm_eps) * gain
        swapped = jnp.where(even, pltpu.roll(u, HEAD - 1, 1), pltpu.roll(u, 1, 1))
        cosine = jnp.where(from_row, row_cos, col_cos)
        sine = jnp.where(from_row, row_sin, col_sin)
        return u * cosine + swapped * sine

    for r in range(q_ref.shape[0] // GRID_W):
        rows = slice(r * GRID_W, (r + 1) * GRID_W)
        q_out[rows, :] = turn(
            q_ref[rows, :].astype(f32), qg_ref[...], cos_ref[r : r + 1, :], sin_ref[r : r + 1, :]
        ).astype(bf16)
    half = k_ref.shape[0] // GRID_W
    first = where_ref[0] * half
    for r in range(half):
        rows = slice(r * GRID_W, (r + 1) * GRID_W)
        row_cos = cos_ref[pl.ds(first + r, 1), :]
        row_sin = sin_ref[pl.ds(first + r, 1), :]
        kv_out = kv_a if r < half // 2 else kv_b
        at = r % (half // 2)
        rows_out = slice(at * GRID_W, (at + 1) * GRID_W)
        kv_out[rows_out, :HEAD] = turn(
            k_ref[rows, :].astype(f32), kg_ref[...], row_cos, row_sin
        ).astype(bf16)
        kv_out[rows_out, HEAD:] = v_ref[rows, :]


def prep(where, queries, keys, values, query_gain, key_gain, cosine, sine):
    tokens = queries.shape[0]
    half = tokens // 2
    whole = lambda shape: pl.BlockSpec(shape, lambda i, w: (0, 0))
    part = pl.BlockSpec((half, HEAD), lambda i, w: (w[0], w[1]))
    return pl.pallas_call(
        prep_kernel,
        grid_spec=pltpu.PrefetchScalarGridSpec(
            num_scalar_prefetch=1,
            grid=(1,),
            in_specs=[
                whole((tokens, HEAD)),
                part,
                part,
                whole((1, HEAD)),
                whole((1, HEAD)),
                whole(cosine.shape),
                whole(sine.shape),
            ],
            out_specs=[
                whole((tokens, HEAD)),
                whole((half // 2, 2 * HEAD)),
                whole((half // 2, 2 * HEAD)),
            ],
        ),
        out_shape=[
            jax.ShapeDtypeStruct((tokens, HEAD), bf16),
            jax.ShapeDtypeStruct((half // 2, 2 * HEAD), bf16),
            jax.ShapeDtypeStruct((half // 2, 2 * HEAD), bf16),
        ],
        name="prep",
    )(where, queries, keys, values, query_gain, key_gain, cosine, sine)


def stack_kernel(*refs):
    *parts, out_a, out_b = refs
    half = len(parts) // 2
    rows = parts[0].shape[0]
    for i in range(half):
        out_a[i * rows : (i + 1) * rows, :] = parts[i][...]
        out_b[i * rows : (i + 1) * rows, :] = parts[half + i][...]


def stack(parts_a, parts_b):
    rows, width = parts_a[0].shape
    out = jax.ShapeDtypeStruct((len(parts_a) * rows, width), bf16)
    return pl.pallas_call(
        stack_kernel,
        in_specs=[pl.BlockSpec(memory_space=pltpu.VMEM)] * (2 * len(parts_a)),
        out_specs=[pl.BlockSpec(memory_space=pltpu.VMEM)] * 2,
        out_shape=[out, out],
        compiler_params=room(8),
        name="stack",
    )(*parts_a, *parts_b)


BQ = 256


def attend_kernel(first, last, count, where_ref, own_ref, sib_ref, *refs):
    kv_refs, refs = refs[:count], refs[count:]
    if not first:
        acc_in, top_in, *refs = refs
    out_a, out_b, kk, vv = refs
    rows = kv_refs[0].shape[0]

    @pl.when((pl.program_id(0) == 0) & (pl.program_id(1) == 0))
    def _():
        for b in range(count):
            span = slice(b * rows, (b + 1) * rows)
            k = kv_refs[b][:, :HEAD]
            kk[span, :HEAD] = k
            kk[span, HEAD:] = k
            vv[span, :HEAD] = kv_refs[b][:, HEAD:]
            vv[span, HEAD:] = jnp.ones((rows, HEAD), bf16)

    q = jnp.where(pl.program_id(0) == 0, own_ref[...].astype(f32), sib_ref[...].astype(f32))
    scaled = q * (HEAD ** (-0.5) * math.log2(math.e))
    high = scaled.astype(bf16)
    low = (scaled - high.astype(f32)).astype(bf16)
    pair = jnp.concatenate([high, low], axis=1)
    top = None if first else jnp.max(top_in[0], axis=1, keepdims=True)
    acc = None if first else acc_in[0]
    for j in range(count):
        span = slice(j * rows, (j + 1) * rows)
        s = lax.dot_general(
            pair, kk[span, :], (((1,), (1,)), ((), ())), preferred_element_type=f32
        )
        block_top = jnp.max(s, axis=1, keepdims=True)
        new_top = block_top if top is None else jnp.maximum(top, block_top)
        raised = jnp.exp2(s - new_top).astype(bf16)
        part = dot(raised, vv[span, :])
        acc = part if top is None else acc * jnp.exp2(top - new_top) + part
        top = new_top
    if not last:
        out_a[0] = acc
        out_b[0] = jnp.broadcast_to(top, (top.shape[0], HEAD))
        return
    total = acc[:, HEAD:]
    normal = acc[:, :HEAD] / total
    level = top + jnp.log2(total)
    first_core = where_ref[0] == 0
    lane = lax.broadcasted_iota(jnp.int32, (64, HEAD), 1)
    for z in range(BQ // 128):
        a = slice(z * 128, z * 128 + 64)
        b = slice(z * 128 + 64, z * 128 + 128)
        out_a[0, z, :, :HEAD] = jnp.where(first_core, normal[a], normal[b])
        out_a[0, z, :, HEAD:] = jnp.where(first_core, level[a], level[b])
        out_b[0, z, :, :HEAD] = jnp.where(first_core, normal[b], normal[a]).astype(bf16)
        sent = jnp.where(first_core, level[b], level[a])
        l0 = sent.astype(bf16).astype(f32)
        l1 = (sent - l0).astype(bf16).astype(f32)
        l2 = sent - l0 - l1
        out_b[0, z, :, HEAD:] = jnp.where(lane < 32, l0, jnp.where(lane < 64, l1, l2)).astype(bf16)


def attend(where, own, sib, kvs, state, last):
    tokens = own.shape[0]
    rows = kvs[0].shape[0]
    first = state is None
    count = len(kvs)
    q_spec = pl.BlockSpec((BQ, HEAD), lambda h, i, w: (i, 0))
    kv_spec = pl.BlockSpec((rows, 2 * HEAD), lambda h, i, w: (0, 0))
    acc_spec = pl.BlockSpec((1, BQ, 2 * HEAD), lambda h, i, w: (h, i, 0))
    top_spec = pl.BlockSpec((1, BQ, HEAD), lambda h, i, w: (h, i, 0))
    if last:
        out_spec = pl.BlockSpec((1, BQ // 128, 64, 2 * HEAD), lambda h, i, w: (h, i, 0, 0))
        out_specs = [out_spec, out_spec]
        out_shape = [
            jax.ShapeDtypeStruct((2, tokens // 128, 64, 2 * HEAD), f32),
            jax.ShapeDtypeStruct((2, tokens // 128, 64, 2 * HEAD), bf16),
        ]
    else:
        out_specs = [acc_spec, top_spec]
        out_shape = [
            jax.ShapeDtypeStruct((2, tokens, 2 * HEAD), f32),
            jax.ShapeDtypeStruct((2, tokens, HEAD), f32),
        ]
    return pl.pallas_call(
        functools.partial(attend_kernel, first, last, count),
        grid_spec=pltpu.PrefetchScalarGridSpec(
            num_scalar_prefetch=1,
            grid=(2, tokens // BQ),
            in_specs=[q_spec, q_spec]
            + [kv_spec] * count
            + ([] if first else [acc_spec, top_spec]),
            out_specs=out_specs,
            scratch_shapes=[
                pltpu.VMEM((count * rows, 2 * HEAD), bf16),
                pltpu.VMEM((count * rows, 2 * HEAD), bf16),
            ],
        ),
        out_shape=out_shape,
        compiler_params=room(28),
        name="attend",
    )(where, own, sib, *kvs, *([] if first else state))


def merge_kernel(where_ref, keep_ref, got_ref, out_ref):
    def merged(mine, other):
        other = other.astype(f32)
        theirs = other[:, HEAD : HEAD + 1] + other[:, HEAD + 32 : HEAD + 33]
        theirs = theirs + other[:, HEAD + 64 : HEAD + 65]
        level = jnp.maximum(mine[:, HEAD:], theirs)
        a = jnp.exp2(mine[:, HEAD:] - level)
        b = jnp.exp2(theirs - level)
        return (mine[:, :HEAD] * a + other[:, :HEAD] * b) / (a + b)

    first_core = where_ref[0] == 0
    for z in range(keep_ref.shape[1]):
        own = merged(keep_ref[0, z], got_ref[1, z])
        sib = merged(keep_ref[1, z], got_ref[0, z])
        out_ref[z, :, :HEAD] = jnp.where(first_core, own, sib).astype(bf16)
        out_ref[z, :, HEAD:] = jnp.where(first_core, sib, own).astype(bf16)


def merge(where, keep, got):
    _, z, rows, _ = keep.shape
    return pl.pallas_call(
        merge_kernel,
        grid_spec=pltpu.PrefetchScalarGridSpec(
            num_scalar_prefetch=1,
            grid=(1,),
            in_specs=[pl.BlockSpec(keep.shape, lambda i, w: (0, 0, 0, 0))] * 2,
            out_specs=pl.BlockSpec((z, rows, 2 * HEAD), lambda i, w: (0, 0, 0)),
        ),
        out_shape=jax.ShapeDtypeStruct((z, rows, 2 * HEAD), bf16),
        compiler_params=room(8),
        name="merge",
    )(where, keep, got)


def swap_matrix(experts, blocks):
    count = experts * blocks * 2
    row = lax.broadcasted_iota(jnp.int32, (count, count), 0)
    col = lax.broadcasted_iota(jnp.int32, (count, count), 1)
    a, b, j = row // (blocks * 2), (row // 2) % blocks, row % 2
    return jnp.where(col == b * (experts * 2) + a * 2 + j, 1.0, 0.0).astype(bf16)


def pack(rows_of, out_ref, swap):
    peers = out_ref.shape[0]
    blocks = 16
    tails = []
    for k in range(blocks):
        block = rows_of(k)
        head = block[: peers * 8].reshape(peers, 8, HEAD)
        out_ref[:, k * 8 : (k + 1) * 8, :] = head.astype(bf16)
        tails.append(block[peers * 8 :])
    tail = jnp.concatenate(tails, axis=0).astype(bf16)
    turned = dot(swap, tail)
    out_ref[:, blocks * 8 :, :] = turned.reshape(peers, blocks * 2, HEAD).astype(bf16)


def unpack(in_ref, store, swap):
    peers = in_ref.shape[0]
    blocks = 16
    tail = in_ref[:, blocks * 8 :, :].astype(f32).reshape(peers * blocks * 2, HEAD).astype(bf16)
    turned = dot(swap, tail)
    for k in range(blocks):
        head = in_ref[:, k * 8 : (k + 1) * 8, :].astype(f32).reshape(peers * 8, HEAD)
        store(k, jnp.concatenate([head, turned[k * peers * 2 : (k + 1) * peers * 2]], axis=0))


def slot_of(expert, ordinal, experts):
    return jnp.where(ordinal < 8, expert * 8 + ordinal, experts * 8 + expert * 2 + ordinal - 8)


def project_kernel(
    a_ref, w_ref, res_ref, gain_ref, route_ref, route_t_ref, swap_ref, upd_ref, out_ref, held, sems
):
    steps, rows, depth = a_ref.shape
    copies = [
        pltpu.make_async_copy(
            w_ref.at[pl.ds(i * depth, depth)], held.at[pl.ds(i * depth, depth)], sems.at[i]
        )
        for i in range(steps)
    ]
    for copy in copies:
        copy.start()
    experts = out_ref.shape[0]
    earlier = lax.broadcasted_iota(jnp.int32, (rows, rows), 0)
    later = lax.broadcasted_iota(jnp.int32, (rows, rows), 1)
    slots = lax.broadcasted_iota(jnp.int32, (experts * 10, rows), 0)
    placing = jnp.zeros((experts * 10, rows), f32)
    for t in range(2):
        mine = route_t_ref[t : t + 1, :]
        ordinal = jnp.zeros((1, rows), jnp.int32)
        for u in range(2):
            before = (earlier < later) if u >= t else (earlier <= later)
            same = route_ref[:, u : u + 1] == mine
            ordinal += jnp.sum(jnp.where(before & same, 1, 0), axis=0, keepdims=True)
        placing += jnp.where(slots == slot_of(mine, ordinal, experts), 1.0, 0.0)
    acc = res_ref[...].astype(f32)
    for i in range(steps):
        copies[i].wait()
        acc += dot(a_ref[i], held[i * depth : (i + 1) * depth, :])
    updated = acc.astype(bf16)
    upd_ref[...] = updated
    wide = updated.astype(f32)
    mean = jnp.mean(wide * wide, axis=1, keepdims=True)
    normed = (wide * lax.rsqrt(mean + norm_eps) * gain_ref[...]).astype(bf16)
    sent = dot(placing.astype(bf16), normed)
    pack(lambda k: sent[:, k * HEAD : (k + 1) * HEAD], out_ref, swap_ref[...])


VMEM = pl.BlockSpec(memory_space=pltpu.VMEM)
HBM = pl.BlockSpec(memory_space=pltpu.HBM)


def project(attended, out_weight, residual, norm_gain, route, route_t, swap, peers):
    steps, rows, _ = attended.shape
    width = out_weight.shape[1]
    return pl.pallas_call(
        project_kernel,
        in_specs=[VMEM, HBM, VMEM, VMEM, VMEM, VMEM, VMEM],
        out_specs=[VMEM, VMEM],
        out_shape=[
            jax.ShapeDtypeStruct((rows, width), bf16),
            jax.ShapeDtypeStruct((peers, 160, HEAD), bf16),
        ],
        scratch_shapes=[
            pltpu.VMEM(out_weight.shape, bf16),
            pltpu.SemaphoreType.DMA((steps,)),
        ],
        compiler_params=room(56),
        name="project",
    )(attended, out_weight, residual, norm_gain, route, route_t, swap)


def rows_kernel(in_ref, swap_ref, x_ref):
    def store(k, block):
        x_ref[:, k * HEAD : (k + 1) * HEAD] = block.astype(bf16)

    unpack(in_ref, store, swap_ref[...])


def rows_in(arrived, swap):
    peers = arrived.shape[0]
    return pl.pallas_call(
        rows_kernel,
        in_specs=[VMEM, VMEM],
        out_specs=VMEM,
        out_shape=jax.ShapeDtypeStruct((peers * 10, 16 * HEAD), bf16),
        compiler_params=room(8),
        name="rows_in",
    )(arrived, swap)


def expert_kernel(counts, more, last, own_ref, sib_ref, *refs):
    pieces = []
    for count in counts:
        pieces.append(refs[:count])
        refs = refs[count:]
    if more:
        acc_ref, refs = refs[0], refs[1:]
    out_refs, (x, total) = refs[:-2], refs[-2:]
    rows = own_ref.shape[0]
    width = own_ref.shape[1]

    def take(piece, at, length):
        found, base = [], 0
        for ref in piece:
            lo, hi = max(at - base, 0), min(at + length - base, ref.shape[0])
            if lo < hi:
                found.append(ref[lo:hi, :])
            base += ref.shape[0]
        return found[0] if len(found) == 1 else jnp.concatenate(found, axis=0)

    x[:rows, :] = own_ref[...]
    x[rows:, :] = sib_ref[...]
    parts = []
    for i in range(0, len(pieces), 2):
        pair = pieces[i : i + 2]
        gate = dot(x[...], jnp.concatenate([take(p, 0, width) for p in pair], axis=1))
        up = dot(x[...], jnp.concatenate([take(p, width, width) for p in pair], axis=1))
        parts.append((gate / (1.0 + jnp.exp(-gate)) * up).astype(bf16))
    hid = jnp.concatenate(parts, axis=1)
    for k in range(0, width // HEAD, 2):
        down = jnp.concatenate(
            [
                jnp.concatenate([take(p, 2 * width + c * HEAD, HEAD) for p in pieces], axis=0)
                for c in (k, k + 1)
            ],
            axis=1,
        )
        cols = slice(k * HEAD, (k + 2) * HEAD)
        total[...] = dot(hid, down)
        if more:
            total[...] += acc_ref[:, cols]
        if last:
            keep_ref, send_ref = out_refs
            keep_ref[:, cols] = total[:rows, :]
            send_ref[:, cols] = total[rows:, :].astype(bf16)
        else:
            out_refs[0][:, cols] = total[...]


def expert(own, sib, pieces, acc, last):
    rows, width = own.shape
    flat = [array for piece in pieces for array in piece]
    if last:
        out_shape = [
            jax.ShapeDtypeStruct((rows, width), f32),
            jax.ShapeDtypeStruct((rows, width), bf16),
        ]
    else:
        out_shape = [jax.ShapeDtypeStruct((2 * rows, width), f32)]
    more = [] if acc is None else [acc]
    return pl.pallas_call(
        functools.partial(
            expert_kernel, tuple(len(piece) for piece in pieces), acc is not None, last
        ),
        in_specs=[VMEM] * (2 + len(flat) + len(more)),
        out_specs=[VMEM] * len(out_shape),
        out_shape=out_shape,
        scratch_shapes=[
            pltpu.VMEM((2 * rows, width), bf16),
            pltpu.VMEM((2 * rows, 2 * HEAD), f32),
        ],
        compiler_params=room(40),
        name="expert",
    )(own, sib, *flat, *more)


def finish_kernel(keep_ref, got_ref, swap_ref, out_ref):
    def rows_of(k):
        cols = slice(k * HEAD, (k + 1) * HEAD)
        return keep_ref[:, cols] + got_ref[:, cols].astype(f32)

    pack(rows_of, out_ref, swap_ref[...])


def finish(keep, got, swap, peers):
    return pl.pallas_call(
        finish_kernel,
        in_specs=[VMEM] * 3,
        out_specs=VMEM,
        out_shape=jax.ShapeDtypeStruct((peers, 160, HEAD), bf16),
        compiler_params=room(12),
        name="finish",
    )(keep, got, swap)


def plan_kernel(route_ref, route_t_ref, score_ref, prob_ref, pick_ref, mix_ref, swap_ref):
    rows = route_ref.shape[0]
    experts = pick_ref.shape[2] // 10
    later = lax.broadcasted_iota(jnp.int32, (rows, rows), 0)
    earlier = lax.broadcasted_iota(jnp.int32, (rows, rows), 1)
    slots = lax.broadcasted_iota(jnp.int32, (rows, experts * 10), 1)
    scores = score_ref[...]
    raised = jnp.exp(scores - jnp.max(scores, axis=1, keepdims=True))
    mixing = prob_ref[...] * (raised / jnp.sum(raised, axis=1, keepdims=True))
    for t in range(2):
        mine = route_ref[:, t : t + 1]
        ordinal = jnp.zeros((rows, 1), jnp.int32)
        for u in range(2):
            before = (earlier < later) if u >= t else (earlier <= later)
            same = route_t_ref[u : u + 1, :] == mine
            ordinal += jnp.sum(jnp.where(before & same, 1, 0), axis=1, keepdims=True)
        placed = slots == slot_of(mine, ordinal, experts)
        pick_ref[t] = jnp.where(placed, 1.0, 0.0).astype(bf16)
        mix_ref[t] = jnp.broadcast_to(mixing[:, t : t + 1], (rows, HEAD))
    swap_ref[...] = swap_matrix(experts, 16)


def plan(route, route_t, scores, prob, experts):
    rows = route.shape[0]
    return pl.pallas_call(
        plan_kernel,
        in_specs=[VMEM] * 4,
        out_specs=[VMEM] * 3,
        out_shape=[
            jax.ShapeDtypeStruct((2, rows, experts * 10), bf16),
            jax.ShapeDtypeStruct((2, rows, HEAD), f32),
            jax.ShapeDtypeStruct((experts * 32, experts * 32), bf16),
        ],
        compiler_params=room(8),
        name="plan",
    )(route, route_t, scores, prob)


def mix_kernel(in_ref, upd_ref, pick_ref, mix_ref, swap_ref, out_ref):
    def store(k, block):
        block = block.astype(bf16)
        cols = slice(k * HEAD, (k + 1) * HEAD)
        combined = sum(dot(pick_ref[t], block) * mix_ref[t] for t in range(2))
        out_ref[:, cols] = (upd_ref[:, cols].astype(f32) + combined).astype(bf16)

    unpack(in_ref, store, swap_ref[...])


def mix(returned, updated, picks, mixing, swap):
    return pl.pallas_call(
        mix_kernel,
        in_specs=[VMEM] * 5,
        out_specs=VMEM,
        out_shape=jax.ShapeDtypeStruct(updated.shape, bf16),
        compiler_params=room(12),
        name="mix",
    )(returned, updated, picks, mixing, swap)


def shift(value, axis, by):
    size = lax.axis_size(axis)
    return lax.ppermute(value, axis, [(i, (i + by) % size) for i in range(size)])


def onward(value, axis):
    size = lax.axis_size(axis)
    pairs = []
    for i in range(size):
        pairs.append((2 * i, 2 * ((i + 1) % size)))
        pairs.append((2 * i + 1, 2 * ((i - 1) % size) + 1))
    return lax.ppermute(value, (axis, "core"), pairs)


def swap_cores(value):
    return lax.ppermute(value, "core", ((0, 1), (1, 0)))


def local(
    queries,
    keys,
    values,
    query_gain,
    key_gain,
    out_weight,
    residual,
    norm_gain,
    route_experts,
    expert_scores,
    group_prob,
    w_gate,
    w_up,
    w_down,
):
    peers = lax.axis_size(SP)
    core = lax.axis_index("core")
    z = lax.axis_index("z")
    seq = lax.axis_index(SP)
    tokens = queries.shape[0]

    where = jnp.stack([core, z // 2]).astype(jnp.int32)
    lane = jnp.arange(HEAD, dtype=jnp.int32)
    pair = (lane // 2) % (HEAD // 4)
    frequency = rope_base ** (-pair.astype(f32) * 4.0 / HEAD)
    grid_rows = tokens // GRID_W
    place = jnp.arange(grid_rows + GRID_W, dtype=jnp.int32)
    place = jnp.where(place < grid_rows, seq * grid_rows + place, place - grid_rows)
    angles = place.astype(f32)[:, None] * frequency[None, :]
    cosine = jnp.cos(angles)
    sine = jnp.sin(angles) * jnp.where(lane % 2 == 0, -1.0, 1.0)[None, :]

    w0 = bundle(w_gate[0], w_up[0], w_down[0]).reshape(-1, HEAD)
    w1p, w1m = shift(w0, "z", 1), shift(w0, "z", -1)
    route_t = route_experts.T
    picks, mixing, swap = plan(
        route_experts, route_t, expert_scores, group_prob[:, None], peers
    )
    own, kv_a, kv_b = prep(
        where, queries, keys, values, query_gain[None, :], key_gain[None, :], cosine, sine
    )
    ax, by = stack(
        [kv_a] + [shift(kv_a, "x", d) for d in (1, -1, 2)],
        [kv_b] + [shift(kv_b, "y", d) for d in (1, -1, 2)],
    )
    sib = swap_cores(own)
    a_next = [shift(ax, "y", 1), shift(ax, "y", -1)]
    b_next = [shift(by, "x", 1), shift(by, "x", -1)]
    state = attend(where, own, sib, [ax, by], None, False)
    w1p, w1m, state, a_next, b_next = lax.optimization_barrier((w1p, w1m, state, a_next, b_next))
    w2p, w2m = shift(w1p, "z", 1), shift(w1m, "z", -1)
    a_far = onward(jnp.where(core == 0, a_next[0], a_next[1]), "y")
    b_far = onward(jnp.where(core == 0, b_next[0], b_next[1]), "x")
    state = attend(where, own, sib, a_next + b_next, state, False)
    keep, send = attend(where, own, sib, [a_far, b_far], state, True)
    got = swap_cores(send)
    w2p, w2m, _ = lax.optimization_barrier((w2p, w2m, keep))
    third = w0.shape[0] // 3
    w3p = [shift(w2p[:third], "z", 1)]
    w3m = [shift(w2m[:third], "z", -1)]
    merged = merge(where, keep, got)
    attended = lax.all_to_all(merged, "z", 0, 0, tiled=True)
    rest_p, rest_m, attended = lax.optimization_barrier((w2p[third:], w2m[third:], attended))
    w3p.append(shift(rest_p, "z", 1))
    w3m.append(shift(rest_m, "z", -1))
    w4 = [shift(w3p[0], "z", 1)]
    updated, outgoing = project(
        attended,
        out_weight,
        residual,
        norm_gain[None, :],
        route_experts,
        route_t,
        swap,
        peers,
    )
    arrived = lax.all_to_all(outgoing, SP, 0, 0, tiled=True)
    rest_p, rest_m, arrived = lax.optimization_barrier((w3p[1], w3m[1], arrived))
    cut = 3 * third // 4
    w4 += [shift(rest_m[cut:], "z", -1), shift(rest_p[:cut], "z", 1)]
    w4 = [w4[0], w4[2], w4[1]]
    rows = rows_in(arrived, swap)
    sib_rows = swap_cores(rows)
    (acc,) = expert(rows, sib_rows, [[w0], [w1p], [w1m], [w2p], [w2m], w3p], None, False)
    keep, send = expert(rows, sib_rows, [w3m, w4], acc, True)
    result = finish(keep, swap_cores(send), swap, peers)
    returned = lax.all_to_all(result, SP, 0, 0, tiled=True)
    return mix(returned, updated, picks, mixing, swap)


def solution(mesh):
    torus = Mesh(mesh.devices.reshape(4, 4, 8, 2), ("y", "x", "z", "core"))
    placed = (
        P(SP, TP),
        P(SP, None),
        P(SP, None),
        P(TP),
        P(),
        P(),
        P(SP_TP, None),
        P(),
        P(SP_TP, None),
        P(SP_TP, None),
        P(SP_TP),
        P(SP, None, TP),
        P(SP, None, TP),
        P(SP, TP, None),
    )
    return jax.shard_map(
        local, mesh=torus, in_specs=placed, out_specs=P(SP_TP, None), check_vma=False
    )
```
